32 devices in a mesh: sp: 16 (over z, y, x), tp: 2 (over core).
Axes of the slice: x: 2, y: 2, z: 4, core: 2. Of those that a mesh axis runs over, the one named last changes fastest.
Arguments:
- layer_source_tokens: bfloat16 [2, 1024, 4096], P(None, 'sp'), may hold values from -6 to 6
- address_projection: bfloat16 [4096, 2048], P('sp', 'tp'), may hold values from -0.09375 to 0.09375
- content_projection: bfloat16 [4096, 2048], P('sp', 'tp'), may hold values from -0.09375 to 0.09375
- strength_projection: bfloat16 [4096, 16], replicated, may hold values from -0.09375 to 0.09375
- fading_driver_projection: bfloat16 [4096, 16], replicated, may hold values from -0.25 to 0.25
- strength_offset: float32 [16], P('tp'), may hold values from -2.5 to 1
- channel_fading_speed: float32 [16], P('tp')
- added_fading_exponent: float32 [2, 1024, 16], P(None, 'sp', 'tp'), may hold values from -0.7 to 0, as said below
- first_step_probe: bfloat16 [2, 2048], P(None, 'tp'), may hold values from -6 to 6
- first_step_address: bfloat16 [2, 2048], P(None, 'tp'), may hold values from -6 to 6
- first_step_content: bfloat16 [2, 2048], P(None, 'tp'), may hold values from -6 to 6
- first_step_outgate: bfloat16 [2, 2048], P(None, 'tp'), may hold values from -6 to 6
- first_step_strength_raw: float32 [2, 16], P(None, 'tp'), may hold values from -6 to 6
- channel_scaling_factor: float32 [128], replicated, may hold values from 0.1 to 1.9
- readout_projection: bfloat16 [2048, 4096], P('tp', 'sp'), may hold values from -0.125 to 0.125
Outputs:
- state_cache: bfloat16 [2, 16, 128, 128], P(None, 'tp')
- mixed_read: bfloat16 [2, 4096], P(None, 'sp')
- boundary_cache: bfloat16 [2, 16, 16, 128, 128], P(None, 'sp', 'tp')
The draws below stay inside these ranges and needn't reach their ends.
Inputs may be any that keep to these rules, and one draw needn't show every extreme that they name: `added_fading_exponent`: zero at most positions.
All inputs are finite; a program needn't handle non-finite values.
Results may differ from the reference program's by a relative error of at most 0.017.
Values may be sent and summed in bfloat16 or wider, within the bound.
A program may use at most 64 MiB of HBM per device.

```python
import jax
import jax.numpy as jnp
from jax import lax

D = 4096
H = 16
ADDRESS_WIDTH = 128
BLOCK = 64
NSEQ = 2
LEN = 1024
RANGES = 16
N_TP = 2


def draw_channel_fading_speed(key, part):
    low_rate = 0.3 / LEN
    high_rate = 0.05
    uniform_draw = jax.random.uniform(jax.random.fold_in(key, 11), (H,), jnp.float32)
    return jnp.exp(jnp.log(low_rate) + uniform_draw * (jnp.log(high_rate) - jnp.log(low_rate)))


def draw_added_fading_exponent(key, part):
    chosen = jax.random.uniform(jax.random.fold_in(key, 21), (NSEQ, LEN, H), jnp.float32)
    kept_share = jax.random.uniform(jax.random.fold_in(key, 22), (NSEQ, LEN, H), jnp.float32, 0.5, 0.8)
    return jnp.where(chosen < 3.0 / LEN, jnp.log(kept_share), 0.0)


def block_levels(rng, shape, shards, low, top_value):
    factor_of = 1.0
    for position, shards_of in shards:
        steps = jax.random.uniform(jax.random.fold_in(jax.random.fold_in(rng, 6), position), (shards_of,), jnp.float32, low / len(shards), top_value / len(shards))
        factor_of = factor_of * jnp.repeat(jnp.exp(steps), shape[position] // shards_of).reshape((-1,) + (1,) * (len(shape) - 1 - position))
    return factor_of


def centred(own_key, dims, width, most, shards=(), kind=jnp.bfloat16):
    drawn = width * jax.random.normal(own_key, dims, jnp.float32)
    if shards:
        drawn = drawn * block_levels(own_key, dims, shards, -0.22, 0.18)
    return jnp.clip(drawn, -most, most).astype(kind)


def setup_inputs(seed: int = 0) -> dict:
    key_list = jax.random.split(jax.random.key(seed), 16)
    layer_source_tokens = centred(key_list[0], (NSEQ, LEN, D), 1.0, 6.0, ((1, 16),))
    address_projection = centred(key_list[1], (D, H * ADDRESS_WIDTH), D ** -0.5, 0.09375, ((0, 16), (1, 2)))
    content_projection = centred(key_list[2], (D, H * ADDRESS_WIDTH), D ** -0.5, 0.09375, ((0, 16), (1, 2)))
    strength_projection = centred(key_list[3], (D, H), D ** -0.5, 0.09375)
    fading_driver_projection = centred(key_list[4], (D, H), (D // 9) ** -0.5, 0.25)
    strength_offset = jnp.clip(-2.5 + 3.5 * jax.random.uniform(key_list[5], (H,), jnp.float32) ** block_levels(key_list[5], (H,), ((0, 2),), -0.2, 0.2), -2.5, 1.0)
    channel_fading_speed = draw_channel_fading_speed(jax.random.fold_in(key_list[15], 71), 0)
    added_fading_exponent = draw_added_fading_exponent(jax.random.fold_in(key_list[15], 71), 0)
    first_step_probe = centred(key_list[8], (NSEQ, H * ADDRESS_WIDTH), 1.0, 6.0, ((1, 2),))
    first_step_address = centred(key_list[9], (NSEQ, H * ADDRESS_WIDTH), 1.0, 6.0, ((1, 2),))
    first_step_content = centred(key_list[10], (NSEQ, H * ADDRESS_WIDTH), 1.0, 6.0, ((1, 2),))
    first_step_outgate = centred(key_list[11], (NSEQ, H * ADDRESS_WIDTH), 1.0, 6.0, ((1, 2),))
    first_step_strength_raw = centred(key_list[12], (NSEQ, H), 1.5, 6.0, ((1, 2),), jnp.float32)
    channel_scaling_factor = jnp.clip(1.0 + 0.18 * jax.random.normal(key_list[13], (ADDRESS_WIDTH,), jnp.float32), 0.1, 1.9)
    readout_projection = centred(key_list[14], (H * ADDRESS_WIDTH, D), (H * ADDRESS_WIDTH) ** -0.5, 0.125, ((0, 2), (1, 16)))
    return {"layer_source_tokens": layer_source_tokens, "address_projection": address_projection, "content_projection": content_projection, "strength_projection": strength_projection, "fading_driver_projection": fading_driver_projection, "strength_offset": strength_offset, "channel_fading_speed": channel_fading_speed, "added_fading_exponent": added_fading_exponent, "first_step_probe": first_step_probe, "first_step_address": first_step_address, "first_step_content": first_step_content, "first_step_outgate": first_step_outgate, "first_step_strength_raw": first_step_strength_raw, "channel_scaling_factor": channel_scaling_factor, "readout_projection": readout_projection}


EPSILON = 1e-06
HIGHEST_ACCURACY = lax.Precision.HIGHEST

def unit_inverse(lower_part):
    matrix_order = lower_part.shape[-1]
    identity = jnp.eye(matrix_order, dtype=jnp.float32)
    result = identity - lower_part
    power_term = lower_part
    reached = 2
    while reached < matrix_order:
        power_term = jnp.matmul(power_term, power_term, precision=HIGHEST_ACCURACY)
        result = jnp.matmul(result, identity + power_term, precision=HIGHEST_ACCURACY)
        reached = reached * 2
    return result

def build_arguments(address_vectors, content_vectors, outgate_raw_scores, strength_offset, channel_fading_speed, added_fading_exponent, channel_width):
    length = address_vectors.shape[0]
    attention_channels_total = channel_fading_speed.shape[0]
    address_token_slab = jax.nn.silu(address_vectors.astype(jnp.float32)).reshape(length, attention_channels_total, channel_width)
    address_token_slab = address_token_slab * lax.rsqrt(lax.optimization_barrier(jnp.sum(address_token_slab * address_token_slab, axis=-1, keepdims=True)) + EPSILON)
    content_token_slab = jax.nn.silu(content_vectors.astype(jnp.float32)).reshape(length, attention_channels_total, channel_width)
    strength_raw_expanded = outgate_raw_scores.astype(jnp.float32)
    storing_strength = jax.nn.sigmoid(strength_raw_expanded[:, :attention_channels_total] + strength_offset)
    fading_exponent = added_fading_exponent - channel_fading_speed * jax.nn.softplus(strength_raw_expanded[:, attention_channels_total:])
    return (address_token_slab, content_token_slab, storing_strength, fading_exponent)

def final_state(address_token_slab, content_token_slab, storing_strength, fading_exponent, block):
    length, attention_channels_total, channel_width = address_token_slab.shape
    blocks = length // block

    def split_blocks(tensor):
        moved_axes = jnp.swapaxes(tensor, 0, 1)
        return moved_axes.reshape((attention_channels_total, blocks, block) + moved_axes.shape[2:])
    block_keys = split_blocks(address_token_slab)
    block_values = split_blocks(content_token_slab)
    block_beta = split_blocks(storing_strength)
    cumulative = jnp.cumsum(split_blocks(fading_exponent), axis=-1)
    positions = jnp.arange(block)
    strict = positions[:, None] > positions[None, :]
    spread_log = jnp.where(strict, cumulative[..., :, None] - cumulative[..., None, :], 0.0)
    scaled_keys = block_keys * block_beta[..., None]
    inner_prod = jnp.einsum('hnik,hnjk->hnij', scaled_keys, block_keys, precision=HIGHEST_ACCURACY)
    lower_part = jnp.where(strict, inner_prod * jnp.exp(spread_log), 0.0)
    inverse = unit_inverse(lower_part)
    targets = jnp.concatenate([block_values * block_beta[..., None], scaled_keys * jnp.exp(cumulative)[..., None]], axis=-1)
    solved = jnp.einsum('hnij,hnjk->hnik', inverse, targets, precision=HIGHEST_ACCURACY)
    updates = solved[..., :channel_width]
    key_weights = solved[..., channel_width:]
    tail_keys = block_keys * jnp.exp(cumulative[..., -1:] - cumulative)[..., None]
    last_decay = jnp.exp(cumulative[..., -1])

    def advance(carried_state, block_items):
        update_index, weight_index, tail_index, last_index = block_items
        fresh_value_rows = update_index - jnp.einsum('xbg,xgp->xbp', weight_index, carried_state, precision=HIGHEST_ACCURACY)
        carried_state = carried_state * last_index[:, None, None] + jnp.einsum('tjo,tjw->tow', tail_index, fresh_value_rows, precision=HIGHEST_ACCURACY)
        return (carried_state, None)

    def range_advance(carried_state, range_items):
        carried_state, _ = lax.scan(advance, carried_state, range_items)
        return (carried_state, carried_state)
    blocks_per_range = blocks // RANGES
    initial = jnp.zeros((attention_channels_total, channel_width, channel_width), jnp.float32)
    block_items = (jnp.moveaxis(updates, 1, 0), jnp.moveaxis(key_weights, 1, 0), jnp.moveaxis(tail_keys, 1, 0), jnp.moveaxis(last_decay, 1, 0))
    range_items = tuple((item.reshape((RANGES, blocks_per_range) + item.shape[1:]) for item in block_items))
    _, range_states = lax.scan(range_advance, initial, range_items)
    return range_states

def read_heads(state_cache, first_step_probe, first_step_address, first_step_content, first_step_outgate, first_step_strength_raw, channel_scaling_factor):
    seq_count, attention_channels_total, channel_width, _ = state_cache.shape
    carried_state = state_cache.astype(jnp.float32)

    def activate(tensor):
        return jax.nn.silu(tensor.astype(jnp.float32)).reshape(seq_count, attention_channels_total, channel_width)
    query_rows = activate(first_step_probe)
    address_token_slab = activate(first_step_address)
    address_token_slab = address_token_slab * lax.rsqrt(lax.optimization_barrier(jnp.sum(address_token_slab * address_token_slab, axis=-1, keepdims=True)) + EPSILON)
    content_token_slab = activate(first_step_content)
    storing_strength = jax.nn.sigmoid(first_step_strength_raw)
    recalled = jnp.einsum('nhk,nhkv->nhv', address_token_slab, carried_state, precision=HIGHEST_ACCURACY)
    updated = carried_state + storing_strength[..., None, None] * address_token_slab[..., :, None] * (content_token_slab - recalled)[..., None, :]
    output = jnp.einsum('nhk,nhkv->nhv', query_rows, updated, precision=HIGHEST_ACCURACY)
    normed = output * lax.rsqrt(lax.optimization_barrier(jnp.mean(output * output, axis=-1, keepdims=True)) + EPSILON) * channel_scaling_factor
    gated_out = normed * activate(first_step_outgate)
    return gated_out.reshape(seq_count, attention_channels_total * channel_width).astype(jnp.bfloat16)

def reference(layer_source_tokens, address_projection, content_projection, strength_projection, fading_driver_projection, strength_offset, channel_fading_speed, added_fading_exponent, first_step_probe, first_step_address, first_step_content, first_step_outgate, first_step_strength_raw, channel_scaling_factor, readout_projection):
    seq_count, length, model_width = layer_source_tokens.shape
    flat_rows = layer_source_tokens.reshape(seq_count * length, model_width)

    def product(weight):
        return jnp.dot(flat_rows, weight, preferred_element_type=jnp.float32).astype(jnp.bfloat16)
    address_vectors = product(address_projection).reshape(seq_count, length, -1)
    content_vectors = product(content_projection).reshape(seq_count, length, -1)
    outgate_raw_scores = jnp.concatenate([product(strength_projection), product(fading_driver_projection)], axis=-1).reshape(seq_count, length, -1)

    def solitary_prompt(prompt_members):
        address_token_list, content_token_list, strength_raw_list, prompt_group_tokens = prompt_members
        address_token_slab, content_token_slab, storing_strength, fading_exponent = build_arguments(address_token_list, content_token_list, strength_raw_list, strength_offset, channel_fading_speed, prompt_group_tokens, ADDRESS_WIDTH)
        return final_state(address_token_slab, content_token_slab, storing_strength, fading_exponent, BLOCK)
    range_memories = lax.map(solitary_prompt, (address_vectors, content_vectors, outgate_raw_scores, added_fading_exponent))
    boundary_cache = range_memories.astype(jnp.bfloat16)
    state_cache = range_memories[:, -1].astype(jnp.bfloat16)
    heads_read = read_heads(state_cache, first_step_probe, first_step_address, first_step_content, first_step_outgate, first_step_strength_raw, channel_scaling_factor)
    group_rows = heads_read.astype(jnp.float32).reshape(seq_count, N_TP, -1)
    group_weights = readout_projection.astype(jnp.float32).reshape(N_TP, -1, model_width)
    group_terms = jnp.einsum('stc,tcd->tsd', group_rows, group_weights)
    rounded = lax.optimization_barrier(group_terms.astype(jnp.bfloat16))
    mixed_read = lax.optimization_barrier(jnp.sum(rounded.astype(jnp.float32), axis=0)).astype(jnp.bfloat16)
    return (state_cache, mixed_read, boundary_cache)
```

```python
import jax
import jax.numpy as jnp
from jax import lax
from jax.experimental import pallas as pl
from jax.experimental.pallas import tpu as pltpu
from jax.sharding import PartitionSpec as P

ADDRESS_WIDTH = 128
BLOCK = 64


EPSILON = 1e-06
HIGHEST_ACCURACY = lax.Precision.HIGHEST


def prefix(array, axis, combine, identity):
    peers, index = (lax.axis_size(axis), lax.axis_index(axis))
    everything = jax.tree.map(
        lambda part, kind: lax.all_gather(part.astype(kind), axis),
        array,
        (jnp.bfloat16, jnp.bfloat16),
    )
    start = jax.tree.map(
        lambda part, zero: jnp.broadcast_to(jnp.asarray(zero, part.dtype), part.shape),
        array,
        identity,
    )

    def step(k, before):
        reached = k < index
        new = combine(
            before, jax.tree.map(lambda part, own: part[k].astype(own.dtype), everything, array)
        )
        return jax.tree.map(lambda a, b: jnp.where(reached, a, b), new, before)

    return lax.fori_loop(0, peers, step, start)


def as_sent(array):
    return jax.tree.map(lambda a: a.astype(jnp.bfloat16) if a.dtype == jnp.float32 else a, array)


def broadcast(value, axis, source):
    kept = jnp.where(lax.axis_index(axis) == source, value, 0).astype(value.dtype)
    return lax.psum(kept, axis)


def unit_inverse(lower_part):
    matrix_order = lower_part.shape[-1]
    identity = jnp.eye(matrix_order, dtype=jnp.float32)
    result = identity - lower_part
    power_term = lower_part
    reached = 2
    while reached < matrix_order:
        power_term = jnp.matmul(power_term, power_term, precision=HIGHEST_ACCURACY)
        result = jnp.matmul(result, identity + power_term, precision=HIGHEST_ACCURACY)
        reached = reached * 2
    return result


def build_arguments(
    address_vectors,
    content_vectors,
    outgate_raw_scores,
    strength_offset,
    channel_fading_speed,
    added_fading_exponent,
    channel_width,
):
    length = address_vectors.shape[0]
    attention_channels_total = channel_fading_speed.shape[0]
    address_token_slab = jax.nn.silu(address_vectors.astype(jnp.float32)).reshape(
        length, attention_channels_total, channel_width
    )
    address_token_slab = address_token_slab * lax.rsqrt(
        jnp.sum(address_token_slab * address_token_slab, axis=-1, keepdims=True) + EPSILON
    )
    content_token_slab = jax.nn.silu(content_vectors.astype(jnp.float32)).reshape(
        length, attention_channels_total, channel_width
    )
    strength_raw_expanded = outgate_raw_scores.astype(jnp.float32)
    storing_strength = jax.nn.sigmoid(
        strength_raw_expanded[:, :attention_channels_total] + strength_offset
    )
    fading_exponent = added_fading_exponent - channel_fading_speed * jax.nn.softplus(
        strength_raw_expanded[:, attention_channels_total:]
    )
    return (address_token_slab, content_token_slab, storing_strength, fading_exponent)


def range_map(address_token_slab, content_token_slab, storing_strength, fading_exponent, block):
    length, attention_channels_total, channel_width = address_token_slab.shape
    blocks = length // block

    def split_blocks(tensor):
        moved_axes = jnp.swapaxes(tensor, 0, 1)
        return moved_axes.reshape((attention_channels_total, blocks, block) + moved_axes.shape[2:])

    block_keys = split_blocks(address_token_slab)
    block_values = split_blocks(content_token_slab)
    block_beta = split_blocks(storing_strength)
    cumulative = jnp.cumsum(split_blocks(fading_exponent), axis=-1)
    positions = jnp.arange(block)
    strict = positions[:, None] > positions[None, :]
    spread_log = jnp.where(strict, cumulative[..., :, None] - cumulative[..., None, :], 0.0)
    scaled_keys = block_keys * block_beta[..., None]
    inner_prod = jnp.einsum("hnik,hnjk->hnij", scaled_keys, block_keys, precision=HIGHEST_ACCURACY)
    lower_part = jnp.where(strict, inner_prod * jnp.exp(spread_log), 0.0)
    inverse = unit_inverse(lower_part)
    targets = jnp.concatenate(
        [block_values * block_beta[..., None], scaled_keys * jnp.exp(cumulative)[..., None]],
        axis=-1,
    )
    solved = jnp.einsum("hnij,hnjk->hnik", inverse, targets, precision=HIGHEST_ACCURACY)
    updates = solved[..., :channel_width]
    key_weights = solved[..., channel_width:]
    tail_keys = block_keys * jnp.exp(cumulative[..., -1:] - cumulative)[..., None]
    last_decay = jnp.exp(cumulative[..., -1])
    identity = jnp.eye(channel_width, dtype=jnp.float32)

    def advance(state_pair, block_items):
        transition, carried_state = state_pair
        update_index, weight_index, tail_index, last_index = block_items
        fresh_value_rows = update_index - jnp.einsum(
            "xbg,xgp->xbp", weight_index, carried_state, precision=HIGHEST_ACCURACY
        )
        carried_state = carried_state * last_index[:, None, None] + jnp.einsum(
            "tjo,tjw->tow", tail_index, fresh_value_rows, precision=HIGHEST_ACCURACY
        )
        block_move = last_index[:, None, None] * identity - jnp.einsum(
            "hck,hcj->hkj", tail_index, weight_index, precision=HIGHEST_ACCURACY
        )
        transition = jnp.einsum("hij,hjk->hik", block_move, transition, precision=HIGHEST_ACCURACY)
        return ((transition, carried_state), None)

    initial = (
        jnp.broadcast_to(identity, (attention_channels_total, channel_width, channel_width)),
        jnp.zeros((attention_channels_total, channel_width, channel_width), jnp.float32),
    )
    block_items = (
        jnp.moveaxis(updates, 1, 0),
        jnp.moveaxis(key_weights, 1, 0),
        jnp.moveaxis(tail_keys, 1, 0),
        jnp.moveaxis(last_decay, 1, 0),
    )
    (transition, carried_state), _ = lax.scan(advance, initial, block_items)
    return (transition, carried_state)


def read_heads(
    state_cache,
    first_step_probe,
    first_step_address,
    first_step_content,
    first_step_outgate,
    first_step_strength_raw,
    channel_scaling_factor,
):
    seq_count, attention_channels_total, channel_width, _ = state_cache.shape
    carried_state = state_cache.astype(jnp.float32)

    def activate(tensor):
        return jax.nn.silu(tensor.astype(jnp.float32)).reshape(
            seq_count, attention_channels_total, channel_width
        )

    query_rows = activate(first_step_probe)
    address_token_slab = activate(first_step_address)
    address_token_slab = address_token_slab * lax.rsqrt(
        jnp.sum(address_token_slab * address_token_slab, axis=-1, keepdims=True) + EPSILON
    )
    content_token_slab = activate(first_step_content)
    storing_strength = jax.nn.sigmoid(first_step_strength_raw)
    recalled = jnp.einsum(
        "nhk,nhkv->nhv", address_token_slab, carried_state, precision=HIGHEST_ACCURACY
    )
    updated = (
        carried_state
        + storing_strength[..., None, None]
        * address_token_slab[..., :, None]
        * (content_token_slab - recalled)[..., None, :]
    )
    output = jnp.einsum("nhk,nhkv->nhv", query_rows, updated, precision=HIGHEST_ACCURACY)
    normed = (
        output
        * lax.rsqrt(jnp.mean(output * output, axis=-1, keepdims=True) + EPSILON)
        * channel_scaling_factor
    )
    gated_out = normed * activate(first_step_outgate)
    return gated_out.reshape(seq_count, attention_channels_total * channel_width).astype(
        jnp.bfloat16
    )


def matmul_maps(left, right):
    return jnp.einsum("shij,shjk->shik", left, right, precision=HIGHEST_ACCURACY)


def join_pairs(earlier, later):
    return (matmul_maps(later[0], earlier[0]), matmul_maps(later[0], earlier[1]) + later[1])


def per_device(
    layer_source_tokens,
    address_projection,
    content_projection,
    strength_projection,
    fading_driver_projection,
    strength_offset,
    channel_fading_speed,
    added_fading_exponent,
    first_step_probe,
    first_step_address,
    first_step_content,
    first_step_outgate,
    first_step_strength_raw,
    channel_scaling_factor,
    readout_projection,
):
    head_local = channel_fading_speed.shape[0]
    first_head = lax.axis_index("tp") * head_local
    beta_slice = lax.dynamic_slice_in_dim(strength_projection, first_head, head_local, 1)
    alpha_slice = lax.dynamic_slice_in_dim(fading_driver_projection, first_head, head_local, 1)
    seq_count, local_len, model_width = layer_source_tokens.shape
    flat_rows = layer_source_tokens.reshape(seq_count * local_len, model_width)
    key_sum = jnp.dot(
        flat_rows,
        lax.all_gather(address_projection, "sp", axis=0, tiled=True),
        preferred_element_type=jnp.float32,
    )
    value_sum = jnp.dot(
        flat_rows,
        lax.all_gather(content_projection, "sp", axis=0, tiled=True),
        preferred_element_type=jnp.float32,
    )
    beta_sum = jnp.dot(flat_rows, beta_slice, preferred_element_type=jnp.float32)
    alpha_sum = jnp.dot(flat_rows, alpha_slice, preferred_element_type=jnp.float32)
    outgate_raw_scores = (
        jnp.concatenate([beta_sum, alpha_sum], axis=1)
        .astype(jnp.bfloat16)
        .reshape(seq_count, local_len, -1)
    )
    address_vectors = key_sum.astype(jnp.bfloat16).reshape(seq_count, local_len, -1)
    content_vectors = value_sum.astype(jnp.bfloat16).reshape(seq_count, local_len, -1)
    transitions = []
    offsets = []
    for prompt_number in range(seq_count):
        address_token_slab, content_token_slab, storing_strength, fading_exponent = build_arguments(
            address_vectors[prompt_number],
            content_vectors[prompt_number],
            outgate_raw_scores[prompt_number],
            strength_offset,
            channel_fading_speed,
            added_fading_exponent[prompt_number],
            ADDRESS_WIDTH,
        )
        transition, carried_state = range_map(
            address_token_slab, content_token_slab, storing_strength, fading_exponent, BLOCK
        )
        transitions.append(transition)
        offsets.append(carried_state)
    transition = jnp.stack(transitions)
    offset = jnp.stack(offsets)
    identity = jnp.broadcast_to(jnp.eye(ADDRESS_WIDTH, dtype=jnp.float32), transition.shape)
    entered = prefix((transition, offset), "sp", join_pairs, (identity, jnp.zeros_like(offset)))
    leaving = matmul_maps(transition, entered[1]) + offset
    final = broadcast(as_sent(leaving), "sp", lax.axis_size("sp") - 1).astype(leaving.dtype)
    boundary_cache = leaving.astype(jnp.bfloat16)[:, None]
    state_cache = final.astype(jnp.bfloat16)
    heads_read = read_heads(
        state_cache,
        first_step_probe,
        first_step_address,
        first_step_content,
        first_step_outgate,
        first_step_strength_raw,
        channel_scaling_factor,
    )
    group_terms = jnp.dot(
        heads_read, readout_projection, preferred_element_type=jnp.float32
    ).astype(jnp.bfloat16)
    mixed_read = lax.psum(group_terms.astype(jnp.float32).astype(jnp.bfloat16), "tp")
    return (state_cache, mixed_read, boundary_cache)


MESH = pl.DeviceIdType.MESH
PIECES = 2
DEEP = 4
PLANE = 4


def remote(src, dst, send, recv, sp, tp):
    return pltpu.make_async_remote_copy(
        src_ref=src,
        dst_ref=dst,
        send_sem=send,
        recv_sem=recv,
        device_id={"sp": sp, "tp": tp},
        device_id_type=MESH,
    )


def silu(v):
    return v / (1.0 + jnp.exp(-v))


def sigmoid(v):
    return 1.0 / (1.0 + jnp.exp(-v))


def softplus(v):
    return jnp.maximum(v, 0.0) + jnp.log1p(jnp.exp(-jnp.abs(v)))


def halves(a):
    high = a.astype(jnp.bfloat16)
    return high, (a - high.astype(jnp.float32)).astype(jnp.bfloat16)


NN = (((1,), (0,)), ((), ()))
NT = (((1,), (1,)), ((), ()))
TN = (((0,), (0,)), ((), ()))


def dot3(a, b, dims=NN):
    def one(p, q):
        return lax.dot_general(p, q, dims, preferred_element_type=jnp.float32)

    (ah, al), (bh, bl) = a, b
    return one(ah, bh) + (one(ah, bl) + one(al, bh))


def choose(table, index):
    value = jnp.int32(table[0])
    for at in range(1, len(table)):
        value = jnp.where(index == at, jnp.int32(table[at]), value)
    return value


def by_distance(k):
    order = []
    for z in range(DEEP):
        others = sorted((abs(o - z), o) for o in range(DEEP) if o != z)
        order.append(others[k - 1][1])
    return order


def prefill_kernel(
    peers,
    tok,
    wk,
    wv,
    gate_b,
    gate_a,
    add,
    offset,
    speed,
    probe,
    address,
    content,
    outgate,
    strength,
    gain,
    readout,
    final,
    bound,
    mixed,
    xall,
    wall,
    wcross,
    tokv,
    gatev,
    addv,
    logit,
    msg,
    gall,
    keep,
    give,
    got,
    pair,
    states,
    rv,
    rmsg,
    rall,
    part,
    partgot,
    load,
    own_sem,
    z_send,
    tok_recv,
    x_send,
    y_send,
    xf_send,
    yf_send,
    w_send,
    w_recv,
    c_recv,
    relay_send,
    cross_send,
    outer_send,
    blk_recv,
    g_send,
    g_recv,
    give_send,
    give_recv,
    f_send,
    f_recv,
    b_send,
    b_recv,
    r_send,
    r_recv,
    t_send,
    t_recv,
):
    s, t = lax.axis_index("sp"), lax.axis_index("tp")
    heads = add.shape[1]
    width = ADDRESS_WIDTH
    length = tok.shape[1]
    half = tok.shape[2] // 2
    rows = wk.shape[0]
    piece = length // PIECES
    x, y, z = s % 2, (s // 2) % 2, s // PLANE
    prompt, side = z % 2, z // 2
    j = side * PLANE + s % PLANE
    mate = z + 1 - 2 * prompt
    columns = pl.ds(pl.multiple_of(t * half, 128), half)

    def chip(cx, cy, cz):
        return PLANE * cz + 2 * cy + cx

    def slot_of(c):
        return (c // PLANE % 2) * heads + (c // PLANE // 2) * PLANE + c % PLANE

    x_peer, y_peer, z_peer = chip(1 - x, y, z), chip(x, 1 - y, z), chip(x, y, mate)
    diagonal = chip(1 - x, 1 - y, z)
    home = t == side

    def part_of(i):
        return pl.ds(i * piece, piece)

    sent = []

    def go(copy):
        copy.start()
        sent.append(copy)

    def token_wait(c, i):
        ref = xall.at[c, part_of(i)]
        remote(ref, ref, own_sem, tok_recv.at[c, i], s, t).wait_recv()

    loads = []
    for i, (src, dst) in enumerate(
        (
            (tok, tokv),
            (gate_b, gatev.at[0]),
            (gate_a, gatev.at[1]),
            (add, addv),
            (readout, rv),
        )
    ):
        copy = pltpu.make_async_copy(src, dst, load.at[i])
        copy.start()
        loads.append(copy)

    near = [z] + [choose(by_distance(k), z) for k in range(1, DEEP)]
    for k in range(1, DEEP):
        for i in range(PIECES):
            go(
                remote(
                    tok.at[near[k] % 2, part_of(i), columns],
                    xall.at[s, part_of(i)],
                    z_send.at[k, i],
                    tok_recv.at[s, i],
                    chip(x, y, near[k]),
                    t,
                )
            )
    own = pltpu.make_async_copy(tok.at[prompt, :, columns], xall.at[s], own_sem)
    own.start()

    side_of = (t + side) % 2
    own_row = s % (peers // 2)
    q_own = s % PLANE
    spot = pl.ds(pl.multiple_of(own_row * rows, 16), rows)

    def weight_copies(dx, dy, cross, kv):
        xd, yd = (x + dx) % 2, (y + dy) % 2
        head = ((side + cross) % 2) * PLANE + 2 * yd + xd
        src = (wk, wv)[kv].at[:, pl.ds(pl.multiple_of(head * width, 128), width)]
        at = pl.ds(pl.multiple_of((2 * side_of + kv) * width, 128), width)
        if cross:
            dst, sem = wcross.at[q_own, :, at], c_recv.at[q_own, 2 * side_of + kv]
        else:
            dst, sem = wall.at[spot, at], w_recv.at[own_row, 2 * side_of + kv]
        out = w_send.at[2 * dy + dx, 2 * cross + kv]
        return src, dst, sem, remote(src, dst, out, sem, chip(xd, yd, z), side)

    for dx, dy in ((0, 0), (1, 0), (0, 1), (1, 1)):
        for cross in (1, 0):
            for kv in range(2):
                src, dst, sem, copy = weight_copies(dx, dy, cross, kv)
                if dx + dy == 0:

                    @pl.when(home)
                    def _():
                        pltpu.make_async_copy(src, dst, sem).start()

                    @pl.when(jnp.logical_not(home))
                    def _():
                        copy.start()
                else:
                    go(copy)

    for i in range(PIECES):
        src = tok.at[prompt, part_of(i), columns]
        dst = xall.at[s, part_of(i)]
        go(remote(src, dst, x_send.at[0, i], tok_recv.at[s, i], x_peer, t))
        go(remote(src, dst, y_send.at[0, i], tok_recv.at[s, i], y_peer, t))

    loads[0].wait()
    loads[1].wait()
    loads[2].wait()
    loads[3].wait()
    total_heads = gate_b.shape[0]
    msg[...] = jnp.zeros_like(msg)
    for p in range(2):
        for kind in range(2):
            logit[p, kind] = (
                lax.dot_general(gatev[kind], tokv[p], NT, preferred_element_type=jnp.float32)
                .astype(jnp.bfloat16)
                .astype(jnp.float32)
            )
        for h in range(heads):
            for kind in range(2):
                msg[p, h, kind : kind + 1, :] = logit[p, kind, pl.ds(t * heads + h, 1), :]
            msg[p, h, 2:3, :] = addv[p, h : h + 1, :]
    for off in range(1, peers):
        to = (s + off) % peers
        to_z = to // PLANE
        go(
            remote(
                msg.at[to_z % 2, (to_z // 2) * PLANE + to % PLANE],
                gall.at[s],
                g_send.at[off],
                g_recv.at[s],
                to,
                t,
            )
        )
    gall[s] = msg[prompt, j]

    def home_relay(dx, dy):
        q = 2 * ((y + dy) % 2) + (x + dx) % 2
        row = prompt * PLANE + q
        block = wall.at[pl.ds(pl.multiple_of(row * rows, 16), rows)]
        landing = chip(x, y, DEEP // 2 - side)
        for c in range(4):
            one = wcross.at[q, :, pl.ds(c * width, width)]
            pltpu.make_async_copy(one, one, c_recv.at[q, c]).wait()
        remote(
            wcross.at[q], block, cross_send.at[q], blk_recv.at[row], landing, t
        ).start()
        for c in range(4):
            one = wall.at[
                pl.ds(pl.multiple_of(row * rows, 16), rows), pl.ds(c * width, width)
            ]
            pltpu.make_async_copy(one, one, w_recv.at[row, c]).wait()
        remote(block, block, relay_send.at[q], blk_recv.at[row], z_peer, t).start()

    inner = prompt != side
    lands = jnp.logical_and(jnp.logical_not(home), inner)

    def block_of(row):
        return wall.at[pl.ds(pl.multiple_of(row * rows, 16), rows)]

    def land_relay(n):
        row = arrival_row(n)
        ref = block_of(row)
        remote(ref, ref, outer_send.at[n], blk_recv.at[row], s, t).wait_recv()
        remote(ref, ref, outer_send.at[n], blk_recv.at[row], z_peer, t).start()

    def arrival_row(n):
        plane = (side + n) % 2
        step = n // 2
        q = 2 * ((y + step // 2) % 2) + (x + step % 2) % 2
        return plane * PLANE + q

    def on_home(dx, dy):
        @pl.when(home)
        def _():
            home_relay(dx, dy)

    def on_land(ns):
        @pl.when(lands)
        def _():
            for n in ns:
                land_relay(n)

    def spread_column(k):
        for i in range(PIECES):
            c = chip(x, y, near[k])
            token_wait(c, i)
            ref = xall.at[c, part_of(i)]
            go(remote(ref, ref, x_send.at[k, i], tok_recv.at[c, i], x_peer, t))
            go(remote(ref, ref, y_send.at[k, i], tok_recv.at[c, i], y_peer, t))

    def cross_plane(k):
        c = chip(1 - x, y, near[k])
        token_wait(c, 0)
        ref = xall.at[c, part_of(0)]
        go(remote(ref, ref, yf_send.at[k], tok_recv.at[c, 0], y_peer, t))
        c = chip(x, 1 - y, near[k])
        token_wait(c, 1)
        ref = xall.at[c, part_of(1)]
        go(remote(ref, ref, xf_send.at[k], tok_recv.at[c, 1], x_peer, t))

    on_home(0, 0)
    on_home(1, 0)
    on_home(0, 1)
    spread_column(1)
    on_home(1, 1)
    cross_plane(0)
    on_land((0, 1))
    spread_column(2)
    cross_plane(1)
    on_land((2, 3))
    spread_column(3)
    on_land((4, 5))
    cross_plane(2)
    on_land((6, 7))
    cross_plane(3)

    for n in range(PLANE):

        @pl.when(home)
        def _():
            row = (1 - prompt) * PLANE + n
            ref = block_of(row)
            remote(ref, ref, own_sem, blk_recv.at[row], s, t).wait_recv()

    for row in range(2 * PLANE):

        @pl.when(jnp.logical_and(jnp.logical_not(home), jnp.logical_not(inner)))
        def _():
            ref = block_of(row)
            remote(ref, ref, own_sem, blk_recv.at[row], s, t).wait_recv()

    own.wait()
    for off in range(1, peers):
        c = (s + off) % peers
        remote(gall.at[c], gall.at[c], own_sem, g_recv.at[c], s, t).wait_recv()

    def slots_of(g):
        cx, cy = (x + g % 2) % 2, (y + g // 2) % 2
        return [chip(cx, cy, k) for k in range(DEEP)]

    def exchange(c):
        return remote(give.at[c], got.at[c], give_send.at[c], give_recv.at[c], s, 1 - t)

    def project(g):
        slots = slots_of(g)

        @pl.when(g % 2 == 1)
        def _():
            for c in slots:
                token_wait(c, 1)

        @pl.when(g // 2 == 1)
        def _():
            for c in slots:
                token_wait(c, 0)

        rows_in = jnp.concatenate([xall[c] for c in slots], axis=0)
        wide = jnp.dot(rows_in, wall[...], preferred_element_type=jnp.float32)
        for i, c in enumerate(slots):
            part_rows = slice(i * length, (i + 1) * length)
            keep[c] = wide[part_rows, : 2 * width]
            give[c] = wide[part_rows, 2 * width :]
        for c in slots:
            exchange(c).start()

    many = DEEP * length

    def local(g):
        slots = slots_of(g)
        for c in slots:
            exchange(c).wait_recv()
        wide = jnp.concatenate([keep[c] + got[c] for c in slots], axis=0)
        acted = silu(wide.astype(jnp.bfloat16).astype(jnp.float32))
        k = acted[:, :width]
        k = k * lax.rsqrt(jnp.sum(k * k, axis=-1, keepdims=True) + EPSILON)
        v = acted[:, width:]

        def row_of(kind):
            return jnp.concatenate([gall[c, kind : kind + 1, :] for c in slots], axis=1)

        beta_row = sigmoid(row_of(0) + offset[j])
        fade_row = row_of(2) - speed[j] * softplus(row_of(1))
        r = lax.broadcasted_iota(jnp.int32, (many, many), 0)
        c = lax.broadcasted_iota(jnp.int32, (many, many), 1)
        same = r // length == c // length
        strict = jnp.logical_and(same, r > c)
        eye = r == c

        def column(mask, row):
            return jnp.sum(jnp.where(mask, row, 0.0), axis=1, keepdims=True)

        sum_col = column(jnp.logical_and(same, r >= c), fade_row)
        all_col = column(same, fade_row)
        beta_col = column(eye, beta_row)
        sum_row = jnp.sum(jnp.where(eye, sum_col, 0.0), axis=0, keepdims=True)
        scaled = k * beta_col
        inner_products = dot3(halves(scaled), halves(k), NT)
        spread = jnp.exp(jnp.where(strict, sum_col - sum_row, 0.0))
        power = halves(jnp.where(strict, inner_products * spread, 0.0))
        solved = jnp.concatenate([scaled * jnp.exp(sum_col), v * beta_col], axis=1)
        solved = solved - dot3(power, halves(solved))
        reached = 2
        while reached < length:
            power = halves(dot3(power, power))
            solved = solved + dot3(power, halves(solved))
            reached *= 2
        tail = halves(k * jnp.exp(all_col - sum_col))
        solved = halves(solved)
        unit = (
            lax.broadcasted_iota(jnp.int32, (width, width), 0)
            == lax.broadcasted_iota(jnp.int32, (width, width), 1)
        ).astype(jnp.float32)
        last = jnp.exp(all_col)
        for i, slot in enumerate(slots):
            at = slice(i * length, (i + 1) * length)
            maps = dot3(
                tuple(a[at] for a in tail), tuple(a[at] for a in solved), TN
            )
            moves = last[i * length : i * length + 1] * unit - maps[:, :width]
            pair[slot, :, :width] = moves
            pair[slot, :, width:] = maps[:, width:]

    groups = peers // DEEP

    def stage(g, carry):
        @pl.when(g < groups)
        def _():
            project(g)

        @pl.when(g > 0)
        def _():
            local(g - 1)

        return carry

    lax.fori_loop(0, groups + 1, stage, 0)

    chains = []
    for g in range(groups):
        first = pair[g * DEEP]
        chain = [(first[:, :width], first[:, width:])]
        for i in range(1, DEEP):
            late = pair[g * DEEP + i]
            before = jnp.concatenate(chain[-1], axis=1)
            joined = dot3(halves(late[:, :width]), halves(before))
            chain.append((joined[:, :width], joined[:, width:] + late[:, width:]))
        chains.append(chain)
    carry = None
    found = {}
    for g in range(groups):
        move, shift = chains[g][-1]
        if carry is not None:
            move = halves(move)
            shift = dot3(move, carry[0]) + shift
        found[g * DEEP + DEEP - 1] = shift
        for i in range(DEEP - 1):
            found_shift = chains[g][i][1]
            if carry is not None:
                found_shift = dot3(halves(chains[g][i][0]), carry[0]) + found_shift
            found[g * DEEP + i] = found_shift
        carry = (halves(shift),)
    slot = slot_of(s)
    end = found[peers - 1].astype(jnp.bfloat16)
    final[slot] = end
    f_sent = [0]

    def pass_on(slot_at, to):
        n = f_sent[0]
        f_sent[0] += 1
        ref = final.at[slot_at]
        go(remote(ref, ref, f_send.at[n], f_recv.at[slot_at], to, t))

    def arrived(slot_at):
        ref = final.at[slot_at]
        remote(ref, ref, own_sem, f_recv.at[slot_at], s, t).wait_recv()

    def own_row_of(ref):
        two = ref[:, pl.ds(pl.multiple_of(j * width, 128), width)].astype(jnp.float32)
        return jnp.where(prompt == 0, two[0:1], two[1:2])

    q1 = silu(own_row_of(probe))
    k1 = silu(own_row_of(address))
    k1 = k1 * lax.rsqrt(jnp.sum(k1 * k1, axis=-1, keepdims=True) + EPSILON)
    v1 = silu(own_row_of(content))
    b1 = sigmoid(jnp.full((1, width), strength[prompt, j], jnp.float32))
    q_and_k = jnp.concatenate([q1, k1, jnp.zeros((6, width), jnp.float32)], axis=0)
    recalled = jnp.dot(
        q_and_k,
        end.astype(jnp.float32),
        precision=HIGHEST_ACCURACY,
        preferred_element_type=jnp.float32,
    )
    weight = b1 * jnp.sum(q1 * k1, axis=-1, keepdims=True)
    read = recalled[0:1] + weight * (v1 - recalled[1:2])
    normed = read * lax.rsqrt(jnp.mean(read * read, axis=-1, keepdims=True) + EPSILON)
    gated = normed * gain[...] * silu(own_row_of(outgate))
    rmsg[...] = jnp.broadcast_to(gated.astype(jnp.bfloat16).astype(jnp.float32), rmsg.shape)
    for off in range(1, peers):
        to = (s + off) % peers
        go(remote(rmsg, rall.at[slot], r_send.at[off], r_recv.at[slot], to, t))
    rall[slot] = rmsg[...]

    others = [near[k] for k in range(1, DEEP)]
    for cz in others:
        pass_on(slot, chip(x, y, cz))
    pass_on(slot, y_peer)
    pass_on(slot, x_peer)
    for n in range(peers):
        states[n] = found[n].astype(jnp.bfloat16)
    for off in range(1, peers):
        to = (s + off) % peers
        go(remote(states.at[to], bound.at[slot], b_send.at[off], b_recv.at[slot], to, t))
    bound[slot] = states[s]
    for cz in others:
        come = slot_of(chip(x, y, cz))
        arrived(come)
        pass_on(come, y_peer)
        pass_on(come, x_peer)
    for cz in near:
        come = slot_of(chip(x, 1 - y, cz))
        arrived(come)
        pass_on(come, x_peer)

    for off in range(1, peers):
        come = slot_of((s + off) % peers)
        remote(rall.at[come], rall.at[come], own_sem, r_recv.at[come], s, t).wait_recv()
    lines = [
        jnp.concatenate([rall[p * heads + h, 0:1, :] for h in range(heads)], axis=1)
        for p in range(2)
    ]
    lines.append(jnp.zeros((6, heads * width), jnp.float32))
    heads_read = jnp.concatenate(lines, axis=0).astype(jnp.bfloat16)
    loads[4].wait()
    terms = jnp.dot(heads_read, rv[...], preferred_element_type=jnp.float32)
    part[...] = terms.astype(jnp.bfloat16).astype(jnp.float32)
    swap = remote(part, partgot, t_send, t_recv, s, 1 - t)
    swap.start()
    swap.wait()
    mixed[...] = (part[...] + partgot[...])[:2].astype(mixed.dtype)

    for cz in range(DEEP):
        for cy in range(2):
            arrived(slot_of(chip(1 - x, cy, cz)))
    for off in range(1, peers):
        come = slot_of((s + off) % peers)
        ref = bound.at[come]
        remote(ref, ref, own_sem, b_recv.at[come], s, t).wait_recv()

    for copy in sent:
        copy.wait_send()

    @pl.when(home)
    def _():
        for q in range(PLANE):
            row = prompt * PLANE + q
            ref = block_of(row)
            remote(wcross.at[q], ref, cross_send.at[q], blk_recv.at[row], s, t).wait_send()
            remote(ref, ref, relay_send.at[q], blk_recv.at[row], s, t).wait_send()

    @pl.when(lands)
    def _():
        for n in range(2 * PLANE):
            ref = block_of(arrival_row(n))
            remote(ref, ref, outer_send.at[n], own_sem, s, t).wait_send()

    @pl.when(jnp.logical_not(home))
    def _():
        for cross in (1, 0):
            for kv in range(2):
                weight_copies(0, 0, cross, kv)[3].wait_send()

    def give_done(c, carry):
        exchange(c).wait_send()
        return carry

    lax.fori_loop(0, peers, give_done, 0)


def prefill(tok, wk, wv, gate_b, gate_a, add, offset, speed, first, strength, gain, readout, peers):
    _, length, model_width = tok.shape
    heads = add.shape[1]
    rows = wk.shape[0]
    width = ADDRESS_WIDTH
    half = model_width // 2
    dma = pltpu.SemaphoreType.DMA
    anywhere = pl.BlockSpec(memory_space=pl.ANY)
    vmem = pl.BlockSpec(memory_space=pltpu.VMEM)
    smem = pl.BlockSpec(memory_space=pltpu.SMEM)
    f32, bf16 = jnp.float32, jnp.bfloat16
    return pl.pallas_call(
        lambda *refs: prefill_kernel(peers, *refs),
        out_shape=(
            jax.ShapeDtypeStruct((peers, width, width), bf16),
            jax.ShapeDtypeStruct((peers, width, width), bf16),
            jax.ShapeDtypeStruct((2, readout.shape[1]), bf16),
        ),
        in_specs=[anywhere] * 6 + [smem] * 2 + [vmem] * 4 + [smem, vmem, anywhere],
        out_specs=(vmem, vmem, vmem),
        scratch_shapes=[
            pltpu.VMEM((peers, length, half), bf16),
            pltpu.VMEM((half, 4 * width), bf16),
            pltpu.VMEM((PLANE, rows, 4 * width), bf16),
            pltpu.VMEM(tok.shape, bf16),
            pltpu.VMEM((2,) + gate_b.shape, bf16),
            pltpu.VMEM(add.shape, f32),
            pltpu.VMEM((2, 2, gate_b.shape[0], length), f32),
            pltpu.VMEM((2, heads, 8, length), f32),
            pltpu.VMEM((peers, 8, length), f32),
            pltpu.VMEM((peers, length, 2 * width), f32),
            pltpu.VMEM((peers, length, 2 * width), f32),
            pltpu.VMEM((peers, length, 2 * width), f32),
            pltpu.VMEM((peers, width, 2 * width), f32),
            pltpu.VMEM((peers, width, width), bf16),
            pltpu.VMEM(readout.shape, bf16),
            pltpu.VMEM((8, width), f32),
            pltpu.VMEM((peers, 8, width), f32),
            pltpu.VMEM((8, readout.shape[1]), f32),
            pltpu.VMEM((8, readout.shape[1]), f32),
            dma((5,)),
            dma(()),
            dma((DEEP, PIECES)),
            dma((peers, PIECES)),
            dma((DEEP, PIECES)),
            dma((DEEP, PIECES)),
            dma((DEEP,)),
            dma((DEEP,)),
            dma((4, 4)),
            dma((2 * PLANE, 4)),
            dma((PLANE, 4)),
            dma((PLANE,)),
            dma((PLANE,)),
            dma((2 * PLANE,)),
            dma((2 * PLANE,)),
            dma((peers,)),
            dma((peers,)),
            dma((peers,)),
            dma((peers,)),
            dma((peers,)),
            dma((peers,)),
            dma((peers,)),
            dma((peers,)),
            dma((peers,)),
            dma((peers,)),
            dma(()),
            dma(()),
        ],
        compiler_params=pltpu.CompilerParams(has_side_effects=True),
        name="prefill",
    )(tok, wk, wv, gate_b, gate_a, add, offset, speed, *first, strength, gain, readout)


def per_device_heads(
    layer_source_tokens,
    address_projection,
    content_projection,
    strength_projection,
    fading_driver_projection,
    strength_offset,
    channel_fading_speed,
    added_fading_exponent,
    first_step_probe,
    first_step_address,
    first_step_content,
    first_step_outgate,
    first_step_strength_raw,
    channel_scaling_factor,
    readout_projection,
):
    peers = lax.axis_size("sp")
    head_local = channel_fading_speed.shape[0]
    width = ADDRESS_WIDTH
    final, bound, mixed = prefill(
        layer_source_tokens,
        address_projection,
        content_projection,
        strength_projection.T,
        fading_driver_projection.T,
        jnp.swapaxes(added_fading_exponent, 1, 2),
        strength_offset,
        channel_fading_speed,
        (first_step_probe, first_step_address, first_step_content, first_step_outgate),
        first_step_strength_raw,
        channel_scaling_factor.reshape(1, width),
        readout_projection,
        peers,
    )
    state_cache = final.reshape(2, head_local, width, width)
    boundary_cache = bound.reshape(2, 1, head_local, width, width)
    return (state_cache, mixed, boundary_cache)


def by_heads(mesh):
    def choose_form(*args):
        seq_count, length, model_width = args[0].shape
        peers, heads = lax.axis_size("sp"), args[6].shape[0]
        fits = (
            lax.axis_size("tp") == 2
            and seq_count == 2
            and peers == DEEP * PLANE
            and heads == 2 * PLANE
            and length == BLOCK
            and args[1].shape[0] * peers == model_width
        )
        return per_device_heads(*args) if fits else per_device(*args)

    return choose_form


def solution(mesh):
    return jax.shard_map(
        by_heads(mesh),
        mesh=mesh,
        in_specs=(
            P(None, "sp", None),
            P("sp", "tp"),
            P("sp", "tp"),
            P(),
            P(),
            P("tp"),
            P("tp"),
            P(None, "sp", "tp"),
            P(None, "tp"),
            P(None, "tp"),
            P(None, "tp"),
            P(None, "tp"),
            P(None, "tp"),
            P(),
            P("tp", "sp"),
        ),
        out_specs=(P(None, "tp", None, None), P(None, "sp"), P(None, "sp", "tp", None, None)),
        check_vma=False,
    )
```

```python
import jax
import jax.numpy as jnp
from jax import lax
from jax.experimental import pallas as pl
from jax.experimental.pallas import tpu as pltpu
from jax.sharding import PartitionSpec as P

ADDRESS_WIDTH = 128
BLOCK = 64


EPSILON = 1e-06
HIGHEST_ACCURACY = lax.Precision.HIGHEST


def prefix(array, axis, combine, identity):
    peers, index = (lax.axis_size(axis), lax.axis_index(axis))
    everything = jax.tree.map(
        lambda part, kind: lax.all_gather(part.astype(kind), axis),
        array,
        (jnp.bfloat16, jnp.bfloat16),
    )
    start = jax.tree.map(
        lambda part, zero: jnp.broadcast_to(jnp.asarray(zero, part.dtype), part.shape),
        array,
        identity,
    )

    def step(k, before):
        reached = k < index
        new = combine(
            before, jax.tree.map(lambda part, own: part[k].astype(own.dtype), everything, array)
        )
        return jax.tree.map(lambda a, b: jnp.where(reached, a, b), new, before)

    return lax.fori_loop(0, peers, step, start)


def as_sent(array):
    return jax.tree.map(lambda a: a.astype(jnp.bfloat16) if a.dtype == jnp.float32 else a, array)


def broadcast(value, axis, source):
    kept = jnp.where(lax.axis_index(axis) == source, value, 0).astype(value.dtype)
    return lax.psum(kept, axis)


def unit_inverse(lower_part):
    matrix_order = lower_part.shape[-1]
    identity = jnp.eye(matrix_order, dtype=jnp.float32)
    result = identity - lower_part
    power_term = lower_part
    reached = 2
    while reached < matrix_order:
        power_term = jnp.matmul(power_term, power_term, precision=HIGHEST_ACCURACY)
        result = jnp.matmul(result, identity + power_term, precision=HIGHEST_ACCURACY)
        reached = reached * 2
    return result


def build_arguments(
    address_vectors,
    content_vectors,
    outgate_raw_scores,
    strength_offset,
    channel_fading_speed,
    added_fading_exponent,
    channel_width,
):
    length = address_vectors.shape[0]
    attention_channels_total = channel_fading_speed.shape[0]
    address_token_slab = jax.nn.silu(address_vectors.astype(jnp.float32)).reshape(
        length, attention_channels_total, channel_width
    )
    address_token_slab = address_token_slab * lax.rsqrt(
        jnp.sum(address_token_slab * address_token_slab, axis=-1, keepdims=True) + EPSILON
    )
    content_token_slab = jax.nn.silu(content_vectors.astype(jnp.float32)).reshape(
        length, attention_channels_total, channel_width
    )
    strength_raw_expanded = outgate_raw_scores.astype(jnp.float32)
    storing_strength = jax.nn.sigmoid(
        strength_raw_expanded[:, :attention_channels_total] + strength_offset
    )
    fading_exponent = added_fading_exponent - channel_fading_speed * jax.nn.softplus(
        strength_raw_expanded[:, attention_channels_total:]
    )
    return (address_token_slab, content_token_slab, storing_strength, fading_exponent)


def range_map(address_token_slab, content_token_slab, storing_strength, fading_exponent, block):
    length, attention_channels_total, channel_width = address_token_slab.shape
    blocks = length // block

    def split_blocks(tensor):
        moved_axes = jnp.swapaxes(tensor, 0, 1)
        return moved_axes.reshape((attention_channels_total, blocks, block) + moved_axes.shape[2:])

    block_keys = split_blocks(address_token_slab)
    block_values = split_blocks(content_token_slab)
    block_beta = split_blocks(storing_strength)
    cumulative = jnp.cumsum(split_blocks(fading_exponent), axis=-1)
    positions = jnp.arange(block)
    strict = positions[:, None] > positions[None, :]
    spread_log = jnp.where(strict, cumulative[..., :, None] - cumulative[..., None, :], 0.0)
    scaled_keys = block_keys * block_beta[..., None]
    inner_prod = jnp.einsum("hnik,hnjk->hnij", scaled_keys, block_keys, precision=HIGHEST_ACCURACY)
    lower_part = jnp.where(strict, inner_prod * jnp.exp(spread_log), 0.0)
    inverse = unit_inverse(lower_part)
    targets = jnp.concatenate(
        [block_values * block_beta[..., None], scaled_keys * jnp.exp(cumulative)[..., None]],
        axis=-1,
    )
    solved = jnp.einsum("hnij,hnjk->hnik", inverse, targets, precision=HIGHEST_ACCURACY)
    updates = solved[..., :channel_width]
    key_weights = solved[..., channel_width:]
    tail_keys = block_keys * jnp.exp(cumulative[..., -1:] - cumulative)[..., None]
    last_decay = jnp.exp(cumulative[..., -1])
    identity = jnp.eye(channel_width, dtype=jnp.float32)

    def advance(state_pair, block_items):
        transition, carried_state = state_pair
        update_index, weight_index, tail_index, last_index = block_items
        fresh_value_rows = update_index - jnp.einsum(
            "xbg,xgp->xbp", weight_index, carried_state, precision=HIGHEST_ACCURACY
        )
        carried_state = carried_state * last_index[:, None, None] + jnp.einsum(
            "tjo,tjw->tow", tail_index, fresh_value_rows, precision=HIGHEST_ACCURACY
        )
        block_move = last_index[:, None, None] * identity - jnp.einsum(
            "hck,hcj->hkj", tail_index, weight_index, precision=HIGHEST_ACCURACY
        )
        transition = jnp.einsum("hij,hjk->hik", block_move, transition, precision=HIGHEST_ACCURACY)
        return ((transition, carried_state), None)

    initial = (
        jnp.broadcast_to(identity, (attention_channels_total, channel_width, channel_width)),
        jnp.zeros((attention_channels_total, channel_width, channel_width), jnp.float32),
    )
    block_items = (
        jnp.moveaxis(updates, 1, 0),
        jnp.moveaxis(key_weights, 1, 0),
        jnp.moveaxis(tail_keys, 1, 0),
        jnp.moveaxis(last_decay, 1, 0),
    )
    (transition, carried_state), _ = lax.scan(advance, initial, block_items)
    return (transition, carried_state)


def read_heads(
    state_cache,
    first_step_probe,
    first_step_address,
    first_step_content,
    first_step_outgate,
    first_step_strength_raw,
    channel_scaling_factor,
):
    seq_count, attention_channels_total, channel_width, _ = state_cache.shape
    carried_state = state_cache.astype(jnp.float32)

    def activate(tensor):
        return jax.nn.silu(tensor.astype(jnp.float32)).reshape(
            seq_count, attention_channels_total, channel_width
        )

    query_rows = activate(first_step_probe)
    address_token_slab = activate(first_step_address)
    address_token_slab = address_token_slab * lax.rsqrt(
        jnp.sum(address_token_slab * address_token_slab, axis=-1, keepdims=True) + EPSILON
    )
    content_token_slab = activate(first_step_content)
    storing_strength = jax.nn.sigmoid(first_step_strength_raw)
    recalled = jnp.einsum(
        "nhk,nhkv->nhv", address_token_slab, carried_state, precision=HIGHEST_ACCURACY
    )
    updated = (
        carried_state
        + storing_strength[..., None, None]
        * address_token_slab[..., :, None]
        * (content_token_slab - recalled)[..., None, :]
    )
    output = jnp.einsum("nhk,nhkv->nhv", query_rows, updated, precision=HIGHEST_ACCURACY)
    normed = (
        output
        * lax.rsqrt(jnp.mean(output * output, axis=-1, keepdims=True) + EPSILON)
        * channel_scaling_factor
    )
    gated_out = normed * activate(first_step_outgate)
    return gated_out.reshape(seq_count, attention_channels_total * channel_width).astype(
        jnp.bfloat16
    )


def matmul_maps(left, right):
    return jnp.einsum("shij,shjk->shik", left, right, precision=HIGHEST_ACCURACY)


def join_pairs(earlier, later):
    return (matmul_maps(later[0], earlier[0]), matmul_maps(later[0], earlier[1]) + later[1])


def per_device(
    layer_source_tokens,
    address_projection,
    content_projection,
    strength_projection,
    fading_driver_projection,
    strength_offset,
    channel_fading_speed,
    added_fading_exponent,
    first_step_probe,
    first_step_address,
    first_step_content,
    first_step_outgate,
    first_step_strength_raw,
    channel_scaling_factor,
    readout_projection,
):
    head_local = channel_fading_speed.shape[0]
    first_head = lax.axis_index("tp") * head_local
    beta_slice = lax.dynamic_slice_in_dim(strength_projection, first_head, head_local, 1)
    alpha_slice = lax.dynamic_slice_in_dim(fading_driver_projection, first_head, head_local, 1)
    seq_count, local_len, model_width = layer_source_tokens.shape
    flat_rows = layer_source_tokens.reshape(seq_count * local_len, model_width)
    key_sum = jnp.dot(
        flat_rows,
        lax.all_gather(address_projection, "sp", axis=0, tiled=True),
        preferred_element_type=jnp.float32,
    )
    value_sum = jnp.dot(
        flat_rows,
        lax.all_gather(content_projection, "sp", axis=0, tiled=True),
        preferred_element_type=jnp.float32,
    )
    beta_sum = jnp.dot(flat_rows, beta_slice, preferred_element_type=jnp.float32)
    alpha_sum = jnp.dot(flat_rows, alpha_slice, preferred_element_type=jnp.float32)
    outgate_raw_scores = (
        jnp.concatenate([beta_sum, alpha_sum], axis=1)
        .astype(jnp.bfloat16)
        .reshape(seq_count, local_len, -1)
    )
    address_vectors = key_sum.astype(jnp.bfloat16).reshape(seq_count, local_len, -1)
    content_vectors = value_sum.astype(jnp.bfloat16).reshape(seq_count, local_len, -1)
    transitions = []
    offsets = []
    for prompt_number in range(seq_count):
        address_token_slab, content_token_slab, storing_strength, fading_exponent = build_arguments(
            address_vectors[prompt_number],
            content_vectors[prompt_number],
            outgate_raw_scores[prompt_number],
            strength_offset,
            channel_fading_speed,
            added_fading_exponent[prompt_number],
            ADDRESS_WIDTH,
        )
        transition, carried_state = range_map(
            address_token_slab, content_token_slab, storing_strength, fading_exponent, BLOCK
        )
        transitions.append(transition)
        offsets.append(carried_state)
    transition = jnp.stack(transitions)
    offset = jnp.stack(offsets)
    identity = jnp.broadcast_to(jnp.eye(ADDRESS_WIDTH, dtype=jnp.float32), transition.shape)
    entered = prefix((transition, offset), "sp", join_pairs, (identity, jnp.zeros_like(offset)))
    leaving = matmul_maps(transition, entered[1]) + offset
    final = broadcast(as_sent(leaving), "sp", lax.axis_size("sp") - 1).astype(leaving.dtype)
    boundary_cache = leaving.astype(jnp.bfloat16)[:, None]
    state_cache = final.astype(jnp.bfloat16)
    heads_read = read_heads(
        state_cache,
        first_step_probe,
        first_step_address,
        first_step_content,
        first_step_outgate,
        first_step_strength_raw,
        channel_scaling_factor,
    )
    group_terms = jnp.dot(
        heads_read, readout_projection, preferred_element_type=jnp.float32
    ).astype(jnp.bfloat16)
    mixed_read = lax.psum(group_terms.astype(jnp.float32).astype(jnp.bfloat16), "tp")
    return (state_cache, mixed_read, boundary_cache)


MESH = pl.DeviceIdType.MESH
PIECES = 2
DEEP = 4
PLANE = 4


def remote(src, dst, send, recv, sp, tp):
    return pltpu.make_async_remote_copy(
        src_ref=src,
        dst_ref=dst,
        send_sem=send,
        recv_sem=recv,
        device_id={"sp": sp, "tp": tp},
        device_id_type=MESH,
    )


def silu(v):
    return v / (1.0 + jnp.exp(-v))


def sigmoid(v):
    return 1.0 / (1.0 + jnp.exp(-v))


def softplus(v):
    return jnp.maximum(v, 0.0) + jnp.log1p(jnp.exp(-jnp.abs(v)))


def halves(a):
    high = a.astype(jnp.bfloat16)
    return high, (a - high.astype(jnp.float32)).astype(jnp.bfloat16)


NN = (((1,), (0,)), ((), ()))
NT = (((1,), (1,)), ((), ()))
TN = (((0,), (0,)), ((), ()))


def dot3(a, b, dims=NN):
    def one(p, q):
        return lax.dot_general(p, q, dims, preferred_element_type=jnp.float32)

    (ah, al), (bh, bl) = a, b
    return one(ah, bh) + (one(ah, bl) + one(al, bh))


def prefill_kernel(
    peers,
    tok,
    wk,
    wv,
    gate_b,
    gate_a,
    add,
    offset,
    speed,
    probe,
    address,
    content,
    outgate,
    strength,
    gain,
    readout,
    final,
    bound,
    mixed,
    xall,
    wall,
    wcross,
    tokv,
    gatev,
    addv,
    logit,
    msg,
    gz,
    gall,
    keep,
    give,
    got,
    pair,
    states,
    rv,
    rmsg,
    rall,
    part,
    partgot,
    load,
    own_sem,
    z_send,
    tok_recv,
    x_send,
    y_send,
    xf_send,
    yf_send,
    w_send,
    w_recv,
    c_recv,
    relay_send,
    cross_send,
    blk_recv,
    gz_send,
    gz_recv,
    g_send,
    g_recv,
    give_send,
    give_recv,
    f_send,
    f_recv,
    b_send,
    b_recv,
    r_send,
    r_recv,
    t_send,
    t_recv,
):
    s, t = lax.axis_index("sp"), lax.axis_index("tp")
    heads = add.shape[1]
    width = ADDRESS_WIDTH
    length = tok.shape[1]
    half = tok.shape[2] // 2
    rows = wk.shape[0]
    piece = length // PIECES
    x, y, z = s % 2, (s // 2) % 2, s // PLANE
    prompt, side = z % 2, z // 2
    j = side * PLANE + s % PLANE
    mate = z + 1 - 2 * prompt
    columns = pl.ds(pl.multiple_of(t * half, 128), half)

    def chip(cx, cy, cz):
        return PLANE * cz + 2 * cy + cx

    def slot_of(c):
        return (c // PLANE % 2) * heads + (c // PLANE // 2) * PLANE + c % PLANE

    x_peer, y_peer, z_peer = chip(1 - x, y, z), chip(x, 1 - y, z), chip(x, y, mate)
    diagonal = chip(1 - x, 1 - y, z)
    home = t == side

    def part_of(i):
        return pl.ds(i * piece, piece)

    sent = []

    def go(copy):
        copy.start()
        sent.append(copy)

    def token_wait(c, i):
        ref = xall.at[c, part_of(i)]
        remote(ref, ref, own_sem, tok_recv.at[c, i], s, t).wait_recv()

    near = [z, mate, DEEP - 1 - z, (z + DEEP // 2) % DEEP]
    barrier = pltpu.get_barrier_semaphore()
    partners = [(chip(x, y, near[k]), t) for k in range(1, DEEP)] + [(s, 1 - t)]
    partners += [(c, core) for c in (x_peer, y_peer, diagonal) for core in (t, 1 - t)]
    for c, core in partners:
        pl.semaphore_signal(
            barrier, inc=1, device_id={"sp": c, "tp": core}, device_id_type=MESH
        )
    loads = []
    for i, (src, dst) in enumerate(
        (
            (tok, tokv),
            (gate_b, gatev.at[0]),
            (gate_a, gatev.at[1]),
            (add, addv),
            (readout, rv),
        )
    ):
        copy = pltpu.make_async_copy(src, dst, load.at[i])
        copy.start()
        loads.append(copy)
    own = pltpu.make_async_copy(tok.at[prompt, :, columns], xall.at[s], own_sem)
    own.start()
    pl.semaphore_wait(barrier, len(partners))

    def along_z(k, source):
        for i in range(PIECES):
            go(
                remote(
                    source.at[near[k] % 2, part_of(i), columns],
                    xall.at[s, part_of(i)],
                    z_send.at[k, i],
                    tok_recv.at[s, i],
                    chip(x, y, near[k]),
                    t,
                )
            )

    along_z(1, tok)
    along_z(2, tok)

    side_of = (t + side) % 2
    own_row = s % (peers // 2)
    q_own = s % PLANE
    spot = pl.ds(pl.multiple_of(own_row * rows, 16), rows)

    def weight_copies(dx, dy, cross, kv):
        xd, yd = (x + dx) % 2, (y + dy) % 2
        head = ((side + cross) % 2) * PLANE + 2 * yd + xd
        src = (wk, wv)[kv].at[:, pl.ds(pl.multiple_of(head * width, 128), width)]
        at = pl.ds(pl.multiple_of((2 * side_of + kv) * width, 128), width)
        if cross:
            dst, sem = wcross.at[q_own, :, at], c_recv.at[q_own, 2 * side_of + kv]
        else:
            dst, sem = wall.at[spot, at], w_recv.at[own_row, 2 * side_of + kv]
        out = w_send.at[2 * dy + dx, 2 * cross + kv]
        return src, dst, sem, remote(src, dst, out, sem, chip(xd, yd, z), side)

    for dx, dy in ((0, 0), (1, 0), (0, 1), (1, 1)):
        for cross in (1, 0):
            for kv in range(2):
                src, dst, sem, copy = weight_copies(dx, dy, cross, kv)
                if dx + dy == 0:

                    @pl.when(home)
                    def _():
                        pltpu.make_async_copy(src, dst, sem).start()

                    @pl.when(jnp.logical_not(home))
                    def _():
                        copy.start()
                else:
                    go(copy)

    for i in range(PIECES):
        src = tok.at[prompt, part_of(i), columns]
        dst = xall.at[s, part_of(i)]
        go(remote(src, dst, x_send.at[0, i], tok_recv.at[s, i], x_peer, t))
        go(remote(src, dst, y_send.at[0, i], tok_recv.at[s, i], y_peer, t))

    def gates():
        for copy in loads[:4]:
            copy.wait()
        msg[...] = jnp.zeros_like(msg)
        for p in range(2):
            for kind in range(2):
                logit[p, kind] = (
                    lax.dot_general(gatev[kind], tokv[p], NT, preferred_element_type=jnp.float32)
                    .astype(jnp.bfloat16)
                    .astype(jnp.float32)
                )
            for h in range(heads):
                for kind in range(2):
                    msg[p, h, kind : kind + 1, :] = logit[p, kind, pl.ds(t * heads + h, 1), :]
                msg[p, h, 2:3, :] = addv[p, h : h + 1, :]
        for k in range(1, DEEP):
            src = msg.at[near[k] % 2, pl.ds(near[k] // 2 * PLANE, PLANE)]
            go(remote(src, gz.at[z], gz_send.at[k], gz_recv.at[z], chip(x, y, near[k]), t))
        for n, c in enumerate((x_peer, y_peer, diagonal)):
            src = msg.at[prompt, side * PLANE + c % PLANE]
            go(remote(src, gall.at[s], g_send.at[0, n], g_recv.at[s], c, t))
        gall[s] = msg[prompt, j]

    def pass_gates(k):
        cz = near[k]
        remote(gz.at[cz], gz.at[cz], own_sem, gz_recv.at[cz], s, t).wait_recv()
        c = chip(x, y, cz)
        for n, to in enumerate((x_peer, y_peer, diagonal)):
            go(remote(gz.at[cz, to % PLANE], gall.at[c], g_send.at[k, n], g_recv.at[c], to, t))
        gall[c] = gz[cz, q_own]

    def block_of(row):
        return wall.at[pl.ds(pl.multiple_of(row * rows, 16), rows)]

    def row_at(n):
        q = 2 * ((y + n // 2) % 2) + (x + n % 2) % 2
        return q, prompt * PLANE + q

    def home_relay(n):
        q, row = row_at(n)
        block = block_of(row)
        landing = chip(x, y, (z + DEEP // 2) % DEEP)
        for c in range(4):
            one = wcross.at[q, :, pl.ds(c * width, width)]
            pltpu.make_async_copy(one, one, c_recv.at[q, c]).wait()
        remote(wcross.at[q], block, cross_send.at[q], blk_recv.at[row], landing, t).start()
        for c in range(4):
            one = block.at[:, pl.ds(c * width, width)]
            pltpu.make_async_copy(one, one, w_recv.at[row, c]).wait()
        remote(block, block, relay_send.at[q], blk_recv.at[row], z_peer, t).start()

    def land_relay(n):
        q, row = row_at(n)
        ref = block_of(row)
        remote(ref, ref, relay_send.at[q], blk_recv.at[row], s, t).wait_recv()
        remote(ref, ref, relay_send.at[q], blk_recv.at[row], z_peer, t).start()

    def on_home(*ns):
        @pl.when(home)
        def _():
            for n in ns:
                home_relay(n)

    def on_land(*ns):
        @pl.when(jnp.logical_not(home))
        def _():
            for n in ns:
                land_relay(n)

    def spread_column(k):
        for i in range(PIECES):
            c = chip(x, y, near[k])
            token_wait(c, i)
            ref = xall.at[c, part_of(i)]
            go(remote(ref, ref, x_send.at[k, i], tok_recv.at[c, i], x_peer, t))
            go(remote(ref, ref, y_send.at[k, i], tok_recv.at[c, i], y_peer, t))

    def cross_plane(k):
        c = chip(1 - x, y, near[k])
        token_wait(c, 0)
        ref = xall.at[c, part_of(0)]
        go(remote(ref, ref, yf_send.at[k], tok_recv.at[c, 0], y_peer, t))
        c = chip(x, 1 - y, near[k])
        token_wait(c, 1)
        ref = xall.at[c, part_of(1)]
        go(remote(ref, ref, xf_send.at[k], tok_recv.at[c, 1], x_peer, t))

    on_home(0)
    gates()
    on_home(1, 2)
    on_land(0)
    spread_column(1)
    along_z(3, tokv)
    on_home(3)
    on_land(1)
    cross_plane(0)
    pass_gates(1)
    on_land(2)
    spread_column(2)
    on_land(3)
    cross_plane(1)
    pass_gates(2)
    spread_column(3)
    pass_gates(3)
    cross_plane(2)
    cross_plane(3)

    for n in range(PLANE):
        row = (1 - prompt) * PLANE + n
        ref = block_of(row)
        remote(ref, ref, own_sem, blk_recv.at[row], s, t).wait_recv()

    own.wait()
    for off in range(1, PLANE):
        for cz in near:
            c = PLANE * cz + (s + off) % PLANE
            remote(gall.at[c], gall.at[c], own_sem, g_recv.at[c], s, t).wait_recv()

    def plane_of(g):
        value = near[0]
        for k in range(1, DEEP):
            value = jnp.where(g == k, near[k], value)
        return value

    def slots_of(g):
        return [PLANE * plane_of(g) + q for q in range(PLANE)]

    def exchange(c):
        return remote(give.at[c], got.at[c], give_send.at[c], give_recv.at[c], s, 1 - t)

    def project(g):
        slots = slots_of(g)

        cz = plane_of(g)
        token_wait(chip(1 - x, y, cz), 1)
        token_wait(chip(x, 1 - y, cz), 0)
        token_wait(chip(1 - x, 1 - y, cz), 0)
        token_wait(chip(1 - x, 1 - y, cz), 1)
        rows_in = jnp.concatenate([xall[c] for c in slots], axis=0)
        wide = jnp.dot(rows_in, wall[...], preferred_element_type=jnp.float32)
        for i, c in enumerate(slots):
            part_rows = slice(i * length, (i + 1) * length)
            keep[c] = wide[part_rows, : 2 * width]
            give[c] = wide[part_rows, 2 * width :]
        for c in slots:
            exchange(c).start()

    many = PLANE * length

    def left_form(full):
        two = full[:, : many // 2] + full[:, many // 2 :]
        high, low = halves(two + pltpu.roll(two, length, 1))
        return jnp.concatenate([high, low], axis=1)

    def right_form(full):
        blocks = [full[i * length : (i + 1) * length] for i in range(PLANE)]
        high, low = halves((blocks[0] + blocks[1]) + (blocks[2] + blocks[3]))
        return jnp.concatenate([high, low, high, low], axis=0)

    def one_dot(a, b, dims=NN):
        return lax.dot_general(a, b, dims, preferred_element_type=jnp.float32)

    def maps_of(wide, bare_beta, bare_decay, added_decay):
        acted = silu(wide.astype(jnp.bfloat16).astype(jnp.float32))
        k = acted[:, :width]
        k = k * lax.rsqrt(jnp.sum(k * k, axis=-1, keepdims=True) + EPSILON)
        v = acted[:, width:]
        beta_row = sigmoid(bare_beta + offset[j])
        fade_row = added_decay - speed[j] * softplus(bare_decay)
        r = lax.broadcasted_iota(jnp.int32, (many, many), 0)
        c = lax.broadcasted_iota(jnp.int32, (many, many), 1)
        same = r // length == c // length
        strict = jnp.logical_and(same, r > c)
        eye = r == c

        def column(mask, row):
            return jnp.sum(jnp.where(mask, row, 0.0), axis=1, keepdims=True)

        def kept(full):
            return jnp.where(same, full, 0.0)

        sum_col = column(jnp.logical_and(same, r >= c), fade_row)
        all_col = column(same, fade_row)
        beta_col = column(eye, beta_row)
        sum_row = jnp.sum(jnp.where(eye, sum_col, 0.0), axis=0, keepdims=True)
        scaled = k * beta_col
        inner_products = dot3(halves(scaled), halves(k), NT)
        spread = jnp.exp(jnp.where(strict, sum_col - sum_row, 0.0))
        lower = jnp.where(strict, inner_products * spread, 0.0)
        left, right = left_form(lower), right_form(lower)
        inverse = jnp.where(eye, 1.0, 0.0) - lower
        reached = 2
        while reached < length:
            power = kept(one_dot(left, right))
            right = right_form(power)
            inverse = inverse + kept(one_dot(left_form(inverse), right))
            reached *= 2
            if reached < length:
                left = left_form(power)
        inverse = left_form(inverse)
        targets = halves(jnp.concatenate([scaled * jnp.exp(sum_col), v * beta_col], axis=1))
        tail = halves(k * jnp.exp(all_col - sum_col))
        last = jnp.exp(all_col)
        unit = (
            lax.broadcasted_iota(jnp.int32, (width, width), 0)
            == lax.broadcasted_iota(jnp.int32, (width, width), 1)
        ).astype(jnp.float32)
        pairs = []
        for i in range(PLANE):
            at = slice(i * length, (i + 1) * length)
            high, low = targets[0][at], targets[1][at]
            solved = one_dot(inverse[at], jnp.concatenate([high, low, high, low], axis=0))
            high, low = halves(solved)
            keys = jnp.concatenate([tail[0][at]] * 2 + [tail[1][at]] * 2, axis=0)
            maps = one_dot(keys, jnp.concatenate([high, low, high, low], axis=0), TN)
            moves = last[i * length : i * length + 1] * unit - maps[:, :width]
            pairs.append((moves, maps[:, width:]))
        return pairs

    def local(n):
        slots = [slots_of(2 * n + i) for i in range(2)]
        for group in slots:
            for c in group:
                exchange(c).wait_recv()
        given = []
        for group in slots:

            def row_of(kind, group=group):
                return jnp.concatenate([gall[c, kind : kind + 1, :] for c in group], axis=1)

            wide = jnp.concatenate([keep[c] + got[c] for c in group], axis=0)
            given.append((wide, row_of(0), row_of(1), row_of(2)))
        found = [maps_of(*g) for g in given]
        for group, pairs in zip(slots, found):
            for slot, (moves, shift) in zip(group, pairs):
                pair[slot, :, :width] = moves
                pair[slot, :, width:] = shift

    groups = peers // PLANE
    lax.fori_loop(0, groups, lambda g, carry: (project(g), carry)[1], 0)
    lax.fori_loop(0, groups // 2, lambda n, carry: (local(n), carry)[1], 0)

    chains = []
    for g in range(groups):
        first = pair[g * DEEP]
        chain = [(first[:, :width], first[:, width:])]
        for i in range(1, DEEP):
            late = pair[g * DEEP + i]
            before = jnp.concatenate(chain[-1], axis=1)
            joined = dot3(halves(late[:, :width]), halves(before))
            chain.append((joined[:, :width], joined[:, width:] + late[:, width:]))
        chains.append(chain)
    carry = None
    found = {}
    for g in range(groups):
        move, shift = chains[g][-1]
        if carry is not None:
            move = halves(move)
            shift = dot3(move, carry[0]) + shift
        found[g * DEEP + DEEP - 1] = shift
        for i in range(DEEP - 1):
            found_shift = chains[g][i][1]
            if carry is not None:
                found_shift = dot3(halves(chains[g][i][0]), carry[0]) + found_shift
            found[g * DEEP + i] = found_shift
        carry = (halves(shift),)
    slot = slot_of(s)
    end = found[peers - 1].astype(jnp.bfloat16)
    final[slot] = end
    f_sent = [0]

    def pass_on(slot_at, to):
        n = f_sent[0]
        f_sent[0] += 1
        ref = final.at[slot_at]
        go(remote(ref, ref, f_send.at[n], f_recv.at[slot_at], to, t))

    def arrived(slot_at):
        ref = final.at[slot_at]
        remote(ref, ref, own_sem, f_recv.at[slot_at], s, t).wait_recv()

    def own_row_of(ref):
        two = ref[:, pl.ds(pl.multiple_of(j * width, 128), width)].astype(jnp.float32)
        return jnp.where(prompt == 0, two[0:1], two[1:2])

    q1 = silu(own_row_of(probe))
    k1 = silu(own_row_of(address))
    k1 = k1 * lax.rsqrt(jnp.sum(k1 * k1, axis=-1, keepdims=True) + EPSILON)
    v1 = silu(own_row_of(content))
    b1 = sigmoid(jnp.full((1, width), strength[prompt, j], jnp.float32))
    q_and_k = jnp.concatenate([q1, k1, jnp.zeros((6, width), jnp.float32)], axis=0)
    recalled = jnp.dot(
        q_and_k,
        end.astype(jnp.float32),
        precision=HIGHEST_ACCURACY,
        preferred_element_type=jnp.float32,
    )
    weight = b1 * jnp.sum(q1 * k1, axis=-1, keepdims=True)
    read = recalled[0:1] + weight * (v1 - recalled[1:2])
    normed = read * lax.rsqrt(jnp.mean(read * read, axis=-1, keepdims=True) + EPSILON)
    gated = normed * gain[...] * silu(own_row_of(outgate))
    rmsg[...] = jnp.broadcast_to(gated.astype(jnp.bfloat16).astype(jnp.float32), rmsg.shape)
    for off in range(1, peers):
        to = (s + off) % peers
        go(remote(rmsg, rall.at[slot], r_send.at[off], r_recv.at[slot], to, t))
    rall[slot] = rmsg[...]

    others = near[1:]
    for cz in others:
        pass_on(slot, chip(x, y, cz))
    pass_on(slot, y_peer)
    pass_on(slot, x_peer)
    for n in range(peers):
        states[n] = found[n].astype(jnp.bfloat16)
    for off in range(1, peers):
        to = (s + off) % peers
        go(remote(states.at[to], bound.at[slot], b_send.at[off], b_recv.at[slot], to, t))
    bound[slot] = states[s]
    for cz in others:
        come = slot_of(chip(x, y, cz))
        arrived(come)
        pass_on(come, y_peer)
        pass_on(come, x_peer)
    for cz in near:
        come = slot_of(chip(x, 1 - y, cz))
        arrived(come)
        pass_on(come, x_peer)

    for off in range(1, peers):
        come = slot_of((s + off) % peers)
        remote(rall.at[come], rall.at[come], own_sem, r_recv.at[come], s, t).wait_recv()
    lines = [
        jnp.concatenate([rall[p * heads + h, 0:1, :] for h in range(heads)], axis=1)
        for p in range(2)
    ]
    lines.append(jnp.zeros((6, heads * width), jnp.float32))
    heads_read = jnp.concatenate(lines, axis=0).astype(jnp.bfloat16)
    loads[4].wait()
    terms = jnp.dot(heads_read, rv[...], preferred_element_type=jnp.float32)
    part[...] = terms.astype(jnp.bfloat16).astype(jnp.float32)
    swap = remote(part, partgot, t_send, t_recv, s, 1 - t)
    swap.start()
    swap.wait()
    mixed[...] = (part[...] + partgot[...])[:2].astype(mixed.dtype)

    for cz in range(DEEP):
        for cy in range(2):
            arrived(slot_of(chip(1 - x, cy, cz)))
    for off in range(1, peers):
        come = slot_of((s + off) % peers)
        ref = bound.at[come]
        remote(ref, ref, own_sem, b_recv.at[come], s, t).wait_recv()

    for copy in sent:
        copy.wait_send()

    for q in range(PLANE):
        row = prompt * PLANE + q
        ref = block_of(row)
        remote(ref, ref, relay_send.at[q], blk_recv.at[row], s, t).wait_send()

        @pl.when(home)
        def _():
            remote(wcross.at[q], ref, cross_send.at[q], blk_recv.at[row], s, t).wait_send()

    @pl.when(jnp.logical_not(home))
    def _():
        for cross in (1, 0):
            for kv in range(2):
                weight_copies(0, 0, cross, kv)[3].wait_send()

    def give_done(c, carry):
        exchange(c).wait_send()
        return carry

    lax.fori_loop(0, peers, give_done, 0)


def prefill(tok, wk, wv, gate_b, gate_a, add, offset, speed, first, strength, gain, readout, peers):
    _, length, model_width = tok.shape
    heads = add.shape[1]
    rows = wk.shape[0]
    width = ADDRESS_WIDTH
    half = model_width // 2
    dma = pltpu.SemaphoreType.DMA
    anywhere = pl.BlockSpec(memory_space=pl.ANY)
    vmem = pl.BlockSpec(memory_space=pltpu.VMEM)
    smem = pl.BlockSpec(memory_space=pltpu.SMEM)
    f32, bf16 = jnp.float32, jnp.bfloat16
    return pl.pallas_call(
        lambda *refs: prefill_kernel(peers, *refs),
        out_shape=(
            jax.ShapeDtypeStruct((peers, width, width), bf16),
            jax.ShapeDtypeStruct((peers, width, width), bf16),
            jax.ShapeDtypeStruct((2, readout.shape[1]), bf16),
        ),
        in_specs=[anywhere] * 6 + [smem] * 2 + [vmem] * 4 + [smem, vmem, anywhere],
        out_specs=(vmem, vmem, vmem),
        scratch_shapes=[
            pltpu.VMEM((peers, length, half), bf16),
            pltpu.VMEM((half, 4 * width), bf16),
            pltpu.VMEM((PLANE, rows, 4 * width), bf16),
            pltpu.VMEM(tok.shape, bf16),
            pltpu.VMEM((2,) + gate_b.shape, bf16),
            pltpu.VMEM(add.shape, f32),
            pltpu.VMEM((2, 2, gate_b.shape[0], length), f32),
            pltpu.VMEM((2, heads, 8, length), f32),
            pltpu.VMEM((DEEP, PLANE, 8, length), f32),
            pltpu.VMEM((peers, 8, length), f32),
            pltpu.VMEM((peers, length, 2 * width), f32),
            pltpu.VMEM((peers, length, 2 * width), f32),
            pltpu.VMEM((peers, length, 2 * width), f32),
            pltpu.VMEM((peers, width, 2 * width), f32),
            pltpu.VMEM((peers, width, width), bf16),
            pltpu.VMEM(readout.shape, bf16),
            pltpu.VMEM((8, width), f32),
            pltpu.VMEM((peers, 8, width), f32),
            pltpu.VMEM((8, readout.shape[1]), f32),
            pltpu.VMEM((8, readout.shape[1]), f32),
            dma((5,)),
            dma(()),
            dma((DEEP, PIECES)),
            dma((peers, PIECES)),
            dma((DEEP, PIECES)),
            dma((DEEP, PIECES)),
            dma((DEEP,)),
            dma((DEEP,)),
            dma((4, 4)),
            dma((2 * PLANE, 4)),
            dma((PLANE, 4)),
            dma((PLANE,)),
            dma((PLANE,)),
            dma((2 * PLANE,)),
            dma((DEEP,)),
            dma((DEEP,)),
            dma((DEEP, PLANE)),
            dma((peers,)),
            dma((peers,)),
            dma((peers,)),
            dma((peers,)),
            dma((peers,)),
            dma((peers,)),
            dma((peers,)),
            dma((peers,)),
            dma((peers,)),
            dma(()),
            dma(()),
        ],
        compiler_params=pltpu.CompilerParams(has_side_effects=True, collective_id=0),
        name="prefill",
    )(tok, wk, wv, gate_b, gate_a, add, offset, speed, *first, strength, gain, readout)


def per_device_heads(
    layer_source_tokens,
    address_projection,
    content_projection,
    strength_projection,
    fading_driver_projection,
    strength_offset,
    channel_fading_speed,
    added_fading_exponent,
    first_step_probe,
    first_step_address,
    first_step_content,
    first_step_outgate,
    first_step_strength_raw,
    channel_scaling_factor,
    readout_projection,
):
    peers = lax.axis_size("sp")
    head_local = channel_fading_speed.shape[0]
    width = ADDRESS_WIDTH
    final, bound, mixed = prefill(
        layer_source_tokens,
        address_projection,
        content_projection,
        strength_projection.T,
        fading_driver_projection.T,
        jnp.swapaxes(added_fading_exponent, 1, 2),
        strength_offset,
        channel_fading_speed,
        (first_step_probe, first_step_address, first_step_content, first_step_outgate),
        first_step_strength_raw,
        channel_scaling_factor.reshape(1, width),
        readout_projection,
        peers,
    )
    state_cache = final.reshape(2, head_local, width, width)
    boundary_cache = bound.reshape(2, 1, head_local, width, width)
    return (state_cache, mixed, boundary_cache)


def by_heads(mesh):
    def choose_form(*args):
        seq_count, length, model_width = args[0].shape
        peers, heads = lax.axis_size("sp"), args[6].shape[0]
        fits = (
            lax.axis_size("tp") == 2
            and seq_count == 2
            and peers == DEEP * PLANE
            and heads == 2 * PLANE
            and length == BLOCK
            and args[1].shape[0] * peers == model_width
        )
        return per_device_heads(*args) if fits else per_device(*args)

    return choose_form


def solution(mesh):
    return jax.shard_map(
        by_heads(mesh),
        mesh=mesh,
        in_specs=(
            P(None, "sp", None),
            P("sp", "tp"),
            P("sp", "tp"),
            P(),
            P(),
            P("tp"),
            P("tp"),
            P(None, "sp", "tp"),
            P(None, "tp"),
            P(None, "tp"),
            P(None, "tp"),
            P(None, "tp"),
            P(None, "tp"),
            P(),
            P("tp", "sp"),
        ),
        out_specs=(P(None, "tp", None, None), P(None, "sp"), P(None, "sp", "tp", None, None)),
        check_vma=False,
    )
```

```python
import jax
import jax.numpy as jnp
from jax import lax
from jax.experimental import pallas as pl
from jax.experimental.pallas import tpu as pltpu
from jax.sharding import PartitionSpec as P

ADDRESS_WIDTH = 128
BLOCK = 64


EPSILON = 1e-06
HIGHEST_ACCURACY = lax.Precision.HIGHEST


def prefix(array, axis, combine, identity):
    peers, index = (lax.axis_size(axis), lax.axis_index(axis))
    everything = jax.tree.map(
        lambda part, kind: lax.all_gather(part.astype(kind), axis),
        array,
        (jnp.bfloat16, jnp.bfloat16),
    )
    start = jax.tree.map(
        lambda part, zero: jnp.broadcast_to(jnp.asarray(zero, part.dtype), part.shape),
        array,
        identity,
    )

    def step(k, before):
        reached = k < index
        new = combine(
            before, jax.tree.map(lambda part, own: part[k].astype(own.dtype), everything, array)
        )
        return jax.tree.map(lambda a, b: jnp.where(reached, a, b), new, before)

    return lax.fori_loop(0, peers, step, start)


def as_sent(array):
    return jax.tree.map(lambda a: a.astype(jnp.bfloat16) if a.dtype == jnp.float32 else a, array)


def broadcast(value, axis, source):
    kept = jnp.where(lax.axis_index(axis) == source, value, 0).astype(value.dtype)
    return lax.psum(kept, axis)


def unit_inverse(lower_part):
    matrix_order = lower_part.shape[-1]
    identity = jnp.eye(matrix_order, dtype=jnp.float32)
    result = identity - lower_part
    power_term = lower_part
    reached = 2
    while reached < matrix_order:
        power_term = jnp.matmul(power_term, power_term, precision=HIGHEST_ACCURACY)
        result = jnp.matmul(result, identity + power_term, precision=HIGHEST_ACCURACY)
        reached = reached * 2
    return result


def build_arguments(
    address_vectors,
    content_vectors,
    outgate_raw_scores,
    strength_offset,
    channel_fading_speed,
    added_fading_exponent,
    channel_width,
):
    length = address_vectors.shape[0]
    attention_channels_total = channel_fading_speed.shape[0]
    address_token_slab = jax.nn.silu(address_vectors.astype(jnp.float32)).reshape(
        length, attention_channels_total, channel_width
    )
    address_token_slab = address_token_slab * lax.rsqrt(
        jnp.sum(address_token_slab * address_token_slab, axis=-1, keepdims=True) + EPSILON
    )
    content_token_slab = jax.nn.silu(content_vectors.astype(jnp.float32)).reshape(
        length, attention_channels_total, channel_width
    )
    strength_raw_expanded = outgate_raw_scores.astype(jnp.float32)
    storing_strength = jax.nn.sigmoid(
        strength_raw_expanded[:, :attention_channels_total] + strength_offset
    )
    fading_exponent = added_fading_exponent - channel_fading_speed * jax.nn.softplus(
        strength_raw_expanded[:, attention_channels_total:]
    )
    return (address_token_slab, content_token_slab, storing_strength, fading_exponent)


def range_map(address_token_slab, content_token_slab, storing_strength, fading_exponent, block):
    length, attention_channels_total, channel_width = address_token_slab.shape
    blocks = length // block

    def split_blocks(tensor):
        moved_axes = jnp.swapaxes(tensor, 0, 1)
        return moved_axes.reshape((attention_channels_total, blocks, block) + moved_axes.shape[2:])

    block_keys = split_blocks(address_token_slab)
    block_values = split_blocks(content_token_slab)
    block_beta = split_blocks(storing_strength)
    cumulative = jnp.cumsum(split_blocks(fading_exponent), axis=-1)
    positions = jnp.arange(block)
    strict = positions[:, None] > positions[None, :]
    spread_log = jnp.where(strict, cumulative[..., :, None] - cumulative[..., None, :], 0.0)
    scaled_keys = block_keys * block_beta[..., None]
    inner_prod = jnp.einsum("hnik,hnjk->hnij", scaled_keys, block_keys, precision=HIGHEST_ACCURACY)
    lower_part = jnp.where(strict, inner_prod * jnp.exp(spread_log), 0.0)
    inverse = unit_inverse(lower_part)
    targets = jnp.concatenate(
        [block_values * block_beta[..., None], scaled_keys * jnp.exp(cumulative)[..., None]],
        axis=-1,
    )
    solved = jnp.einsum("hnij,hnjk->hnik", inverse, targets, precision=HIGHEST_ACCURACY)
    updates = solved[..., :channel_width]
    key_weights = solved[..., channel_width:]
    tail_keys = block_keys * jnp.exp(cumulative[..., -1:] - cumulative)[..., None]
    last_decay = jnp.exp(cumulative[..., -1])
    identity = jnp.eye(channel_width, dtype=jnp.float32)

    def advance(state_pair, block_items):
        transition, carried_state = state_pair
        update_index, weight_index, tail_index, last_index = block_items
        fresh_value_rows = update_index - jnp.einsum(
            "xbg,xgp->xbp", weight_index, carried_state, precision=HIGHEST_ACCURACY
        )
        carried_state = carried_state * last_index[:, None, None] + jnp.einsum(
            "tjo,tjw->tow", tail_index, fresh_value_rows, precision=HIGHEST_ACCURACY
        )
        block_move = last_index[:, None, None] * identity - jnp.einsum(
            "hck,hcj->hkj", tail_index, weight_index, precision=HIGHEST_ACCURACY
        )
        transition = jnp.einsum("hij,hjk->hik", block_move, transition, precision=HIGHEST_ACCURACY)
        return ((transition, carried_state), None)

    initial = (
        jnp.broadcast_to(identity, (attention_channels_total, channel_width, channel_width)),
        jnp.zeros((attention_channels_total, channel_width, channel_width), jnp.float32),
    )
    block_items = (
        jnp.moveaxis(updates, 1, 0),
        jnp.moveaxis(key_weights, 1, 0),
        jnp.moveaxis(tail_keys, 1, 0),
        jnp.moveaxis(last_decay, 1, 0),
    )
    (transition, carried_state), _ = lax.scan(advance, initial, block_items)
    return (transition, carried_state)


def read_heads(
    state_cache,
    first_step_probe,
    first_step_address,
    first_step_content,
    first_step_outgate,
    first_step_strength_raw,
    channel_scaling_factor,
):
    seq_count, attention_channels_total, channel_width, _ = state_cache.shape
    carried_state = state_cache.astype(jnp.float32)

    def activate(tensor):
        return jax.nn.silu(tensor.astype(jnp.float32)).reshape(
            seq_count, attention_channels_total, channel_width
        )

    query_rows = activate(first_step_probe)
    address_token_slab = activate(first_step_address)
    address_token_slab = address_token_slab * lax.rsqrt(
        jnp.sum(address_token_slab * address_token_slab, axis=-1, keepdims=True) + EPSILON
    )
    content_token_slab = activate(first_step_content)
    storing_strength = jax.nn.sigmoid(first_step_strength_raw)
    recalled = jnp.einsum(
        "nhk,nhkv->nhv", address_token_slab, carried_state, precision=HIGHEST_ACCURACY
    )
    updated = (
        carried_state
        + storing_strength[..., None, None]
        * address_token_slab[..., :, None]
        * (content_token_slab - recalled)[..., None, :]
    )
    output = jnp.einsum("nhk,nhkv->nhv", query_rows, updated, precision=HIGHEST_ACCURACY)
    normed = (
        output
        * lax.rsqrt(jnp.mean(output * output, axis=-1, keepdims=True) + EPSILON)
        * channel_scaling_factor
    )
    gated_out = normed * activate(first_step_outgate)
    return gated_out.reshape(seq_count, attention_channels_total * channel_width).astype(
        jnp.bfloat16
    )


def matmul_maps(left, right):
    return jnp.einsum("shij,shjk->shik", left, right, precision=HIGHEST_ACCURACY)


def join_pairs(earlier, later):
    return (matmul_maps(later[0], earlier[0]), matmul_maps(later[0], earlier[1]) + later[1])


def per_device(
    layer_source_tokens,
    address_projection,
    content_projection,
    strength_projection,
    fading_driver_projection,
    strength_offset,
    channel_fading_speed,
    added_fading_exponent,
    first_step_probe,
    first_step_address,
    first_step_content,
    first_step_outgate,
    first_step_strength_raw,
    channel_scaling_factor,
    readout_projection,
):
    head_local = channel_fading_speed.shape[0]
    first_head = lax.axis_index("tp") * head_local
    beta_slice = lax.dynamic_slice_in_dim(strength_projection, first_head, head_local, 1)
    alpha_slice = lax.dynamic_slice_in_dim(fading_driver_projection, first_head, head_local, 1)
    seq_count, local_len, model_width = layer_source_tokens.shape
    flat_rows = layer_source_tokens.reshape(seq_count * local_len, model_width)
    key_sum = jnp.dot(
        flat_rows,
        lax.all_gather(address_projection, "sp", axis=0, tiled=True),
        preferred_element_type=jnp.float32,
    )
    value_sum = jnp.dot(
        flat_rows,
        lax.all_gather(content_projection, "sp", axis=0, tiled=True),
        preferred_element_type=jnp.float32,
    )
    beta_sum = jnp.dot(flat_rows, beta_slice, preferred_element_type=jnp.float32)
    alpha_sum = jnp.dot(flat_rows, alpha_slice, preferred_element_type=jnp.float32)
    outgate_raw_scores = (
        jnp.concatenate([beta_sum, alpha_sum], axis=1)
        .astype(jnp.bfloat16)
        .reshape(seq_count, local_len, -1)
    )
    address_vectors = key_sum.astype(jnp.bfloat16).reshape(seq_count, local_len, -1)
    content_vectors = value_sum.astype(jnp.bfloat16).reshape(seq_count, local_len, -1)
    transitions = []
    offsets = []
    for prompt_number in range(seq_count):
        address_token_slab, content_token_slab, storing_strength, fading_exponent = build_arguments(
            address_vectors[prompt_number],
            content_vectors[prompt_number],
            outgate_raw_scores[prompt_number],
            strength_offset,
            channel_fading_speed,
            added_fading_exponent[prompt_number],
            ADDRESS_WIDTH,
        )
        transition, carried_state = range_map(
            address_token_slab, content_token_slab, storing_strength, fading_exponent, BLOCK
        )
        transitions.append(transition)
        offsets.append(carried_state)
    transition = jnp.stack(transitions)
    offset = jnp.stack(offsets)
    identity = jnp.broadcast_to(jnp.eye(ADDRESS_WIDTH, dtype=jnp.float32), transition.shape)
    entered = prefix((transition, offset), "sp", join_pairs, (identity, jnp.zeros_like(offset)))
    leaving = matmul_maps(transition, entered[1]) + offset
    final = broadcast(as_sent(leaving), "sp", lax.axis_size("sp") - 1).astype(leaving.dtype)
    boundary_cache = leaving.astype(jnp.bfloat16)[:, None]
    state_cache = final.astype(jnp.bfloat16)
    heads_read = read_heads(
        state_cache,
        first_step_probe,
        first_step_address,
        first_step_content,
        first_step_outgate,
        first_step_strength_raw,
        channel_scaling_factor,
    )
    group_terms = jnp.dot(
        heads_read, readout_projection, preferred_element_type=jnp.float32
    ).astype(jnp.bfloat16)
    mixed_read = lax.psum(group_terms.astype(jnp.float32).astype(jnp.bfloat16), "tp")
    return (state_cache, mixed_read, boundary_cache)


MESH = pl.DeviceIdType.MESH
PIECES = 2
DEEP = 4
PLANE = 4


def remote(src, dst, send, recv, sp, tp):
    return pltpu.make_async_remote_copy(
        src_ref=src,
        dst_ref=dst,
        send_sem=send,
        recv_sem=recv,
        device_id={"sp": sp, "tp": tp},
        device_id_type=MESH,
    )


def silu(v):
    return v / (1.0 + jnp.exp(-v))


def sigmoid(v):
    return 1.0 / (1.0 + jnp.exp(-v))


def softplus(v):
    return jnp.maximum(v, 0.0) + jnp.log1p(jnp.exp(-jnp.abs(v)))


def halves(a):
    high = a.astype(jnp.bfloat16)
    return high, (a - high.astype(jnp.float32)).astype(jnp.bfloat16)


NN = (((1,), (0,)), ((), ()))
NT = (((1,), (1,)), ((), ()))
TN = (((0,), (0,)), ((), ()))


def prefill_kernel(
    peers,
    tok,
    wk,
    wv,
    gate_b,
    gate_a,
    add,
    offset,
    speed,
    probe,
    address,
    content,
    outgate,
    strength,
    gain,
    readout,
    final_out,
    bound_out,
    mixed,
    final,
    bound,
    xall,
    wall,
    wcross,
    tokv,
    gatev,
    addv,
    logit,
    msg,
    gz,
    gall,
    keep,
    give,
    got,
    states,
    rv,
    rmsg,
    rall,
    part,
    partgot,
    load,
    own_sem,
    z_send,
    tok_recv,
    x_send,
    y_send,
    xf_send,
    yf_send,
    w_send,
    w_recv,
    c_recv,
    relay_send,
    cross_send,
    blk_recv,
    gz_send,
    gz_recv,
    g_send,
    g_recv,
    give_send,
    give_recv,
    f_send,
    f_recv,
    b_send,
    b_recv,
    r_send,
    r_recv,
    t_send,
    t_recv,
    final_sem,
    bound_sem,
):
    s, t = lax.axis_index("sp"), lax.axis_index("tp")
    heads = add.shape[1]
    width = ADDRESS_WIDTH
    length = tok.shape[1]
    half = tok.shape[2] // 2
    rows = wk.shape[0]
    piece = length // PIECES
    x, y, z = s % 2, (s // 2) % 2, s // PLANE
    prompt, side = z % 2, z // 2
    j = side * PLANE + s % PLANE
    mate = z + 1 - 2 * prompt
    columns = pl.ds(pl.multiple_of(t * half, 128), half)

    def chip(cx, cy, cz):
        return PLANE * cz + 2 * cy + cx

    def slot_of(c):
        return (c // PLANE % 2) * heads + (c // PLANE // 2) * PLANE + c % PLANE

    x_peer, y_peer, z_peer = chip(1 - x, y, z), chip(x, 1 - y, z), chip(x, y, mate)
    diagonal = chip(1 - x, 1 - y, z)
    home = t == side

    def part_of(i):
        return pl.ds(i * piece, piece)

    sent = []

    def go(copy):
        copy.start()
        sent.append(copy)

    def token_wait(c, i):
        ref = xall.at[c, part_of(i)]
        remote(ref, ref, own_sem, tok_recv.at[c, i], s, t).wait_recv()

    near = [z, mate, DEEP - 1 - z, (z + DEEP // 2) % DEEP]
    barrier = pltpu.get_barrier_semaphore()
    partners = [(chip(x, y, near[k]), t) for k in range(1, DEEP)] + [(s, 1 - t)]
    partners += [(c, core) for c in (x_peer, y_peer, diagonal) for core in (t, 1 - t)]
    for c, core in partners:
        pl.semaphore_signal(
            barrier, inc=1, device_id={"sp": c, "tp": core}, device_id_type=MESH
        )
    loads = []
    for i, (src, dst) in enumerate(
        (
            (tok, tokv),
            (gate_b, gatev.at[0]),
            (gate_a, gatev.at[1]),
            (add, addv),
            (readout, rv),
        )
    ):
        copy = pltpu.make_async_copy(src, dst, load.at[i])
        copy.start()
        loads.append(copy)
    own = pltpu.make_async_copy(tok.at[prompt, :, columns], xall.at[s], own_sem)
    own.start()
    pl.semaphore_wait(barrier, len(partners))

    def along_z(k, source):
        for i in range(PIECES):
            go(
                remote(
                    source.at[near[k] % 2, part_of(i), columns],
                    xall.at[s, part_of(i)],
                    z_send.at[k, i],
                    tok_recv.at[s, i],
                    chip(x, y, near[k]),
                    t,
                )
            )

    along_z(1, tok)
    along_z(2, tok)

    side_of = (t + side) % 2
    own_row = s % (peers // 2)
    q_own = s % PLANE
    spot = pl.ds(pl.multiple_of(own_row * rows, 16), rows)

    def weight_copies(dx, dy, cross, kv):
        xd, yd = (x + dx) % 2, (y + dy) % 2
        head = ((side + cross) % 2) * PLANE + 2 * yd + xd
        src = (wk, wv)[kv].at[:, pl.ds(pl.multiple_of(head * width, 128), width)]
        at = pl.ds(pl.multiple_of((2 * side_of + kv) * width, 128), width)
        if cross:
            dst, sem = wcross.at[q_own, :, at], c_recv.at[q_own, 2 * side_of + kv]
        else:
            dst, sem = wall.at[spot, at], w_recv.at[own_row, 2 * side_of + kv]
        out = w_send.at[2 * dy + dx, 2 * cross + kv]
        return src, dst, sem, remote(src, dst, out, sem, chip(xd, yd, z), side)

    for dx, dy in ((0, 0), (1, 0), (0, 1), (1, 1)):
        for cross in (1, 0):
            for kv in range(2):
                src, dst, sem, copy = weight_copies(dx, dy, cross, kv)
                if dx + dy == 0:

                    @pl.when(home)
                    def _():
                        pltpu.make_async_copy(src, dst, sem).start()

                    @pl.when(jnp.logical_not(home))
                    def _():
                        copy.start()
                else:
                    go(copy)

    for i in range(PIECES):
        src = tok.at[prompt, part_of(i), columns]
        dst = xall.at[s, part_of(i)]
        go(remote(src, dst, x_send.at[0, i], tok_recv.at[s, i], x_peer, t))
        go(remote(src, dst, y_send.at[0, i], tok_recv.at[s, i], y_peer, t))

    def gates():
        for copy in loads[:4]:
            copy.wait()
        msg[...] = jnp.zeros_like(msg)
        for p in range(2):
            for kind in range(2):
                logit[p, kind] = (
                    lax.dot_general(gatev[kind], tokv[p], NT, preferred_element_type=jnp.float32)
                    .astype(jnp.bfloat16)
                    .astype(jnp.float32)
                )
            for h in range(heads):
                for kind in range(2):
                    msg[p, h, kind : kind + 1, :] = logit[p, kind, pl.ds(t * heads + h, 1), :]
                msg[p, h, 2:3, :] = addv[p, h : h + 1, :]
        for k in range(1, DEEP):
            src = msg.at[near[k] % 2, pl.ds(near[k] // 2 * PLANE, PLANE)]
            go(remote(src, gz.at[z], gz_send.at[k], gz_recv.at[z], chip(x, y, near[k]), t))
        for n, c in enumerate((x_peer, y_peer, diagonal)):
            src = msg.at[prompt, side * PLANE + c % PLANE]
            go(remote(src, gall.at[s], g_send.at[0, n], g_recv.at[s], c, t))
        gall[s] = msg[prompt, j]

    def pass_gates(k):
        cz = near[k]
        remote(gz.at[cz], gz.at[cz], own_sem, gz_recv.at[cz], s, t).wait_recv()
        c = chip(x, y, cz)
        for n, to in enumerate((x_peer, y_peer, diagonal)):
            go(remote(gz.at[cz, to % PLANE], gall.at[c], g_send.at[k, n], g_recv.at[c], to, t))
        gall[c] = gz[cz, q_own]

    def block_of(row):
        return wall.at[pl.ds(pl.multiple_of(row * rows, 16), rows)]

    def row_at(n):
        q = 2 * ((y + n // 2) % 2) + (x + n % 2) % 2
        return q, prompt * PLANE + q

    def home_relay(n):
        q, row = row_at(n)
        block = block_of(row)
        landing = chip(x, y, (z + DEEP // 2) % DEEP)
        for c in range(4):
            one = wcross.at[q, :, pl.ds(c * width, width)]
            pltpu.make_async_copy(one, one, c_recv.at[q, c]).wait()
        remote(wcross.at[q], block, cross_send.at[q], blk_recv.at[row], landing, t).start()
        for c in range(4):
            one = block.at[:, pl.ds(c * width, width)]
            pltpu.make_async_copy(one, one, w_recv.at[row, c]).wait()
        remote(block, block, relay_send.at[q], blk_recv.at[row], z_peer, t).start()

    def land_relay(n):
        q, row = row_at(n)
        ref = block_of(row)
        remote(ref, ref, relay_send.at[q], blk_recv.at[row], s, t).wait_recv()
        remote(ref, ref, relay_send.at[q], blk_recv.at[row], z_peer, t).start()

    def on_home(*ns):
        @pl.when(home)
        def _():
            for n in ns:
                home_relay(n)

    def on_land(*ns):
        @pl.when(jnp.logical_not(home))
        def _():
            for n in ns:
                land_relay(n)

    def spread_column(k):
        for i in range(PIECES):
            c = chip(x, y, near[k])
            token_wait(c, i)
            ref = xall.at[c, part_of(i)]
            go(remote(ref, ref, x_send.at[k, i], tok_recv.at[c, i], x_peer, t))
            go(remote(ref, ref, y_send.at[k, i], tok_recv.at[c, i], y_peer, t))

    def cross_plane(k):
        c = chip(1 - x, y, near[k])
        token_wait(c, 0)
        ref = xall.at[c, part_of(0)]
        go(remote(ref, ref, yf_send.at[k], tok_recv.at[c, 0], y_peer, t))
        c = chip(x, 1 - y, near[k])
        token_wait(c, 1)
        ref = xall.at[c, part_of(1)]
        go(remote(ref, ref, xf_send.at[k], tok_recv.at[c, 1], x_peer, t))

    def plane_of(g):
        value = near[0]
        for k in range(1, DEEP):
            value = jnp.where(g == k, near[k], value)
        return value

    def slots_of(g):
        return [PLANE * plane_of(g) + q for q in range(PLANE)]

    def exchange(c):
        return remote(give.at[c], got.at[c], give_send.at[c], give_recv.at[c], s, 1 - t)

    deep_rows = PLANE * rows

    def project(g, parity, first):
        slots = slots_of(g)
        depth = pl.ds(pl.multiple_of(parity * deep_rows, 128), deep_rows)
        rows_in = jnp.concatenate([xall[c, :, depth] for c in slots], axis=0)
        wide = jnp.dot(rows_in, wall[depth], preferred_element_type=jnp.float32)
        for i, c in enumerate(slots):
            part_rows = slice(i * length, (i + 1) * length)
            mine, theirs = wide[part_rows, : 2 * width], wide[part_rows, 2 * width :]
            if first:
                keep[c], give[c] = mine, theirs
            else:
                keep[c] += mine
                give[c] += theirs
        if not first:
            for c in slots:
                exchange(c).start()

    on_home(0)
    gates()
    on_home(1, 2)
    on_land(0)
    spread_column(1)
    along_z(3, tokv)
    on_home(3)
    on_land(1)
    cross_plane(0)
    pass_gates(1)
    on_land(2)
    spread_column(2)
    on_land(3)
    cross_plane(1)
    pass_gates(2)
    spread_column(3)
    pass_gates(3)
    cross_plane(2)
    cross_plane(3)

    def token_rest(g, carry):
        cz = plane_of(g)
        token_wait(chip(1 - x, y, cz), 1)
        token_wait(chip(x, 1 - y, cz), 0)
        token_wait(chip(1 - x, 1 - y, cz), 0)
        token_wait(chip(1 - x, 1 - y, cz), 1)
        project(g, prompt, True)
        return carry

    own.wait()
    lax.fori_loop(0, DEEP, token_rest, 0)

    for n in range(PLANE):
        row = (1 - prompt) * PLANE + n
        ref = block_of(row)
        remote(ref, ref, own_sem, blk_recv.at[row], s, t).wait_recv()

    for off in range(1, PLANE):
        for cz in near:
            c = PLANE * cz + (s + off) % PLANE
            remote(gall.at[c], gall.at[c], own_sem, g_recv.at[c], s, t).wait_recv()

    many = PLANE * length

    def left_form(full):
        two = full[:, : many // 2] + full[:, many // 2 :]
        high, low = halves(two + pltpu.roll(two, length, 1))
        return jnp.concatenate([high, low], axis=1)

    def right_form(full):
        blocks = [full[i * length : (i + 1) * length] for i in range(PLANE)]
        high, low = halves((blocks[0] + blocks[1]) + (blocks[2] + blocks[3]))
        return jnp.concatenate([high, low, high, low], axis=0)

    def one_dot(a, b, dims=NN):
        return lax.dot_general(a, b, dims, preferred_element_type=jnp.float32)

    def packed_dot(a, b):
        first = one_dot(jnp.concatenate(a, axis=1), jnp.concatenate([b[0], b[0]], axis=0))
        return first + one_dot(a[0], b[1])

    def maps_of(wide, bare_beta, bare_decay, added_decay):
        acted = silu(wide.astype(jnp.bfloat16).astype(jnp.float32))
        k = acted[:, :width]
        k = k * lax.rsqrt(jnp.sum(k * k, axis=-1, keepdims=True) + EPSILON)
        v = acted[:, width:]
        beta_row = sigmoid(bare_beta + offset[j])
        fade_row = added_decay - speed[j] * softplus(bare_decay)
        r = lax.broadcasted_iota(jnp.int32, (many, many), 0)
        c = lax.broadcasted_iota(jnp.int32, (many, many), 1)
        same = r // length == c // length
        strict = jnp.logical_and(same, r > c)
        eye = r == c

        def column(mask, row):
            return jnp.sum(jnp.where(mask, row, 0.0), axis=1, keepdims=True)

        def kept(full):
            return jnp.where(same, full, 0.0)

        sum_col = column(jnp.logical_and(same, r >= c), fade_row)
        all_col = column(same, fade_row)
        beta_col = column(eye, beta_row)
        sum_row = jnp.sum(jnp.where(eye, sum_col, 0.0), axis=0, keepdims=True)
        scaled = k * beta_col
        (high, low), (k_high, k_low) = halves(scaled), halves(k)
        inner_products = one_dot(
            jnp.concatenate([high, low], axis=1), jnp.concatenate([k_high, k_high], axis=1), NT
        ) + one_dot(high, k_low, NT)
        spread = jnp.exp(jnp.where(strict, sum_col - sum_row, 0.0))
        lower = jnp.where(strict, inner_products * spread, 0.0)
        left, right = left_form(lower), right_form(lower)
        inverse = jnp.where(eye, 1.0, 0.0) - lower
        reached = 2
        while reached < length:
            power = kept(one_dot(left, right))
            right = right_form(power)
            inverse = inverse + kept(one_dot(left_form(inverse), right))
            reached *= 2
            if reached < length:
                left = left_form(power)
        inverse = left_form(inverse)
        targets = halves(jnp.concatenate([scaled * jnp.exp(sum_col), v * beta_col], axis=1))
        tail = halves(k * jnp.exp(all_col - sum_col))
        last = jnp.exp(all_col)
        unit = (
            lax.broadcasted_iota(jnp.int32, (width, width), 0)
            == lax.broadcasted_iota(jnp.int32, (width, width), 1)
        ).astype(jnp.float32)
        pairs = []
        for i in range(PLANE):
            at = slice(i * length, (i + 1) * length)
            high, low = targets[0][at], targets[1][at]
            solved = one_dot(inverse[at], jnp.concatenate([high, low, high, low], axis=0))
            high, low = halves(solved)
            keys = jnp.concatenate([tail[0][at]] * 2 + [tail[1][at]] * 2, axis=0)
            maps = one_dot(keys, jnp.concatenate([high, low, high, low], axis=0), TN)
            moves = last[i * length : i * length + 1] * unit - maps[:, :width]
            pairs.append((moves, maps[:, width:]))
        return pairs

    def join(late, early):
        both = packed_dot(halves(late[0]), halves(jnp.concatenate(early, axis=1)))
        return both[:, :width], both[:, width:] + late[1]

    groups = peers // PLANE
    lax.fori_loop(0, groups, lambda g, carry: (project(g, 1 - prompt, False), carry)[1], 0)

    for c in range(peers):
        exchange(c).wait_recv()
    slot = slot_of(s)
    carried = None
    for g in range(groups):
        slots = range(g * PLANE, (g + 1) * PLANE)

        def row_of(kind, slots=slots):
            return jnp.concatenate([gall[c, kind : kind + 1, :] for c in slots], axis=1)

        wide = jnp.concatenate([keep[c] + got[c] for c in slots], axis=0)
        pairs = maps_of(wide, row_of(0), row_of(1), row_of(2))
        second = join(pairs[1], pairs[0])
        chain = [pairs[0], second, join(pairs[2], second), join(join(pairs[3], pairs[2]), second)]
        shifts = [shift for _, shift in chain]
        if carried is not None:
            shifts = [
                packed_dot(halves(move), carried) + shift for move, shift in chain
            ]
        carried = halves(shifts[-1])
        for c, shift in zip(slots, shifts):
            states[c] = shift.astype(jnp.bfloat16)
        if g == groups - 1:
            break
        for off in (1, 2, 3, 0):
            to = g * PLANE + (s + off) % PLANE
            copy = remote(
                states.at[to], bound.at[slot], b_send.at[g, off], b_recv.at[slot], to, t
            )
            if off:
                go(copy)
            else:
                pl.when(z != g)(copy.start)
    end = shifts[-1].astype(jnp.bfloat16)
    final[slot] = end
    f_sent = [0]

    def pass_on(slot_at, to):
        n = f_sent[0]
        f_sent[0] += 1
        ref = final.at[slot_at]
        go(remote(ref, ref, f_send.at[n], f_recv.at[slot_at], to, t))

    def store_final(slot_at):
        pltpu.make_async_copy(
            final.at[slot_at], final_out.at[slot_at], final_sem.at[slot_at]
        ).start()

    def store_bound(slot_at):
        pltpu.make_async_copy(
            bound.at[slot_at], bound_out.at[slot_at], bound_sem.at[slot_at]
        ).start()

    def arrived(slot_at):
        ref = final.at[slot_at]
        remote(ref, ref, own_sem, f_recv.at[slot_at], s, t).wait_recv()
        store_final(slot_at)

    def own_row_of(ref):
        two = ref[:, pl.ds(pl.multiple_of(j * width, 128), width)].astype(jnp.float32)
        return jnp.where(prompt == 0, two[0:1], two[1:2])

    q1 = silu(own_row_of(probe))
    k1 = silu(own_row_of(address))
    k1 = k1 * lax.rsqrt(jnp.sum(k1 * k1, axis=-1, keepdims=True) + EPSILON)
    v1 = silu(own_row_of(content))
    b1 = sigmoid(jnp.full((1, width), strength[prompt, j], jnp.float32))
    q_and_k = jnp.concatenate([q1, k1, jnp.zeros((6, width), jnp.float32)], axis=0)
    recalled = jnp.dot(
        q_and_k,
        end.astype(jnp.float32),
        precision=HIGHEST_ACCURACY,
        preferred_element_type=jnp.float32,
    )
    weight = b1 * jnp.sum(q1 * k1, axis=-1, keepdims=True)
    read = recalled[0:1] + weight * (v1 - recalled[1:2])
    normed = read * lax.rsqrt(jnp.mean(read * read, axis=-1, keepdims=True) + EPSILON)
    gated = normed * gain[...] * silu(own_row_of(outgate))
    rmsg[...] = jnp.broadcast_to(gated.astype(jnp.bfloat16).astype(jnp.float32), rmsg.shape)
    for off in range(1, peers):
        to = (s + off) % peers
        go(remote(rmsg, rall.at[slot], r_send.at[off], r_recv.at[slot], to, t))
    rall[slot] = rmsg[...]

    others = near[1:]
    for cz in others:
        pass_on(slot, chip(x, y, cz))
    pass_on(slot, y_peer)
    pass_on(slot, x_peer)
    last_plane = DEEP - 1
    for off in (1, 2, 3, 0):
        to = last_plane * PLANE + (s + off) % PLANE
        copy = remote(
            states.at[to], bound.at[slot], b_send.at[last_plane, off], b_recv.at[slot], to, t
        )
        if off:
            go(copy)
        else:
            pl.when(z != last_plane)(copy.start)
    bound[slot] = states[s]
    store_final(slot)
    store_bound(slot)
    for cz in others:
        come = slot_of(chip(x, y, cz))
        arrived(come)
        pass_on(come, y_peer)
        pass_on(come, x_peer)
    for off in range(1, peers):
        come = slot_of((s + off) % peers)
        remote(rall.at[come], rall.at[come], own_sem, r_recv.at[come], s, t).wait_recv()
    lines = [
        jnp.concatenate([rall[p * heads + h, 0:1, :] for h in range(heads)], axis=1)
        for p in range(2)
    ]
    lines.append(jnp.zeros((6, heads * width), jnp.float32))
    heads_read = jnp.concatenate(lines, axis=0).astype(jnp.bfloat16)
    loads[4].wait()
    terms = jnp.dot(heads_read, rv[...], preferred_element_type=jnp.float32)
    part[...] = terms.astype(jnp.bfloat16).astype(jnp.float32)
    swap = remote(part, partgot, t_send, t_recv, s, 1 - t)
    swap.start()
    swap.wait()
    mixed[...] = (part[...] + partgot[...])[:2].astype(mixed.dtype)

    for cz in near:
        come = slot_of(chip(x, 1 - y, cz))
        arrived(come)
        pass_on(come, x_peer)

    for cz in range(DEEP):
        for cy in range(2):
            arrived(slot_of(chip(1 - x, cy, cz)))
    for off in range(1, peers):
        come = slot_of((s + off) % peers)
        ref = bound.at[come]
        remote(ref, ref, own_sem, b_recv.at[come], s, t).wait_recv()
        store_bound(come)

    for g in range(groups):
        ref = states.at[g * PLANE + s % PLANE]
        copy = remote(ref, bound.at[slot], b_send.at[g, 0], b_recv.at[slot], s, t)
        pl.when(z != g)(copy.wait_send)
    for copy in sent:
        copy.wait_send()

    for q in range(PLANE):
        row = prompt * PLANE + q
        ref = block_of(row)
        remote(ref, ref, relay_send.at[q], blk_recv.at[row], s, t).wait_send()

        @pl.when(home)
        def _():
            remote(wcross.at[q], ref, cross_send.at[q], blk_recv.at[row], s, t).wait_send()

    @pl.when(jnp.logical_not(home))
    def _():
        for cross in (1, 0):
            for kv in range(2):
                weight_copies(0, 0, cross, kv)[3].wait_send()

    def give_done(c, carry):
        exchange(c).wait_send()
        return carry

    lax.fori_loop(0, peers, give_done, 0)
    for c in range(peers):
        pltpu.make_async_copy(final.at[c], final_out.at[c], final_sem.at[c]).wait()
        pltpu.make_async_copy(bound.at[c], bound_out.at[c], bound_sem.at[c]).wait()


def prefill(tok, wk, wv, gate_b, gate_a, add, offset, speed, first, strength, gain, readout, peers):
    _, length, model_width = tok.shape
    heads = add.shape[1]
    rows = wk.shape[0]
    width = ADDRESS_WIDTH
    half = model_width // 2
    dma = pltpu.SemaphoreType.DMA
    anywhere = pl.BlockSpec(memory_space=pl.ANY)
    vmem = pl.BlockSpec(memory_space=pltpu.VMEM)
    smem = pl.BlockSpec(memory_space=pltpu.SMEM)
    f32, bf16 = jnp.float32, jnp.bfloat16
    return pl.pallas_call(
        lambda *refs: prefill_kernel(peers, *refs),
        out_shape=(
            jax.ShapeDtypeStruct((peers, width, width), bf16),
            jax.ShapeDtypeStruct((peers, width, width), bf16),
            jax.ShapeDtypeStruct((2, readout.shape[1]), bf16),
        ),
        in_specs=[anywhere] * 6 + [smem] * 2 + [vmem] * 4 + [smem, vmem, anywhere],
        out_specs=(anywhere, anywhere, vmem),
        scratch_shapes=[
            pltpu.VMEM((peers, width, width), bf16),
            pltpu.VMEM((peers, width, width), bf16),
            pltpu.VMEM((peers, length, half), bf16),
            pltpu.VMEM((half, 4 * width), bf16),
            pltpu.VMEM((PLANE, rows, 4 * width), bf16),
            pltpu.VMEM(tok.shape, bf16),
            pltpu.VMEM((2,) + gate_b.shape, bf16),
            pltpu.VMEM(add.shape, f32),
            pltpu.VMEM((2, 2, gate_b.shape[0], length), f32),
            pltpu.VMEM((2, heads, 8, length), f32),
            pltpu.VMEM((DEEP, PLANE, 8, length), f32),
            pltpu.VMEM((peers, 8, length), f32),
            pltpu.VMEM((peers, length, 2 * width), f32),
            pltpu.VMEM((peers, length, 2 * width), f32),
            pltpu.VMEM((peers, length, 2 * width), f32),
            pltpu.VMEM((peers, width, width), bf16),
            pltpu.VMEM(readout.shape, bf16),
            pltpu.VMEM((8, width), f32),
            pltpu.VMEM((peers, 8, width), f32),
            pltpu.VMEM((8, readout.shape[1]), f32),
            pltpu.VMEM((8, readout.shape[1]), f32),
            dma((5,)),
            dma(()),
            dma((DEEP, PIECES)),
            dma((peers, PIECES)),
            dma((DEEP, PIECES)),
            dma((DEEP, PIECES)),
            dma((DEEP,)),
            dma((DEEP,)),
            dma((4, 4)),
            dma((2 * PLANE, 4)),
            dma((PLANE, 4)),
            dma((PLANE,)),
            dma((PLANE,)),
            dma((2 * PLANE,)),
            dma((DEEP,)),
            dma((DEEP,)),
            dma((DEEP, PLANE)),
            dma((peers,)),
            dma((peers,)),
            dma((peers,)),
            dma((peers,)),
            dma((peers,)),
            dma((DEEP, PLANE)),
            dma((peers,)),
            dma((peers,)),
            dma((peers,)),
            dma(()),
            dma(()),
            dma((peers,)),
            dma((peers,)),
        ],
        compiler_params=pltpu.CompilerParams(has_side_effects=True, collective_id=0),
        name="prefill",
    )(tok, wk, wv, gate_b, gate_a, add, offset, speed, *first, strength, gain, readout)


def hand_over(*arrays):
    def kernel(*refs):
        count = len(arrays)
        sources, targets, held = (refs[i * count : (i + 1) * count] for i in range(3))
        came, left = refs[3 * count :]
        steps = []
        for i in range(count):
            steps.append(
                (
                    pltpu.make_async_copy(sources[i], held[i], came.at[i]),
                    pltpu.make_async_copy(held[i], targets[i], left.at[i]),
                )
            )
        for first, _ in steps:
            first.start()
        for first, second in steps:
            first.wait()
            second.start()
        for _, second in steps:
            second.wait()

    anywhere = pl.BlockSpec(memory_space=pl.ANY)
    return pl.pallas_call(
        kernel,
        out_shape=tuple(jax.ShapeDtypeStruct(a.shape, a.dtype) for a in arrays),
        in_specs=[anywhere] * len(arrays),
        out_specs=(anywhere,) * len(arrays),
        scratch_shapes=[pltpu.VMEM(a.shape, a.dtype) for a in arrays]
        + [pltpu.SemaphoreType.DMA((len(arrays),))] * 2,
        name="hand_over",
    )(*arrays)


def per_device_heads(
    layer_source_tokens,
    address_projection,
    content_projection,
    strength_projection,
    fading_driver_projection,
    strength_offset,
    channel_fading_speed,
    added_fading_exponent,
    first_step_probe,
    first_step_address,
    first_step_content,
    first_step_outgate,
    first_step_strength_raw,
    channel_scaling_factor,
    readout_projection,
):
    peers = lax.axis_size("sp")
    head_local = channel_fading_speed.shape[0]
    width = ADDRESS_WIDTH
    final, bound, mixed = prefill(
        layer_source_tokens,
        address_projection,
        content_projection,
        strength_projection.T,
        fading_driver_projection.T,
        jnp.swapaxes(added_fading_exponent, 1, 2),
        strength_offset,
        channel_fading_speed,
        (first_step_probe, first_step_address, first_step_content, first_step_outgate),
        first_step_strength_raw,
        channel_scaling_factor.reshape(1, width),
        readout_projection,
        peers,
    )
    final, bound, mixed = hand_over(final, bound, mixed)
    state_cache = final.reshape(2, head_local, width, width)
    boundary_cache = bound.reshape(2, 1, head_local, width, width)
    return (state_cache, mixed, boundary_cache)


def by_heads(mesh):
    def choose_form(*args):
        seq_count, length, model_width = args[0].shape
        peers, heads = lax.axis_size("sp"), args[6].shape[0]
        fits = (
            lax.axis_size("tp") == 2
            and seq_count == 2
            and peers == DEEP * PLANE
            and heads == 2 * PLANE
            and length == BLOCK
            and args[1].shape[0] * peers == model_width
        )
        return per_device_heads(*args) if fits else per_device(*args)

    return choose_form


def solution(mesh):
    return jax.shard_map(
        by_heads(mesh),
        mesh=mesh,
        in_specs=(
            P(None, "sp", None),
            P("sp", "tp"),
            P("sp", "tp"),
            P(),
            P(),
            P("tp"),
            P("tp"),
            P(None, "sp", "tp"),
            P(None, "tp"),
            P(None, "tp"),
            P(None, "tp"),
            P(None, "tp"),
            P(None, "tp"),
            P(),
            P("tp", "sp"),
        ),
        out_specs=(P(None, "tp", None, None), P(None, "sp"), P(None, "sp", "tp", None, None)),
        check_vma=False,
    )
```

```python
import jax
import jax.numpy as jnp
from jax import lax
from jax.experimental import pallas as pl
from jax.experimental.pallas import tpu as pltpu
from jax.sharding import PartitionSpec as P

ADDRESS_WIDTH = 128
BLOCK = 64


EPSILON = 1e-06
HIGHEST_ACCURACY = lax.Precision.HIGHEST


def prefix(array, axis, combine, identity):
    peers, index = (lax.axis_size(axis), lax.axis_index(axis))
    everything = jax.tree.map(
        lambda part, kind: lax.all_gather(part.astype(kind), axis),
        array,
        (jnp.bfloat16, jnp.bfloat16),
    )
    start = jax.tree.map(
        lambda part, zero: jnp.broadcast_to(jnp.asarray(zero, part.dtype), part.shape),
        array,
        identity,
    )

    def step(k, before):
        reached = k < index
        new = combine(
            before, jax.tree.map(lambda part, own: part[k].astype(own.dtype), everything, array)
        )
        return jax.tree.map(lambda a, b: jnp.where(reached, a, b), new, before)

    return lax.fori_loop(0, peers, step, start)


def as_sent(array):
    return jax.tree.map(lambda a: a.astype(jnp.bfloat16) if a.dtype == jnp.float32 else a, array)


def broadcast(value, axis, source):
    kept = jnp.where(lax.axis_index(axis) == source, value, 0).astype(value.dtype)
    return lax.psum(kept, axis)


def unit_inverse(lower_part):
    matrix_order = lower_part.shape[-1]
    identity = jnp.eye(matrix_order, dtype=jnp.float32)
    result = identity - lower_part
    power_term = lower_part
    reached = 2
    while reached < matrix_order:
        power_term = jnp.matmul(power_term, power_term, precision=HIGHEST_ACCURACY)
        result = jnp.matmul(result, identity + power_term, precision=HIGHEST_ACCURACY)
        reached = reached * 2
    return result


def build_arguments(
    address_vectors,
    content_vectors,
    outgate_raw_scores,
    strength_offset,
    channel_fading_speed,
    added_fading_exponent,
    channel_width,
):
    length = address_vectors.shape[0]
    attention_channels_total = channel_fading_speed.shape[0]
    address_token_slab = jax.nn.silu(address_vectors.astype(jnp.float32)).reshape(
        length, attention_channels_total, channel_width
    )
    address_token_slab = address_token_slab * lax.rsqrt(
        jnp.sum(address_token_slab * address_token_slab, axis=-1, keepdims=True) + EPSILON
    )
    content_token_slab = jax.nn.silu(content_vectors.astype(jnp.float32)).reshape(
        length, attention_channels_total, channel_width
    )
    strength_raw_expanded = outgate_raw_scores.astype(jnp.float32)
    storing_strength = jax.nn.sigmoid(
        strength_raw_expanded[:, :attention_channels_total] + strength_offset
    )
    fading_exponent = added_fading_exponent - channel_fading_speed * jax.nn.softplus(
        strength_raw_expanded[:, attention_channels_total:]
    )
    return (address_token_slab, content_token_slab, storing_strength, fading_exponent)


def range_map(address_token_slab, content_token_slab, storing_strength, fading_exponent, block):
    length, attention_channels_total, channel_width = address_token_slab.shape
    blocks = length // block

    def split_blocks(tensor):
        moved_axes = jnp.swapaxes(tensor, 0, 1)
        return moved_axes.reshape((attention_channels_total, blocks, block) + moved_axes.shape[2:])

    block_keys = split_blocks(address_token_slab)
    block_values = split_blocks(content_token_slab)
    block_beta = split_blocks(storing_strength)
    cumulative = jnp.cumsum(split_blocks(fading_exponent), axis=-1)
    positions = jnp.arange(block)
    strict = positions[:, None] > positions[None, :]
    spread_log = jnp.where(strict, cumulative[..., :, None] - cumulative[..., None, :], 0.0)
    scaled_keys = block_keys * block_beta[..., None]
    inner_prod = jnp.einsum("hnik,hnjk->hnij", scaled_keys, block_keys, precision=HIGHEST_ACCURACY)
    lower_part = jnp.where(strict, inner_prod * jnp.exp(spread_log), 0.0)
    inverse = unit_inverse(lower_part)
    targets = jnp.concatenate(
        [block_values * block_beta[..., None], scaled_keys * jnp.exp(cumulative)[..., None]],
        axis=-1,
    )
    solved = jnp.einsum("hnij,hnjk->hnik", inverse, targets, precision=HIGHEST_ACCURACY)
    updates = solved[..., :channel_width]
    key_weights = solved[..., channel_width:]
    tail_keys = block_keys * jnp.exp(cumulative[..., -1:] - cumulative)[..., None]
    last_decay = jnp.exp(cumulative[..., -1])
    identity = jnp.eye(channel_width, dtype=jnp.float32)

    def advance(state_pair, block_items):
        transition, carried_state = state_pair
        update_index, weight_index, tail_index, last_index = block_items
        fresh_value_rows = update_index - jnp.einsum(
            "xbg,xgp->xbp", weight_index, carried_state, precision=HIGHEST_ACCURACY
        )
        carried_state = carried_state * last_index[:, None, None] + jnp.einsum(
            "tjo,tjw->tow", tail_index, fresh_value_rows, precision=HIGHEST_ACCURACY
        )
        block_move = last_index[:, None, None] * identity - jnp.einsum(
            "hck,hcj->hkj", tail_index, weight_index, precision=HIGHEST_ACCURACY
        )
        transition = jnp.einsum("hij,hjk->hik", block_move, transition, precision=HIGHEST_ACCURACY)
        return ((transition, carried_state), None)

    initial = (
        jnp.broadcast_to(identity, (attention_channels_total, channel_width, channel_width)),
        jnp.zeros((attention_channels_total, channel_width, channel_width), jnp.float32),
    )
    block_items = (
        jnp.moveaxis(updates, 1, 0),
        jnp.moveaxis(key_weights, 1, 0),
        jnp.moveaxis(tail_keys, 1, 0),
        jnp.moveaxis(last_decay, 1, 0),
    )
    (transition, carried_state), _ = lax.scan(advance, initial, block_items)
    return (transition, carried_state)


def read_heads(
    state_cache,
    first_step_probe,
    first_step_address,
    first_step_content,
    first_step_outgate,
    first_step_strength_raw,
    channel_scaling_factor,
):
    seq_count, attention_channels_total, channel_width, _ = state_cache.shape
    carried_state = state_cache.astype(jnp.float32)

    def activate(tensor):
        return jax.nn.silu(tensor.astype(jnp.float32)).reshape(
            seq_count, attention_channels_total, channel_width
        )

    query_rows = activate(first_step_probe)
    address_token_slab = activate(first_step_address)
    address_token_slab = address_token_slab * lax.rsqrt(
        jnp.sum(address_token_slab * address_token_slab, axis=-1, keepdims=True) + EPSILON
    )
    content_token_slab = activate(first_step_content)
    storing_strength = jax.nn.sigmoid(first_step_strength_raw)
    recalled = jnp.einsum(
        "nhk,nhkv->nhv", address_token_slab, carried_state, precision=HIGHEST_ACCURACY
    )
    updated = (
        carried_state
        + storing_strength[..., None, None]
        * address_token_slab[..., :, None]
        * (content_token_slab - recalled)[..., None, :]
    )
    output = jnp.einsum("nhk,nhkv->nhv", query_rows, updated, precision=HIGHEST_ACCURACY)
    normed = (
        output
        * lax.rsqrt(jnp.mean(output * output, axis=-1, keepdims=True) + EPSILON)
        * channel_scaling_factor
    )
    gated_out = normed * activate(first_step_outgate)
    return gated_out.reshape(seq_count, attention_channels_total * channel_width).astype(
        jnp.bfloat16
    )


def matmul_maps(left, right):
    return jnp.einsum("shij,shjk->shik", left, right, precision=HIGHEST_ACCURACY)


def join_pairs(earlier, later):
    return (matmul_maps(later[0], earlier[0]), matmul_maps(later[0], earlier[1]) + later[1])


def per_device(
    layer_source_tokens,
    address_projection,
    content_projection,
    strength_projection,
    fading_driver_projection,
    strength_offset,
    channel_fading_speed,
    added_fading_exponent,
    first_step_probe,
    first_step_address,
    first_step_content,
    first_step_outgate,
    first_step_strength_raw,
    channel_scaling_factor,
    readout_projection,
):
    head_local = channel_fading_speed.shape[0]
    first_head = lax.axis_index("tp") * head_local
    beta_slice = lax.dynamic_slice_in_dim(strength_projection, first_head, head_local, 1)
    alpha_slice = lax.dynamic_slice_in_dim(fading_driver_projection, first_head, head_local, 1)
    seq_count, local_len, model_width = layer_source_tokens.shape
    flat_rows = layer_source_tokens.reshape(seq_count * local_len, model_width)
    key_sum = jnp.dot(
        flat_rows,
        lax.all_gather(address_projection, "sp", axis=0, tiled=True),
        preferred_element_type=jnp.float32,
    )
    value_sum = jnp.dot(
        flat_rows,
        lax.all_gather(content_projection, "sp", axis=0, tiled=True),
        preferred_element_type=jnp.float32,
    )
    beta_sum = jnp.dot(flat_rows, beta_slice, preferred_element_type=jnp.float32)
    alpha_sum = jnp.dot(flat_rows, alpha_slice, preferred_element_type=jnp.float32)
    outgate_raw_scores = (
        jnp.concatenate([beta_sum, alpha_sum], axis=1)
        .astype(jnp.bfloat16)
        .reshape(seq_count, local_len, -1)
    )
    address_vectors = key_sum.astype(jnp.bfloat16).reshape(seq_count, local_len, -1)
    content_vectors = value_sum.astype(jnp.bfloat16).reshape(seq_count, local_len, -1)
    transitions = []
    offsets = []
    for prompt_number in range(seq_count):
        address_token_slab, content_token_slab, storing_strength, fading_exponent = build_arguments(
            address_vectors[prompt_number],
            content_vectors[prompt_number],
            outgate_raw_scores[prompt_number],
            strength_offset,
            channel_fading_speed,
            added_fading_exponent[prompt_number],
            ADDRESS_WIDTH,
        )
        transition, carried_state = range_map(
            address_token_slab, content_token_slab, storing_strength, fading_exponent, BLOCK
        )
        transitions.append(transition)
        offsets.append(carried_state)
    transition = jnp.stack(transitions)
    offset = jnp.stack(offsets)
    identity = jnp.broadcast_to(jnp.eye(ADDRESS_WIDTH, dtype=jnp.float32), transition.shape)
    entered = prefix((transition, offset), "sp", join_pairs, (identity, jnp.zeros_like(offset)))
    leaving = matmul_maps(transition, entered[1]) + offset
    final = broadcast(as_sent(leaving), "sp", lax.axis_size("sp") - 1).astype(leaving.dtype)
    boundary_cache = leaving.astype(jnp.bfloat16)[:, None]
    state_cache = final.astype(jnp.bfloat16)
    heads_read = read_heads(
        state_cache,
        first_step_probe,
        first_step_address,
        first_step_content,
        first_step_outgate,
        first_step_strength_raw,
        channel_scaling_factor,
    )
    group_terms = jnp.dot(
        heads_read, readout_projection, preferred_element_type=jnp.float32
    ).astype(jnp.bfloat16)
    mixed_read = lax.psum(group_terms.astype(jnp.float32).astype(jnp.bfloat16), "tp")
    return (state_cache, mixed_read, boundary_cache)


MESH = pl.DeviceIdType.MESH
PIECES = 2
DEEP = 4
PLANE = 4


def remote(src, dst, send, recv, sp, tp):
    return pltpu.make_async_remote_copy(
        src_ref=src,
        dst_ref=dst,
        send_sem=send,
        recv_sem=recv,
        device_id={"sp": sp, "tp": tp},
        device_id_type=MESH,
    )


def silu(v):
    return v / (1.0 + jnp.exp(-v))


def sigmoid(v):
    return 1.0 / (1.0 + jnp.exp(-v))


def softplus(v):
    return jnp.maximum(v, 0.0) + jnp.log1p(jnp.exp(-jnp.abs(v)))


def halves(a):
    high = a.astype(jnp.bfloat16)
    return high, (a - high.astype(jnp.float32)).astype(jnp.bfloat16)


NN = (((1,), (0,)), ((), ()))
NT = (((1,), (1,)), ((), ()))
TN = (((0,), (0,)), ((), ()))


def prefill_kernel(
    peers,
    tok,
    wk,
    wv,
    gate_b,
    gate_a,
    add,
    offset,
    speed,
    probe,
    address,
    content,
    outgate,
    strength,
    gain,
    readout,
    final_out,
    bound_out,
    mixed,
    final,
    bound,
    xall,
    wall,
    wcross,
    tokv,
    gatev,
    addv,
    logit,
    msg,
    gz,
    gall,
    keep,
    give,
    got,
    states,
    rv,
    rmsg,
    rall,
    part,
    partgot,
    load,
    own_sem,
    tok_send,
    tok_recv,
    w_send,
    w_away,
    w_recv,
    c_recv,
    relay_send,
    cross_send,
    blk_recv,
    gz_send,
    gz_recv,
    g_send,
    g_recv,
    give_send,
    give_recv,
    f_send,
    f_recv,
    b_send,
    b_recv,
    r_send,
    r_recv,
    t_send,
    t_recv,
    final_sem,
    bound_sem,
):
    s, t = lax.axis_index("sp"), lax.axis_index("tp")
    heads = add.shape[1]
    width = ADDRESS_WIDTH
    length = tok.shape[1]
    half = tok.shape[2] // 2
    rows = wk.shape[0]
    piece = length // PIECES
    x, y, z = s % 2, (s // 2) % 2, s // PLANE
    prompt, side = z % 2, z // 2
    j = side * PLANE + s % PLANE
    mate = z + 1 - 2 * prompt
    columns = pl.ds(pl.multiple_of(t * half, 128), half)

    def chip(cx, cy, cz):
        return PLANE * cz + 2 * cy + cx

    def slot_of(c):
        return (c // PLANE % 2) * heads + (c // PLANE // 2) * PLANE + c % PLANE

    x_peer, y_peer, z_peer = chip(1 - x, y, z), chip(x, 1 - y, z), chip(x, y, mate)
    diagonal = chip(1 - x, 1 - y, z)
    home = t == side

    def part_of(i):
        return pl.ds(i * piece, piece)

    sent = {"tok": 0, "final": 0}

    def go(copy, kind=None):
        copy.start()
        if kind:
            sent[kind] += 1

    def token_wait(c, i):
        ref = xall.at[c, part_of(i)]
        remote(ref, ref, own_sem, tok_recv.at[c, i], s, t).wait_recv()

    near = [z, mate, DEEP - 1 - z, (z + DEEP // 2) % DEEP]
    barrier = pltpu.get_barrier_semaphore()
    partners = [(chip(x, y, near[k]), t) for k in range(1, DEEP)] + [(s, 1 - t)]
    partners += [(c, core) for c in (x_peer, y_peer, diagonal) for core in (t, 1 - t)]
    for c, core in partners:
        pl.semaphore_signal(
            barrier, inc=1, device_id={"sp": c, "tp": core}, device_id_type=MESH
        )
    loads = []
    for i, (src, dst) in enumerate(
        (
            (tok, tokv),
            (gate_b, gatev.at[0]),
            (gate_a, gatev.at[1]),
            (add, addv),
            (readout, rv),
        )
    ):
        copy = pltpu.make_async_copy(src, dst, load.at[i])
        copy.start()
        loads.append(copy)
    own = pltpu.make_async_copy(tok.at[prompt, :, columns], xall.at[s], own_sem)
    own.start()
    pl.semaphore_wait(barrier, len(partners))

    def along_z(k, source):
        for i in range(PIECES):
            go(
                remote(
                    source.at[near[k] % 2, part_of(i), columns],
                    xall.at[s, part_of(i)],
                    tok_send,
                    tok_recv.at[s, i],
                    chip(x, y, near[k]),
                    t,
                ),
                "tok",
            )

    along_z(1, tok)
    along_z(2, tok)

    side_of = (t + side) % 2
    own_row = s % (peers // 2)
    q_own = s % PLANE
    spot = pl.ds(pl.multiple_of(own_row * rows, 16), rows)

    def weight_copies(dx, dy, cross, kv):
        xd, yd = (x + dx) % 2, (y + dy) % 2
        head = ((side + cross) % 2) * PLANE + 2 * yd + xd
        src = (wk, wv)[kv].at[:, pl.ds(pl.multiple_of(head * width, 128), width)]
        at = pl.ds(pl.multiple_of((2 * side_of + kv) * width, 128), width)
        if cross:
            dst, sem = wcross.at[q_own, :, at], c_recv.at[q_own]
        else:
            dst, sem = wall.at[spot, at], w_recv.at[q_own]
        out = w_send if dx + dy else w_away
        return src, dst, sem, remote(src, dst, out, sem, chip(xd, yd, z), side)

    for dx, dy in ((0, 0), (1, 0), (0, 1), (1, 1)):
        for cross in (1, 0):
            for kv in range(2):
                src, dst, sem, copy = weight_copies(dx, dy, cross, kv)
                if dx + dy == 0:

                    @pl.when(home)
                    def _():
                        pltpu.make_async_copy(src, dst, sem).start()

                    @pl.when(jnp.logical_not(home))
                    def _():
                        copy.start()
                else:
                    go(copy)

    for i in range(PIECES):
        src = tok.at[prompt, part_of(i), columns]
        dst = xall.at[s, part_of(i)]
        go(remote(src, dst, tok_send, tok_recv.at[s, i], x_peer, t), "tok")
        go(remote(src, dst, tok_send, tok_recv.at[s, i], y_peer, t), "tok")

    def gates():
        for copy in loads[:4]:
            copy.wait()
        msg[...] = jnp.zeros_like(msg)
        for p in range(2):
            for kind in range(2):
                logit[p, kind] = (
                    lax.dot_general(gatev[kind], tokv[p], NT, preferred_element_type=jnp.float32)
                    .astype(jnp.bfloat16)
                    .astype(jnp.float32)
                )
            for h in range(heads):
                for kind in range(2):
                    msg[p, h, kind : kind + 1, :] = logit[p, kind, pl.ds(t * heads + h, 1), :]
                msg[p, h, 2:3, :] = addv[p, h : h + 1, :]
        for k in range(1, DEEP):
            src = msg.at[near[k] % 2, pl.ds(near[k] // 2 * PLANE, PLANE)]
            go(remote(src, gz.at[z], gz_send, gz_recv.at[z], chip(x, y, near[k]), t))
        for n, c in enumerate((x_peer, y_peer, diagonal)):
            src = msg.at[prompt, side * PLANE + c % PLANE]
            go(remote(src, gall.at[s], g_send, g_recv, c, t))
        gall[s] = msg[prompt, j]

    def pass_gates(k):
        cz = near[k]
        remote(gz.at[cz], gz.at[cz], own_sem, gz_recv.at[cz], s, t).wait_recv()
        c = chip(x, y, cz)
        for n, to in enumerate((x_peer, y_peer, diagonal)):
            go(remote(gz.at[cz, to % PLANE], gall.at[c], g_send, g_recv, to, t))
        gall[c] = gz[cz, q_own]

    def block_of(row):
        return wall.at[pl.ds(pl.multiple_of(row * rows, 16), rows)]

    def row_at(n):
        q = 2 * ((y + n // 2) % 2) + (x + n % 2) % 2
        return q, prompt * PLANE + q

    def home_relay(n):
        q, row = row_at(n)
        block = block_of(row)
        landing = chip(x, y, (z + DEEP // 2) % DEEP)
        pltpu.make_async_copy(wcross.at[q], wcross.at[q], c_recv.at[q]).wait()
        remote(wcross.at[q], block, cross_send, blk_recv.at[row], landing, t).start()
        pltpu.make_async_copy(block, block, w_recv.at[q]).wait()
        remote(block, block, relay_send, blk_recv.at[row], z_peer, t).start()

    def land_relay(n):
        q, row = row_at(n)
        ref = block_of(row)
        remote(ref, ref, relay_send, blk_recv.at[row], s, t).wait_recv()
        remote(ref, ref, relay_send, blk_recv.at[row], z_peer, t).start()

    def on_home(*ns):
        @pl.when(home)
        def _():
            for n in ns:
                home_relay(n)

    def on_land(*ns):
        @pl.when(jnp.logical_not(home))
        def _():
            for n in ns:
                land_relay(n)

    def spread_column(k):
        for i in range(PIECES):
            c = chip(x, y, near[k])
            token_wait(c, i)
            ref = xall.at[c, part_of(i)]
            go(remote(ref, ref, tok_send, tok_recv.at[c, i], x_peer, t), "tok")
            go(remote(ref, ref, tok_send, tok_recv.at[c, i], y_peer, t), "tok")

    def cross_plane(k):
        c = chip(1 - x, y, near[k])
        token_wait(c, 0)
        ref = xall.at[c, part_of(0)]
        go(remote(ref, ref, tok_send, tok_recv.at[c, 0], y_peer, t), "tok")
        c = chip(x, 1 - y, near[k])
        token_wait(c, 1)
        ref = xall.at[c, part_of(1)]
        go(remote(ref, ref, tok_send, tok_recv.at[c, 1], x_peer, t), "tok")

    def plane_of(g):
        value = near[0]
        for k in range(1, DEEP):
            value = jnp.where(g == k, near[k], value)
        return value

    def slots_of(g):
        return [PLANE * plane_of(g) + q for q in range(PLANE)]

    def exchange(c):
        return remote(give.at[c], got.at[c], give_send, give_recv, s, 1 - t)

    def project(g):
        slots = slots_of(g)
        cz = plane_of(g)
        token_wait(chip(1 - x, y, cz), 1)
        token_wait(chip(x, 1 - y, cz), 0)
        token_wait(chip(1 - x, 1 - y, cz), 0)
        token_wait(chip(1 - x, 1 - y, cz), 1)
        rows_in = jnp.concatenate([xall[c] for c in slots], axis=0)
        wide = jnp.dot(rows_in, wall[...], preferred_element_type=jnp.float32)
        for i, c in enumerate(slots):
            part_rows = slice(i * length, (i + 1) * length)
            keep[c] = wide[part_rows, : 2 * width]
            give[c] = wide[part_rows, 2 * width :]
        for c in slots:
            exchange(c).start()

    on_home(0)
    gates()
    on_home(1, 2)
    spread_column(1)
    on_home(3)
    cross_plane(0)
    pass_gates(1)
    on_land(0, 1)
    along_z(3, tokv)
    spread_column(2)
    cross_plane(1)
    pass_gates(2)
    on_land(2, 3)
    spread_column(3)
    pass_gates(3)
    cross_plane(2)
    cross_plane(3)

    for n in range(PLANE):
        row = (1 - prompt) * PLANE + n
        ref = block_of(row)
        remote(ref, ref, own_sem, blk_recv.at[row], s, t).wait_recv()

    relayed = gall.at[pl.ds(0, DEEP * (PLANE - 1))]
    pltpu.make_async_copy(relayed, relayed, g_recv).wait()

    many = PLANE * length

    def left_form(full):
        two = full[:, : many // 2] + full[:, many // 2 :]
        high, low = halves(two + pltpu.roll(two, length, 1))
        return jnp.concatenate([high, low], axis=1)

    def right_form(full):
        blocks = [full[i * length : (i + 1) * length] for i in range(PLANE)]
        high, low = halves((blocks[0] + blocks[1]) + (blocks[2] + blocks[3]))
        return jnp.concatenate([high, low, high, low], axis=0)

    def one_dot(a, b, dims=NN):
        return lax.dot_general(a, b, dims, preferred_element_type=jnp.float32)

    def packed_dot(a, b):
        first = one_dot(jnp.concatenate(a, axis=1), jnp.concatenate([b[0], b[0]], axis=0))
        return first + one_dot(a[0], b[1])

    def maps_of(wide, bare_beta, bare_decay, added_decay):
        acted = silu(wide.astype(jnp.bfloat16).astype(jnp.float32))
        k = acted[:, :width]
        k = k * lax.rsqrt(jnp.sum(k * k, axis=-1, keepdims=True) + EPSILON)
        v = acted[:, width:]
        beta_row = sigmoid(bare_beta + offset[j])
        fade_row = added_decay - speed[j] * softplus(bare_decay)
        r = lax.broadcasted_iota(jnp.int32, (many, many), 0)
        c = lax.broadcasted_iota(jnp.int32, (many, many), 1)
        same = r // length == c // length
        strict = jnp.logical_and(same, r > c)
        eye = r == c

        def column(mask, row):
            return jnp.sum(jnp.where(mask, row, 0.0), axis=1, keepdims=True)

        def kept(full):
            return jnp.where(same, full, 0.0)

        sum_col = column(jnp.logical_and(same, r >= c), fade_row)
        all_col = column(same, fade_row)
        beta_col = column(eye, beta_row)
        sum_row = jnp.sum(jnp.where(eye, sum_col, 0.0), axis=0, keepdims=True)
        scaled = k * beta_col
        (high, low), (k_high, k_low) = halves(scaled), halves(k)
        inner_products = one_dot(
            jnp.concatenate([high, low], axis=1), jnp.concatenate([k_high, k_high], axis=1), NT
        ) + one_dot(high, k_low, NT)
        spread = jnp.exp(jnp.where(strict, sum_col - sum_row, 0.0))
        lower = jnp.where(strict, inner_products * spread, 0.0)
        left, right = left_form(lower), right_form(lower)
        inverse = jnp.where(eye, 1.0, 0.0) - lower
        reached = 2
        while reached < length:
            power = kept(one_dot(left, right))
            right = right_form(power)
            inverse = inverse + kept(one_dot(left_form(inverse), right))
            reached *= 2
            if reached < length:
                left = left_form(power)
        inverse = left_form(inverse)
        targets = halves(jnp.concatenate([scaled * jnp.exp(sum_col), v * beta_col], axis=1))
        tail = halves(k * jnp.exp(all_col - sum_col))
        last = jnp.exp(all_col)
        unit = (
            lax.broadcasted_iota(jnp.int32, (width, width), 0)
            == lax.broadcasted_iota(jnp.int32, (width, width), 1)
        ).astype(jnp.float32)
        pairs = []
        for i in range(PLANE):
            at = slice(i * length, (i + 1) * length)
            high, low = targets[0][at], targets[1][at]
            solved = one_dot(inverse[at], jnp.concatenate([high, low, high, low], axis=0))
            high, low = halves(solved)
            keys = jnp.concatenate([tail[0][at]] * 2 + [tail[1][at]] * 2, axis=0)
            maps = one_dot(keys, jnp.concatenate([high, low, high, low], axis=0), TN)
            moves = last[i * length : i * length + 1] * unit - maps[:, :width]
            pairs.append((moves, maps[:, width:]))
        return pairs

    def join(late, early):
        both = packed_dot(halves(late[0]), halves(jnp.concatenate(early, axis=1)))
        return both[:, :width], both[:, width:] + late[1]

    groups = peers // PLANE
    own.wait()
    lax.fori_loop(0, groups, lambda g, carry: (project(g), carry)[1], 0)

    pltpu.make_async_copy(got, got, give_recv).wait()
    slot = slot_of(s)
    carried = None
    for g in range(groups):
        slots = range(g * PLANE, (g + 1) * PLANE)

        def row_of(kind, slots=slots):
            return jnp.concatenate([gall[c, kind : kind + 1, :] for c in slots], axis=1)

        wide = jnp.concatenate([keep[c] + got[c] for c in slots], axis=0)
        pairs = maps_of(wide, row_of(0), row_of(1), row_of(2))
        second = join(pairs[1], pairs[0])
        chain = [pairs[0], second, join(pairs[2], second), join(join(pairs[3], pairs[2]), second)]
        shifts = [shift for _, shift in chain]
        if carried is not None:
            shifts = [
                packed_dot(halves(move), carried) + shift for move, shift in chain
            ]
        carried = halves(shifts[-1])
        for c, shift in zip(slots, shifts):
            states[c] = shift.astype(jnp.bfloat16)
        if g == groups - 1:
            break
        for off in (1, 2, 3, 0):
            to = g * PLANE + (s + off) % PLANE
            copy = remote(
                states.at[to], bound.at[slot], b_send, b_recv, to, t
            )
            if off:
                go(copy)
            else:
                pl.when(z != g)(copy.start)
    end = shifts[-1].astype(jnp.bfloat16)
    final[slot] = end
    def pass_on(slot_at, to):
        ref = final.at[slot_at]
        go(remote(ref, ref, f_send, f_recv.at[slot_at], to, t), "final")

    def store_final(slot_at):
        pltpu.make_async_copy(final.at[slot_at], final_out.at[slot_at], final_sem).start()

    def arrived(slot_at):
        ref = final.at[slot_at]
        remote(ref, ref, own_sem, f_recv.at[slot_at], s, t).wait_recv()
        store_final(slot_at)

    def own_row_of(ref):
        two = ref[:, pl.ds(pl.multiple_of(j * width, 128), width)].astype(jnp.float32)
        return jnp.where(prompt == 0, two[0:1], two[1:2])

    q1 = silu(own_row_of(probe))
    k1 = silu(own_row_of(address))
    k1 = k1 * lax.rsqrt(jnp.sum(k1 * k1, axis=-1, keepdims=True) + EPSILON)
    v1 = silu(own_row_of(content))
    b1 = sigmoid(jnp.full((1, width), strength[prompt, j], jnp.float32))
    q_and_k = jnp.concatenate([q1, k1, jnp.zeros((6, width), jnp.float32)], axis=0)
    recalled = jnp.dot(
        q_and_k,
        end.astype(jnp.float32),
        precision=HIGHEST_ACCURACY,
        preferred_element_type=jnp.float32,
    )
    weight = b1 * jnp.sum(q1 * k1, axis=-1, keepdims=True)
    read = recalled[0:1] + weight * (v1 - recalled[1:2])
    normed = read * lax.rsqrt(jnp.mean(read * read, axis=-1, keepdims=True) + EPSILON)
    gated = normed * gain[...] * silu(own_row_of(outgate))
    rmsg[...] = jnp.broadcast_to(gated.astype(jnp.bfloat16).astype(jnp.float32), rmsg.shape)
    for off in range(1, peers):
        to = (s + off) % peers
        go(remote(rmsg, rall.at[slot], r_send, r_recv, to, t))
    rall[slot] = rmsg[...]

    others = near[1:]
    for cz in others:
        pass_on(slot, chip(x, y, cz))
    pass_on(slot, y_peer)
    pass_on(slot, x_peer)
    last_plane = DEEP - 1
    for off in (1, 2, 3, 0):
        to = last_plane * PLANE + (s + off) % PLANE
        copy = remote(
            states.at[to], bound.at[slot], b_send, b_recv, to, t
        )
        if off:
            go(copy)
        else:
            pl.when(z != last_plane)(copy.start)
    bound[slot] = states[s]
    store_final(slot)
    for cz in others:
        come = slot_of(chip(x, y, cz))
        arrived(come)
        pass_on(come, y_peer)
        pass_on(come, x_peer)
    far = pl.ds(0, peers - 1)
    pltpu.make_async_copy(rall.at[far], rall.at[far], r_recv).wait()
    lines = [
        jnp.concatenate([rall[p * heads + h, 0:1, :] for h in range(heads)], axis=1)
        for p in range(2)
    ]
    lines.append(jnp.zeros((6, heads * width), jnp.float32))
    heads_read = jnp.concatenate(lines, axis=0).astype(jnp.bfloat16)
    loads[4].wait()
    terms = jnp.dot(heads_read, rv[...], preferred_element_type=jnp.float32)
    part[...] = terms.astype(jnp.bfloat16).astype(jnp.float32)
    swap = remote(part, partgot, t_send, t_recv, s, 1 - t)
    swap.start()
    swap.wait()
    mixed[...] = (part[...] + partgot[...])[:2].astype(mixed.dtype)

    for cz in near:
        come = slot_of(chip(x, 1 - y, cz))
        arrived(come)
        pass_on(come, x_peer)

    for cz in range(DEEP):
        for cy in range(2):
            arrived(slot_of(chip(1 - x, cy, cz)))
    pltpu.make_async_copy(bound.at[far], bound.at[far], b_recv).wait()
    stored = pltpu.make_async_copy(bound, bound_out, bound_sem)
    stored.start()

    def sent_all(ref, sem):
        pltpu.make_async_copy(ref, ref, sem).wait()

    sent_all(xall.at[pl.ds(0, sent["tok"] // PIECES)], tok_send)
    sent_all(wcross.at[pl.ds(0, PLANE - 1)], w_send)
    sent_all(wcross, relay_send)

    @pl.when(home)
    def _():
        sent_all(wcross, cross_send)

    @pl.when(jnp.logical_not(home))
    def _():
        sent_all(wcross.at[0], w_away)

    sent_all(gz.at[pl.ds(0, DEEP - 1)], gz_send)
    sent_all(relayed, g_send)
    sent_all(give, give_send)
    sent_all(final.at[pl.ds(0, sent["final"])], f_send)
    sent_all(states.at[far], b_send)
    sent_all(rall.at[far], r_send)
    sent_all(final, final_sem)
    stored.wait()


def prefill(tok, wk, wv, gate_b, gate_a, add, offset, speed, first, strength, gain, readout, peers):
    _, length, model_width = tok.shape
    heads = add.shape[1]
    rows = wk.shape[0]
    width = ADDRESS_WIDTH
    half = model_width // 2
    dma = pltpu.SemaphoreType.DMA
    anywhere = pl.BlockSpec(memory_space=pl.ANY)
    vmem = pl.BlockSpec(memory_space=pltpu.VMEM)
    smem = pl.BlockSpec(memory_space=pltpu.SMEM)
    f32, bf16 = jnp.float32, jnp.bfloat16
    return pl.pallas_call(
        lambda *refs: prefill_kernel(peers, *refs),
        out_shape=(
            jax.ShapeDtypeStruct((peers, width, width), bf16),
            jax.ShapeDtypeStruct((peers, width, width), bf16),
            jax.ShapeDtypeStruct((2, readout.shape[1]), bf16),
        ),
        in_specs=[anywhere] * 6 + [smem] * 2 + [vmem] * 4 + [smem, vmem, anywhere],
        out_specs=(anywhere, anywhere, vmem),
        scratch_shapes=[
            pltpu.VMEM((peers, width, width), bf16),
            pltpu.VMEM((peers, width, width), bf16),
            pltpu.VMEM((peers, length, half), bf16),
            pltpu.VMEM((half, 4 * width), bf16),
            pltpu.VMEM((PLANE, rows, 4 * width), bf16),
            pltpu.VMEM(tok.shape, bf16),
            pltpu.VMEM((2,) + gate_b.shape, bf16),
            pltpu.VMEM(add.shape, f32),
            pltpu.VMEM((2, 2, gate_b.shape[0], length), f32),
            pltpu.VMEM((2, heads, 8, length), f32),
            pltpu.VMEM((DEEP, PLANE, 8, length), f32),
            pltpu.VMEM((peers, 8, length), f32),
            pltpu.VMEM((peers, length, 2 * width), f32),
            pltpu.VMEM((peers, length, 2 * width), f32),
            pltpu.VMEM((peers, length, 2 * width), f32),
            pltpu.VMEM((peers, width, width), bf16),
            pltpu.VMEM(readout.shape, bf16),
            pltpu.VMEM((8, width), f32),
            pltpu.VMEM((peers, 8, width), f32),
            pltpu.VMEM((8, readout.shape[1]), f32),
            pltpu.VMEM((8, readout.shape[1]), f32),
            dma((5,)),
            dma(()),
            dma(()),
            dma((peers, PIECES)),
            dma(()),
            dma(()),
            dma((PLANE,)),
            dma((PLANE,)),
            dma(()),
            dma(()),
            dma((2 * PLANE,)),
            dma(()),
            dma((DEEP,)),
            dma(()),
            dma(()),
            dma(()),
            dma(()),
            dma(()),
            dma((peers,)),
            dma(()),
            dma(()),
            dma(()),
            dma(()),
            dma(()),
            dma(()),
            dma(()),
            dma(()),
        ],
        compiler_params=pltpu.CompilerParams(has_side_effects=True, collective_id=0),
        name="prefill",
    )(tok, wk, wv, gate_b, gate_a, add, offset, speed, *first, strength, gain, readout)


def hand_over(*arrays):
    def kernel(*refs):
        count = len(arrays)
        sources, targets, held = (refs[i * count : (i + 1) * count] for i in range(3))
        came, left = refs[3 * count :]
        steps = []
        for i in range(count):
            steps.append(
                (
                    pltpu.make_async_copy(sources[i], held[i], came.at[i]),
                    pltpu.make_async_copy(held[i], targets[i], left.at[i]),
                )
            )
        for first, _ in steps:
            first.start()
        for first, second in steps:
            first.wait()
            second.start()
        for _, second in steps:
            second.wait()

    anywhere = pl.BlockSpec(memory_space=pl.ANY)
    return pl.pallas_call(
        kernel,
        out_shape=tuple(jax.ShapeDtypeStruct(a.shape, a.dtype) for a in arrays),
        in_specs=[anywhere] * len(arrays),
        out_specs=(anywhere,) * len(arrays),
        scratch_shapes=[pltpu.VMEM(a.shape, a.dtype) for a in arrays]
        + [pltpu.SemaphoreType.DMA((len(arrays),))] * 2,
        name="hand_over",
    )(*arrays)


def per_device_heads(
    layer_source_tokens,
    address_projection,
    content_projection,
    strength_projection,
    fading_driver_projection,
    strength_offset,
    channel_fading_speed,
    added_fading_exponent,
    first_step_probe,
    first_step_address,
    first_step_content,
    first_step_outgate,
    first_step_strength_raw,
    channel_scaling_factor,
    readout_projection,
):
    peers = lax.axis_size("sp")
    head_local = channel_fading_speed.shape[0]
    width = ADDRESS_WIDTH
    final, bound, mixed = prefill(
        layer_source_tokens,
        address_projection,
        content_projection,
        strength_projection.T,
        fading_driver_projection.T,
        jnp.swapaxes(added_fading_exponent, 1, 2),
        strength_offset,
        channel_fading_speed,
        (first_step_probe, first_step_address, first_step_content, first_step_outgate),
        first_step_strength_raw,
        channel_scaling_factor.reshape(1, width),
        readout_projection,
        peers,
    )
    final, bound, mixed = hand_over(final, bound, mixed)
    state_cache = final.reshape(2, head_local, width, width)
    boundary_cache = bound.reshape(2, 1, head_local, width, width)
    return (state_cache, mixed, boundary_cache)


def by_heads(mesh):
    def choose_form(*args):
        seq_count, length, model_width = args[0].shape
        peers, heads = lax.axis_size("sp"), args[6].shape[0]
        fits = (
            lax.axis_size("tp") == 2
            and seq_count == 2
            and peers == DEEP * PLANE
            and heads == 2 * PLANE
            and length == BLOCK
            and args[1].shape[0] * peers == model_width
        )
        return per_device_heads(*args) if fits else per_device(*args)

    return choose_form


def solution(mesh):
    return jax.shard_map(
        by_heads(mesh),
        mesh=mesh,
        in_specs=(
            P(None, "sp", None),
            P("sp", "tp"),
            P("sp", "tp"),
            P(),
            P(),
            P("tp"),
            P("tp"),
            P(None, "sp", "tp"),
            P(None, "tp"),
            P(None, "tp"),
            P(None, "tp"),
            P(None, "tp"),
            P(None, "tp"),
            P(),
            P("tp", "sp"),
        ),
        out_specs=(P(None, "tp", None, None), P(None, "sp"), P(None, "sp", "tp", None, None)),
        check_vma=False,
    )
```

```python
import jax
import jax.numpy as jnp
from jax import lax
from jax.experimental import pallas as pl
from jax.experimental.pallas import tpu as pltpu
from jax.sharding import PartitionSpec as P

ADDRESS_WIDTH = 128
BLOCK = 64


EPSILON = 1e-06
HIGHEST_ACCURACY = lax.Precision.HIGHEST


def prefix(array, axis, combine, identity):
    peers, index = (lax.axis_size(axis), lax.axis_index(axis))
    everything = jax.tree.map(
        lambda part, kind: lax.all_gather(part.astype(kind), axis),
        array,
        (jnp.bfloat16, jnp.bfloat16),
    )
    start = jax.tree.map(
        lambda part, zero: jnp.broadcast_to(jnp.asarray(zero, part.dtype), part.shape),
        array,
        identity,
    )

    def step(k, before):
        reached = k < index
        new = combine(
            before, jax.tree.map(lambda part, own: part[k].astype(own.dtype), everything, array)
        )
        return jax.tree.map(lambda a, b: jnp.where(reached, a, b), new, before)

    return lax.fori_loop(0, peers, step, start)


def as_sent(array):
    return jax.tree.map(lambda a: a.astype(jnp.bfloat16) if a.dtype == jnp.float32 else a, array)


def broadcast(value, axis, source):
    kept = jnp.where(lax.axis_index(axis) == source, value, 0).astype(value.dtype)
    return lax.psum(kept, axis)


def unit_inverse(lower_part):
    matrix_order = lower_part.shape[-1]
    identity = jnp.eye(matrix_order, dtype=jnp.float32)
    result = identity - lower_part
    power_term = lower_part
    reached = 2
    while reached < matrix_order:
        power_term = jnp.matmul(power_term, power_term, precision=HIGHEST_ACCURACY)
        result = jnp.matmul(result, identity + power_term, precision=HIGHEST_ACCURACY)
        reached = reached * 2
    return result


def build_arguments(
    address_vectors,
    content_vectors,
    outgate_raw_scores,
    strength_offset,
    channel_fading_speed,
    added_fading_exponent,
    channel_width,
):
    length = address_vectors.shape[0]
    attention_channels_total = channel_fading_speed.shape[0]
    address_token_slab = jax.nn.silu(address_vectors.astype(jnp.float32)).reshape(
        length, attention_channels_total, channel_width
    )
    address_token_slab = address_token_slab * lax.rsqrt(
        jnp.sum(address_token_slab * address_token_slab, axis=-1, keepdims=True) + EPSILON
    )
    content_token_slab = jax.nn.silu(content_vectors.astype(jnp.float32)).reshape(
        length, attention_channels_total, channel_width
    )
    strength_raw_expanded = outgate_raw_scores.astype(jnp.float32)
    storing_strength = jax.nn.sigmoid(
        strength_raw_expanded[:, :attention_channels_total] + strength_offset
    )
    fading_exponent = added_fading_exponent - channel_fading_speed * jax.nn.softplus(
        strength_raw_expanded[:, attention_channels_total:]
    )
    return (address_token_slab, content_token_slab, storing_strength, fading_exponent)


def range_map(address_token_slab, content_token_slab, storing_strength, fading_exponent, block):
    length, attention_channels_total, channel_width = address_token_slab.shape
    blocks = length // block

    def split_blocks(tensor):
        moved_axes = jnp.swapaxes(tensor, 0, 1)
        return moved_axes.reshape((attention_channels_total, blocks, block) + moved_axes.shape[2:])

    block_keys = split_blocks(address_token_slab)
    block_values = split_blocks(content_token_slab)
    block_beta = split_blocks(storing_strength)
    cumulative = jnp.cumsum(split_blocks(fading_exponent), axis=-1)
    positions = jnp.arange(block)
    strict = positions[:, None] > positions[None, :]
    spread_log = jnp.where(strict, cumulative[..., :, None] - cumulative[..., None, :], 0.0)
    scaled_keys = block_keys * block_beta[..., None]
    inner_prod = jnp.einsum("hnik,hnjk->hnij", scaled_keys, block_keys, precision=HIGHEST_ACCURACY)
    lower_part = jnp.where(strict, inner_prod * jnp.exp(spread_log), 0.0)
    inverse = unit_inverse(lower_part)
    targets = jnp.concatenate(
        [block_values * block_beta[..., None], scaled_keys * jnp.exp(cumulative)[..., None]],
        axis=-1,
    )
    solved = jnp.einsum("hnij,hnjk->hnik", inverse, targets, precision=HIGHEST_ACCURACY)
    updates = solved[..., :channel_width]
    key_weights = solved[..., channel_width:]
    tail_keys = block_keys * jnp.exp(cumulative[..., -1:] - cumulative)[..., None]
    last_decay = jnp.exp(cumulative[..., -1])
    identity = jnp.eye(channel_width, dtype=jnp.float32)

    def advance(state_pair, block_items):
        transition, carried_state = state_pair
        update_index, weight_index, tail_index, last_index = block_items
        fresh_value_rows = update_index - jnp.einsum(
            "xbg,xgp->xbp", weight_index, carried_state, precision=HIGHEST_ACCURACY
        )
        carried_state = carried_state * last_index[:, None, None] + jnp.einsum(
            "tjo,tjw->tow", tail_index, fresh_value_rows, precision=HIGHEST_ACCURACY
        )
        block_move = last_index[:, None, None] * identity - jnp.einsum(
            "hck,hcj->hkj", tail_index, weight_index, precision=HIGHEST_ACCURACY
        )
        transition = jnp.einsum("hij,hjk->hik", block_move, transition, precision=HIGHEST_ACCURACY)
        return ((transition, carried_state), None)

    initial = (
        jnp.broadcast_to(identity, (attention_channels_total, channel_width, channel_width)),
        jnp.zeros((attention_channels_total, channel_width, channel_width), jnp.float32),
    )
    block_items = (
        jnp.moveaxis(updates, 1, 0),
        jnp.moveaxis(key_weights, 1, 0),
        jnp.moveaxis(tail_keys, 1, 0),
        jnp.moveaxis(last_decay, 1, 0),
    )
    (transition, carried_state), _ = lax.scan(advance, initial, block_items)
    return (transition, carried_state)


def read_heads(
    state_cache,
    first_step_probe,
    first_step_address,
    first_step_content,
    first_step_outgate,
    first_step_strength_raw,
    channel_scaling_factor,
):
    seq_count, attention_channels_total, channel_width, _ = state_cache.shape
    carried_state = state_cache.astype(jnp.float32)

    def activate(tensor):
        return jax.nn.silu(tensor.astype(jnp.float32)).reshape(
            seq_count, attention_channels_total, channel_width
        )

    query_rows = activate(first_step_probe)
    address_token_slab = activate(first_step_address)
    address_token_slab = address_token_slab * lax.rsqrt(
        jnp.sum(address_token_slab * address_token_slab, axis=-1, keepdims=True) + EPSILON
    )
    content_token_slab = activate(first_step_content)
    storing_strength = jax.nn.sigmoid(first_step_strength_raw)
    recalled = jnp.einsum(
        "nhk,nhkv->nhv", address_token_slab, carried_state, precision=HIGHEST_ACCURACY
    )
    updated = (
        carried_state
        + storing_strength[..., None, None]
        * address_token_slab[..., :, None]
        * (content_token_slab - recalled)[..., None, :]
    )
    output = jnp.einsum("nhk,nhkv->nhv", query_rows, updated, precision=HIGHEST_ACCURACY)
    normed = (
        output
        * lax.rsqrt(jnp.mean(output * output, axis=-1, keepdims=True) + EPSILON)
        * channel_scaling_factor
    )
    gated_out = normed * activate(first_step_outgate)
    return gated_out.reshape(seq_count, attention_channels_total * channel_width).astype(
        jnp.bfloat16
    )


def matmul_maps(left, right):
    return jnp.einsum("shij,shjk->shik", left, right, precision=HIGHEST_ACCURACY)


def join_pairs(earlier, later):
    return (matmul_maps(later[0], earlier[0]), matmul_maps(later[0], earlier[1]) + later[1])


def per_device(
    layer_source_tokens,
    address_projection,
    content_projection,
    strength_projection,
    fading_driver_projection,
    strength_offset,
    channel_fading_speed,
    added_fading_exponent,
    first_step_probe,
    first_step_address,
    first_step_content,
    first_step_outgate,
    first_step_strength_raw,
    channel_scaling_factor,
    readout_projection,
):
    head_local = channel_fading_speed.shape[0]
    first_head = lax.axis_index("tp") * head_local
    beta_slice = lax.dynamic_slice_in_dim(strength_projection, first_head, head_local, 1)
    alpha_slice = lax.dynamic_slice_in_dim(fading_driver_projection, first_head, head_local, 1)
    seq_count, local_len, model_width = layer_source_tokens.shape
    flat_rows = layer_source_tokens.reshape(seq_count * local_len, model_width)
    key_sum = jnp.dot(
        flat_rows,
        lax.all_gather(address_projection, "sp", axis=0, tiled=True),
        preferred_element_type=jnp.float32,
    )
    value_sum = jnp.dot(
        flat_rows,
        lax.all_gather(content_projection, "sp", axis=0, tiled=True),
        preferred_element_type=jnp.float32,
    )
    beta_sum = jnp.dot(flat_rows, beta_slice, preferred_element_type=jnp.float32)
    alpha_sum = jnp.dot(flat_rows, alpha_slice, preferred_element_type=jnp.float32)
    outgate_raw_scores = (
        jnp.concatenate([beta_sum, alpha_sum], axis=1)
        .astype(jnp.bfloat16)
        .reshape(seq_count, local_len, -1)
    )
    address_vectors = key_sum.astype(jnp.bfloat16).reshape(seq_count, local_len, -1)
    content_vectors = value_sum.astype(jnp.bfloat16).reshape(seq_count, local_len, -1)
    transitions = []
    offsets = []
    for prompt_number in range(seq_count):
        address_token_slab, content_token_slab, storing_strength, fading_exponent = build_arguments(
            address_vectors[prompt_number],
            content_vectors[prompt_number],
            outgate_raw_scores[prompt_number],
            strength_offset,
            channel_fading_speed,
            added_fading_exponent[prompt_number],
            ADDRESS_WIDTH,
        )
        transition, carried_state = range_map(
            address_token_slab, content_token_slab, storing_strength, fading_exponent, BLOCK
        )
        transitions.append(transition)
        offsets.append(carried_state)
    transition = jnp.stack(transitions)
    offset = jnp.stack(offsets)
    identity = jnp.broadcast_to(jnp.eye(ADDRESS_WIDTH, dtype=jnp.float32), transition.shape)
    entered = prefix((transition, offset), "sp", join_pairs, (identity, jnp.zeros_like(offset)))
    leaving = matmul_maps(transition, entered[1]) + offset
    final = broadcast(as_sent(leaving), "sp", lax.axis_size("sp") - 1).astype(leaving.dtype)
    boundary_cache = leaving.astype(jnp.bfloat16)[:, None]
    state_cache = final.astype(jnp.bfloat16)
    heads_read = read_heads(
        state_cache,
        first_step_probe,
        first_step_address,
        first_step_content,
        first_step_outgate,
        first_step_strength_raw,
        channel_scaling_factor,
    )
    group_terms = jnp.dot(
        heads_read, readout_projection, preferred_element_type=jnp.float32
    ).astype(jnp.bfloat16)
    mixed_read = lax.psum(group_terms.astype(jnp.float32).astype(jnp.bfloat16), "tp")
    return (state_cache, mixed_read, boundary_cache)


MESH = pl.DeviceIdType.MESH
PIECES = 2
DEEP = 4
PLANE = 4


def remote(src, dst, send, recv, sp, tp):
    return pltpu.make_async_remote_copy(
        src_ref=src,
        dst_ref=dst,
        send_sem=send,
        recv_sem=recv,
        device_id={"sp": sp, "tp": tp},
        device_id_type=MESH,
    )


def silu(v):
    return v / (1.0 + jnp.exp(-v))


def sigmoid(v):
    return 1.0 / (1.0 + jnp.exp(-v))


def softplus(v):
    return jnp.maximum(v, 0.0) + jnp.log1p(jnp.exp(-jnp.abs(v)))


def halves(a):
    high = a.astype(jnp.bfloat16)
    return high, (a - high.astype(jnp.float32)).astype(jnp.bfloat16)


NN = (((1,), (0,)), ((), ()))
NT = (((1,), (1,)), ((), ()))
TN = (((0,), (0,)), ((), ()))


def prefill_kernel(
    peers,
    tok,
    wk,
    wv,
    gate_b,
    gate_a,
    add,
    offset,
    speed,
    probe,
    address,
    content,
    outgate,
    strength,
    gain,
    readout,
    final_out,
    bound_out,
    mixed,
    final,
    bound,
    xall,
    wall,
    wcross,
    tokv,
    gatev,
    addv,
    logit,
    msg,
    gz,
    gall,
    keep,
    give,
    got,
    states,
    rv,
    rmsg,
    rall,
    part,
    partgot,
    load,
    own_sem,
    tok_send,
    tok_recv,
    w_send,
    w_away,
    w_recv,
    c_recv,
    relay_send,
    cross_send,
    blk_recv,
    gz_send,
    gz_recv,
    g_send,
    g_recv,
    give_send,
    give_recv,
    f_send,
    f_recv,
    b_send,
    b_recv,
    r_send,
    r_recv,
    t_send,
    t_recv,
    final_sem,
    bound_sem,
):
    s, t = lax.axis_index("sp"), lax.axis_index("tp")
    heads = add.shape[1]
    width = ADDRESS_WIDTH
    length = tok.shape[1]
    half = tok.shape[2] // 2
    rows = wk.shape[0]
    piece = length // PIECES
    x, y, z = s % 2, (s // 2) % 2, s // PLANE
    prompt, side = z % 2, z // 2
    j = side * PLANE + s % PLANE
    mate = z + 1 - 2 * prompt
    columns = pl.ds(pl.multiple_of(t * half, 128), half)

    def chip(cx, cy, cz):
        return PLANE * cz + 2 * cy + cx

    def slot_of(c):
        return (c // PLANE % 2) * heads + (c // PLANE // 2) * PLANE + c % PLANE

    x_peer, y_peer, z_peer = chip(1 - x, y, z), chip(x, 1 - y, z), chip(x, y, mate)
    diagonal = chip(1 - x, 1 - y, z)
    home = t == side

    def part_of(i):
        return pl.ds(i * piece, piece)

    sent = {"tok": 0, "final": 0}

    def go(copy, kind=None):
        copy.start()
        if kind:
            sent[kind] += 1

    def token_wait(c, i):
        ref = xall.at[c, part_of(i)]
        remote(ref, ref, own_sem, tok_recv.at[c, i], s, t).wait_recv()

    near = [z, mate, DEEP - 1 - z, (z + DEEP // 2) % DEEP]
    barrier = pltpu.get_barrier_semaphore()
    partners = [(chip(x, y, near[k]), t) for k in range(1, DEEP)] + [(s, 1 - t)]
    partners += [(c, core) for c in (x_peer, y_peer, diagonal) for core in (t, 1 - t)]
    for c, core in partners:
        pl.semaphore_signal(
            barrier, inc=1, device_id={"sp": c, "tp": core}, device_id_type=MESH
        )
    loads = []
    for i, (src, dst) in enumerate(
        (
            (tok, tokv),
            (gate_b, gatev.at[0]),
            (gate_a, gatev.at[1]),
            (add, addv),
            (readout, rv),
        )
    ):
        copy = pltpu.make_async_copy(src, dst, load.at[i])
        copy.start()
        loads.append(copy)
    own = pltpu.make_async_copy(tok.at[prompt, :, columns], xall.at[s], own_sem)
    own.start()
    pl.semaphore_wait(barrier, len(partners))

    def along_z(k, source):
        for i in range(PIECES):
            go(
                remote(
                    source.at[near[k] % 2, part_of(i), columns],
                    xall.at[s, part_of(i)],
                    tok_send,
                    tok_recv.at[s, i],
                    chip(x, y, near[k]),
                    t,
                ),
                "tok",
            )

    along_z(1, tok)
    along_z(2, tok)

    side_of = (t + side) % 2
    own_row = s % (peers // 2)
    q_own = s % PLANE
    spot = pl.ds(pl.multiple_of(own_row * rows, 16), rows)

    def weight_copies(dx, dy, cross, kv):
        xd, yd = (x + dx) % 2, (y + dy) % 2
        head = ((side + cross) % 2) * PLANE + 2 * yd + xd
        src = (wk, wv)[kv].at[:, pl.ds(pl.multiple_of(head * width, 128), width)]
        at = pl.ds(pl.multiple_of((2 * side_of + kv) * width, 128), width)
        if cross:
            dst, sem = wcross.at[q_own, :, at], c_recv.at[q_own]
        else:
            dst, sem = wall.at[spot, at], w_recv.at[q_own]
        out = w_send if dx + dy else w_away
        return src, dst, sem, remote(src, dst, out, sem, chip(xd, yd, z), side)

    for dx, dy in ((0, 0), (1, 0), (0, 1), (1, 1)):
        for cross in (1, 0):
            for kv in range(2):
                src, dst, sem, copy = weight_copies(dx, dy, cross, kv)
                if dx + dy == 0:

                    @pl.when(home)
                    def _():
                        pltpu.make_async_copy(src, dst, sem).start()

                    @pl.when(jnp.logical_not(home))
                    def _():
                        copy.start()
                else:
                    go(copy)

    for i in range(PIECES):
        src = tok.at[prompt, part_of(i), columns]
        dst = xall.at[s, part_of(i)]
        go(remote(src, dst, tok_send, tok_recv.at[s, i], x_peer, t), "tok")
        go(remote(src, dst, tok_send, tok_recv.at[s, i], y_peer, t), "tok")

    def gates():
        for copy in loads[:4]:
            copy.wait()
        msg[...] = jnp.zeros_like(msg)
        for p in range(2):
            for kind in range(2):
                logit[p, kind] = (
                    lax.dot_general(gatev[kind], tokv[p], NT, preferred_element_type=jnp.float32)
                    .astype(jnp.bfloat16)
                    .astype(jnp.float32)
                )
            for h in range(heads):
                for kind in range(2):
                    msg[p, h, kind : kind + 1, :] = logit[p, kind, pl.ds(t * heads + h, 1), :]
                msg[p, h, 2:3, :] = addv[p, h : h + 1, :]
        for k in range(1, DEEP):
            src = msg.at[near[k] % 2, pl.ds(near[k] // 2 * PLANE, PLANE)]
            go(remote(src, gz.at[z], gz_send, gz_recv.at[z], chip(x, y, near[k]), t))
        for n, c in enumerate((x_peer, y_peer, diagonal)):
            src = msg.at[prompt, side * PLANE + c % PLANE]
            go(remote(src, gall.at[s], g_send, g_recv, c, t))
        gall[s] = msg[prompt, j]

    def pass_gates(k):
        cz = near[k]
        remote(gz.at[cz], gz.at[cz], own_sem, gz_recv.at[cz], s, t).wait_recv()
        c = chip(x, y, cz)
        for n, to in enumerate((x_peer, y_peer, diagonal)):
            go(remote(gz.at[cz, to % PLANE], gall.at[c], g_send, g_recv, to, t))
        gall[c] = gz[cz, q_own]

    def block_of(row):
        return wall.at[pl.ds(pl.multiple_of(row * rows, 16), rows)]

    def row_at(n):
        q = 2 * ((y + n // 2) % 2) + (x + n % 2) % 2
        return q, prompt * PLANE + q

    def home_relay(n):
        q, row = row_at(n)
        block = block_of(row)
        landing = chip(x, y, (z + DEEP // 2) % DEEP)
        pltpu.make_async_copy(wcross.at[q], wcross.at[q], c_recv.at[q]).wait()
        remote(wcross.at[q], block, cross_send, blk_recv.at[row], landing, t).start()
        pltpu.make_async_copy(block, block, w_recv.at[q]).wait()
        remote(block, block, relay_send, blk_recv.at[row], z_peer, t).start()

    def land_relay(n):
        q, row = row_at(n)
        ref = block_of(row)
        remote(ref, ref, relay_send, blk_recv.at[row], s, t).wait_recv()
        remote(ref, ref, relay_send, blk_recv.at[row], z_peer, t).start()

    def on_home(*ns):
        @pl.when(home)
        def _():
            for n in ns:
                home_relay(n)

    def on_land(*ns):
        @pl.when(jnp.logical_not(home))
        def _():
            for n in ns:
                land_relay(n)

    def spread_column(k):
        for i in range(PIECES):
            c = chip(x, y, near[k])
            token_wait(c, i)
            ref = xall.at[c, part_of(i)]
            go(remote(ref, ref, tok_send, tok_recv.at[c, i], x_peer, t), "tok")
            go(remote(ref, ref, tok_send, tok_recv.at[c, i], y_peer, t), "tok")

    def cross_plane(k):
        c = chip(1 - x, y, near[k])
        token_wait(c, 0)
        ref = xall.at[c, part_of(0)]
        go(remote(ref, ref, tok_send, tok_recv.at[c, 0], y_peer, t), "tok")
        c = chip(x, 1 - y, near[k])
        token_wait(c, 1)
        ref = xall.at[c, part_of(1)]
        go(remote(ref, ref, tok_send, tok_recv.at[c, 1], x_peer, t), "tok")

    def plane_of(g):
        value = near[0]
        for k in range(1, DEEP):
            value = jnp.where(g == k, near[k], value)
        return value

    def slots_of(g):
        return [PLANE * plane_of(g) + q for q in range(PLANE)]

    def exchange(c):
        return remote(give.at[c], got.at[c], give_send, give_recv, s, 1 - t)

    def project(g):
        slots = slots_of(g)
        cz = plane_of(g)
        token_wait(chip(1 - x, y, cz), 1)
        token_wait(chip(x, 1 - y, cz), 0)
        token_wait(chip(1 - x, 1 - y, cz), 0)
        token_wait(chip(1 - x, 1 - y, cz), 1)
        rows_in = jnp.concatenate([xall[c] for c in slots], axis=0)
        wide = jnp.dot(rows_in, wall[...], preferred_element_type=jnp.float32)
        for i, c in enumerate(slots):
            part_rows = slice(i * length, (i + 1) * length)
            keep[c] = wide[part_rows, : 2 * width]
            give[c] = wide[part_rows, 2 * width :]
        for c in slots:
            exchange(c).start()

    on_home(0)
    gates()
    on_home(1, 2)
    spread_column(1)
    on_home(3)
    cross_plane(0)
    along_z(3, tokv)
    cross_plane(1)
    pass_gates(1)
    on_land(0, 1)
    spread_column(2)
    cross_plane(2)
    pass_gates(2)
    on_land(2, 3)
    spread_column(3)
    pass_gates(3)
    cross_plane(3)

    for n in range(PLANE):
        row = (1 - prompt) * PLANE + n
        ref = block_of(row)
        remote(ref, ref, own_sem, blk_recv.at[row], s, t).wait_recv()

    relayed = gall.at[pl.ds(0, DEEP * (PLANE - 1))]
    pltpu.make_async_copy(relayed, relayed, g_recv).wait()

    many = PLANE * length

    def left_form(full):
        two = full[:, : many // 2] + full[:, many // 2 :]
        high, low = halves(two + pltpu.roll(two, length, 1))
        return jnp.concatenate([high, low], axis=1)

    def right_form(full):
        blocks = [full[i * length : (i + 1) * length] for i in range(PLANE)]
        high, low = halves((blocks[0] + blocks[1]) + (blocks[2] + blocks[3]))
        return jnp.concatenate([high, low, high, low], axis=0)

    def one_dot(a, b, dims=NN):
        return lax.dot_general(a, b, dims, preferred_element_type=jnp.float32)

    def packed_dot(a, b):
        first = one_dot(jnp.concatenate(a, axis=1), jnp.concatenate([b[0], b[0]], axis=0))
        return first + one_dot(a[0], b[1])

    def maps_of(wide, bare_beta, bare_decay, added_decay):
        acted = silu(wide.astype(jnp.bfloat16).astype(jnp.float32))
        k = acted[:, :width]
        k = k * lax.rsqrt(jnp.sum(k * k, axis=-1, keepdims=True) + EPSILON)
        v = acted[:, width:]
        beta_row = sigmoid(bare_beta + offset[j])
        fade_row = added_decay - speed[j] * softplus(bare_decay)
        r = lax.broadcasted_iota(jnp.int32, (many, many), 0)
        c = lax.broadcasted_iota(jnp.int32, (many, many), 1)
        same = r // length == c // length
        strict = jnp.logical_and(same, r > c)
        eye = r == c

        def column(mask, row):
            return jnp.sum(jnp.where(mask, row, 0.0), axis=1, keepdims=True)

        def kept(full):
            return jnp.where(same, full, 0.0)

        sum_col = column(jnp.logical_and(same, r >= c), fade_row)
        all_col = column(same, fade_row)
        beta_col = column(eye, beta_row)
        sum_row = jnp.sum(jnp.where(eye, sum_col, 0.0), axis=0, keepdims=True)
        scaled = k * beta_col
        (high, low), (k_high, k_low) = halves(scaled), halves(k)
        inner_products = one_dot(
            jnp.concatenate([high, low], axis=1), jnp.concatenate([k_high, k_high], axis=1), NT
        ) + one_dot(high, k_low, NT)
        spread = jnp.exp(jnp.where(strict, sum_col - sum_row, 0.0))
        lower = jnp.where(strict, inner_products * spread, 0.0)
        left, right = left_form(lower), right_form(lower)
        inverse = jnp.where(eye, 1.0, 0.0) - lower
        reached = 2
        while reached < length:
            power = kept(one_dot(left, right))
            right = right_form(power)
            inverse = inverse + kept(one_dot(left_form(inverse), right))
            reached *= 2
            if reached < length:
                left = left_form(power)
        inverse = left_form(inverse)
        targets = halves(jnp.concatenate([scaled * jnp.exp(sum_col), v * beta_col], axis=1))
        tail = halves(k * jnp.exp(all_col - sum_col))
        last = jnp.exp(all_col)
        unit = (
            lax.broadcasted_iota(jnp.int32, (width, width), 0)
            == lax.broadcasted_iota(jnp.int32, (width, width), 1)
        ).astype(jnp.float32)
        pairs = []
        for i in range(PLANE):
            at = slice(i * length, (i + 1) * length)
            high, low = targets[0][at], targets[1][at]
            solved = one_dot(inverse[at], jnp.concatenate([high, low, high, low], axis=0))
            high, low = halves(solved)
            keys = jnp.concatenate([tail[0][at]] * 2 + [tail[1][at]] * 2, axis=0)
            maps = one_dot(keys, jnp.concatenate([high, low, high, low], axis=0), TN)
            moves = last[i * length : i * length + 1] * unit - maps[:, :width]
            pairs.append((moves, maps[:, width:]))
        return pairs

    def join(late, early):
        both = packed_dot(halves(late[0]), halves(jnp.concatenate(early, axis=1)))
        return both[:, :width], both[:, width:] + late[1]

    groups = peers // PLANE
    own.wait()
    lax.fori_loop(0, groups, lambda g, carry: (project(g), carry)[1], 0)

    pltpu.make_async_copy(got, got, give_recv).wait()
    slot = slot_of(s)
    carried = None
    for g in range(groups):
        slots = range(g * PLANE, (g + 1) * PLANE)

        def row_of(kind, slots=slots):
            return jnp.concatenate([gall[c, kind : kind + 1, :] for c in slots], axis=1)

        wide = jnp.concatenate([keep[c] + got[c] for c in slots], axis=0)
        pairs = maps_of(wide, row_of(0), row_of(1), row_of(2))
        second = join(pairs[1], pairs[0])
        chain = [pairs[0], second, join(pairs[2], second), join(join(pairs[3], pairs[2]), second)]
        shifts = [shift for _, shift in chain]
        if carried is not None:
            shifts = [
                packed_dot(halves(move), carried) + shift for move, shift in chain
            ]
        carried = halves(shifts[-1])
        for c, shift in zip(slots, shifts):
            states[c] = shift.astype(jnp.bfloat16)
        if g == groups - 1:
            break
        for off in (1, 2, 3, 0):
            to = g * PLANE + (s + off) % PLANE
            copy = remote(
                states.at[to], bound.at[slot], b_send, b_recv, to, t
            )
            if off:
                go(copy)
            else:
                pl.when(z != g)(copy.start)
    end = shifts[-1].astype(jnp.bfloat16)
    final[slot] = end
    def pass_on(slot_at, to):
        ref = final.at[slot_at]
        go(remote(ref, ref, f_send, f_recv.at[slot_at], to, t), "final")

    def store_final(slot_at):
        pltpu.make_async_copy(final.at[slot_at], final_out.at[slot_at], final_sem).start()

    def arrived(slot_at):
        ref = final.at[slot_at]
        remote(ref, ref, own_sem, f_recv.at[slot_at], s, t).wait_recv()
        store_final(slot_at)

    def own_row_of(ref):
        two = ref[:, pl.ds(pl.multiple_of(j * width, 128), width)].astype(jnp.float32)
        return jnp.where(prompt == 0, two[0:1], two[1:2])

    q1 = silu(own_row_of(probe))
    k1 = silu(own_row_of(address))
    k1 = k1 * lax.rsqrt(jnp.sum(k1 * k1, axis=-1, keepdims=True) + EPSILON)
    v1 = silu(own_row_of(content))
    b1 = sigmoid(jnp.full((1, width), strength[prompt, j], jnp.float32))
    q_and_k = jnp.concatenate([q1, k1, jnp.zeros((6, width), jnp.float32)], axis=0)
    recalled = jnp.dot(
        q_and_k,
        end.astype(jnp.float32),
        precision=HIGHEST_ACCURACY,
        preferred_element_type=jnp.float32,
    )
    weight = b1 * jnp.sum(q1 * k1, axis=-1, keepdims=True)
    read = recalled[0:1] + weight * (v1 - recalled[1:2])
    normed = read * lax.rsqrt(jnp.mean(read * read, axis=-1, keepdims=True) + EPSILON)
    gated = normed * gain[...] * silu(own_row_of(outgate))
    rmsg[...] = jnp.broadcast_to(gated.astype(jnp.bfloat16).astype(jnp.float32), rmsg.shape)
    for off in range(1, peers):
        to = (s + off) % peers
        go(remote(rmsg, rall.at[slot], r_send, r_recv, to, t))
    rall[slot] = rmsg[...]

    others = near[1:]
    for cz in others:
        pass_on(slot, chip(x, y, cz))
    pass_on(slot, y_peer)
    pass_on(slot, x_peer)
    last_plane = DEEP - 1
    for off in (1, 2, 3, 0):
        to = last_plane * PLANE + (s + off) % PLANE
        copy = remote(
            states.at[to], bound.at[slot], b_send, b_recv, to, t
        )
        if off:
            go(copy)
        else:
            pl.when(z != last_plane)(copy.start)
    bound[slot] = states[s]
    store_final(slot)
    for cz in others:
        come = slot_of(chip(x, y, cz))
        arrived(come)
        pass_on(come, y_peer)
        pass_on(come, x_peer)
    for cz in near:
        come = slot_of(chip(x, 1 - y, cz))
        arrived(come)
        pass_on(come, x_peer)

    far = pl.ds(0, peers - 1)
    pltpu.make_async_copy(rall.at[far], rall.at[far], r_recv).wait()
    lines = [
        jnp.concatenate([rall[p * heads + h, 0:1, :] for h in range(heads)], axis=1)
        for p in range(2)
    ]
    lines.append(jnp.zeros((6, heads * width), jnp.float32))
    heads_read = jnp.concatenate(lines, axis=0).astype(jnp.bfloat16)
    loads[4].wait()
    terms = jnp.dot(heads_read, rv[...], preferred_element_type=jnp.float32)
    part[...] = terms.astype(jnp.bfloat16).astype(jnp.float32)
    swap = remote(part, partgot, t_send, t_recv, s, 1 - t)
    swap.start()
    swap.wait()
    mixed[...] = (part[...] + partgot[...])[:2].astype(mixed.dtype)

    for cz in range(DEEP):
        for cy in range(2):
            arrived(slot_of(chip(1 - x, cy, cz)))
    pltpu.make_async_copy(bound.at[far], bound.at[far], b_recv).wait()
    stored = pltpu.make_async_copy(bound, bound_out, bound_sem)
    stored.start()

    def sent_all(ref, sem):
        pltpu.make_async_copy(ref, ref, sem).wait()

    sent_all(xall.at[pl.ds(0, sent["tok"] // PIECES)], tok_send)
    sent_all(wcross.at[pl.ds(0, PLANE - 1)], w_send)
    sent_all(wcross, relay_send)

    @pl.when(home)
    def _():
        sent_all(wcross, cross_send)

    @pl.when(jnp.logical_not(home))
    def _():
        sent_all(wcross.at[0], w_away)

    sent_all(gz.at[pl.ds(0, DEEP - 1)], gz_send)
    sent_all(relayed, g_send)
    sent_all(give, give_send)
    sent_all(final.at[pl.ds(0, sent["final"])], f_send)
    sent_all(states.at[far], b_send)
    sent_all(rall.at[far], r_send)
    sent_all(final, final_sem)
    stored.wait()


def prefill(tok, wk, wv, gate_b, gate_a, add, offset, speed, first, strength, gain, readout, peers):
    _, length, model_width = tok.shape
    heads = add.shape[1]
    rows = wk.shape[0]
    width = ADDRESS_WIDTH
    half = model_width // 2
    dma = pltpu.SemaphoreType.DMA
    anywhere = pl.BlockSpec(memory_space=pl.ANY)
    vmem = pl.BlockSpec(memory_space=pltpu.VMEM)
    smem = pl.BlockSpec(memory_space=pltpu.SMEM)
    f32, bf16 = jnp.float32, jnp.bfloat16
    return pl.pallas_call(
        lambda *refs: prefill_kernel(peers, *refs),
        out_shape=(
            jax.ShapeDtypeStruct((peers, width, width), bf16),
            jax.ShapeDtypeStruct((peers, width, width), bf16),
            jax.ShapeDtypeStruct((2, readout.shape[1]), bf16),
        ),
        in_specs=[anywhere] * 6 + [smem] * 2 + [vmem] * 4 + [smem, vmem, anywhere],
        out_specs=(anywhere, anywhere, vmem),
        scratch_shapes=[
            pltpu.VMEM((peers, width, width), bf16),
            pltpu.VMEM((peers, width, width), bf16),
            pltpu.VMEM((peers, length, half), bf16),
            pltpu.VMEM((half, 4 * width), bf16),
            pltpu.VMEM((PLANE, rows, 4 * width), bf16),
            pltpu.VMEM(tok.shape, bf16),
            pltpu.VMEM((2,) + gate_b.shape, bf16),
            pltpu.VMEM(add.shape, f32),
            pltpu.VMEM((2, 2, gate_b.shape[0], length), f32),
            pltpu.VMEM((2, heads, 8, length), f32),
            pltpu.VMEM((DEEP, PLANE, 8, length), f32),
            pltpu.VMEM((peers, 8, length), f32),
            pltpu.VMEM((peers, length, 2 * width), f32),
            pltpu.VMEM((peers, length, 2 * width), f32),
            pltpu.VMEM((peers, length, 2 * width), f32),
            pltpu.VMEM((peers, width, width), bf16),
            pltpu.VMEM(readout.shape, bf16),
            pltpu.VMEM((8, width), f32),
            pltpu.VMEM((peers, 8, width), f32),
            pltpu.VMEM((8, readout.shape[1]), f32),
            pltpu.VMEM((8, readout.shape[1]), f32),
            dma((5,)),
            dma(()),
            dma(()),
            dma((peers, PIECES)),
            dma(()),
            dma(()),
            dma((PLANE,)),
            dma((PLANE,)),
            dma(()),
            dma(()),
            dma((2 * PLANE,)),
            dma(()),
            dma((DEEP,)),
            dma(()),
            dma(()),
            dma(()),
            dma(()),
            dma(()),
            dma((peers,)),
            dma(()),
            dma(()),
            dma(()),
            dma(()),
            dma(()),
            dma(()),
            dma(()),
            dma(()),
        ],
        compiler_params=pltpu.CompilerParams(has_side_effects=True, collective_id=0),
        name="prefill",
    )(tok, wk, wv, gate_b, gate_a, add, offset, speed, *first, strength, gain, readout)


def hand_over(*arrays):
    def kernel(*refs):
        count = len(arrays)
        sources, targets, held = (refs[i * count : (i + 1) * count] for i in range(3))
        came, left = refs[3 * count :]
        steps = []
        for i in range(count):
            steps.append(
                (
                    pltpu.make_async_copy(sources[i], held[i], came.at[i]),
                    pltpu.make_async_copy(held[i], targets[i], left.at[i]),
                )
            )
        for first, _ in steps:
            first.start()
        for first, second in steps:
            first.wait()
            second.start()
        for _, second in steps:
            second.wait()

    anywhere = pl.BlockSpec(memory_space=pl.ANY)
    return pl.pallas_call(
        kernel,
        out_shape=tuple(jax.ShapeDtypeStruct(a.shape, a.dtype) for a in arrays),
        in_specs=[anywhere] * len(arrays),
        out_specs=(anywhere,) * len(arrays),
        scratch_shapes=[pltpu.VMEM(a.shape, a.dtype) for a in arrays]
        + [pltpu.SemaphoreType.DMA((len(arrays),))] * 2,
        name="hand_over",
    )(*arrays)


def per_device_heads(
    layer_source_tokens,
    address_projection,
    content_projection,
    strength_projection,
    fading_driver_projection,
    strength_offset,
    channel_fading_speed,
    added_fading_exponent,
    first_step_probe,
    first_step_address,
    first_step_content,
    first_step_outgate,
    first_step_strength_raw,
    channel_scaling_factor,
    readout_projection,
):
    peers = lax.axis_size("sp")
    head_local = channel_fading_speed.shape[0]
    width = ADDRESS_WIDTH
    final, bound, mixed = prefill(
        layer_source_tokens,
        address_projection,
        content_projection,
        strength_projection.T,
        fading_driver_projection.T,
        jnp.swapaxes(added_fading_exponent, 1, 2),
        strength_offset,
        channel_fading_speed,
        (first_step_probe, first_step_address, first_step_content, first_step_outgate),
        first_step_strength_raw,
        channel_scaling_factor.reshape(1, width),
        readout_projection,
        peers,
    )
    final, bound, mixed = hand_over(final, bound, mixed)
    state_cache = final.reshape(2, head_local, width, width)
    boundary_cache = bound.reshape(2, 1, head_local, width, width)
    return (state_cache, mixed, boundary_cache)


def by_heads(mesh):
    def choose_form(*args):
        seq_count, length, model_width = args[0].shape
        peers, heads = lax.axis_size("sp"), args[6].shape[0]
        fits = (
            lax.axis_size("tp") == 2
            and seq_count == 2
            and peers == DEEP * PLANE
            and heads == 2 * PLANE
            and length == BLOCK
            and args[1].shape[0] * peers == model_width
        )
        return per_device_heads(*args) if fits else per_device(*args)

    return choose_form


def solution(mesh):
    return jax.shard_map(
        by_heads(mesh),
        mesh=mesh,
        in_specs=(
            P(None, "sp", None),
            P("sp", "tp"),
            P("sp", "tp"),
            P(),
            P(),
            P("tp"),
            P("tp"),
            P(None, "sp", "tp"),
            P(None, "tp"),
            P(None, "tp"),
            P(None, "tp"),
            P(None, "tp"),
            P(None, "tp"),
            P(),
            P("tp", "sp"),
        ),
        out_specs=(P(None, "tp", None, None), P(None, "sp"), P(None, "sp", "tp", None, None)),
        check_vma=False,
    )
```
